32 devices in a mesh: sp: 4 (over z), fs: 4 (over y, x), tp: 2 (over core).
Axes of the slice: x: 2, y: 2, z: 4, core: 2. Of those that a mesh axis runs over, the one named last changes fastest.
Arguments:
- tokens: bfloat16 [8, 1536, 2048], P('fs', ('sp', 'tp')), may hold values from -6 to 6
- norm_gain: float32 [2048], replicated, may hold values from 0.1 to 1.9
- chain_entry: bfloat16 [2048, 2048], P(('sp', 'fs'), 'tp'), may hold values from -0.125 to 0.125
- pool_entry: bfloat16 [2048, 2048], P(('sp', 'fs'), 'tp'), may hold values from -0.125 to 0.125
- conv_taps: bfloat16 [4, 2048], P(None, 'tp'), may hold values from -3 to 3
- recur_gate: bfloat16 [8, 256, 256], P('tp'), may hold values from -0.375 to 0.375
- input_gate: bfloat16 [8, 256, 256], P('tp'), may hold values from -0.375 to 0.375
- decay_log: float32 [2048], P('tp'), may hold values from -9 to 5
- decay_shift: float32 [8, 1536, 2048], P('fs', 'sp', 'tp'), may hold values from -1 to 0
- start_state: float32 [8, 2048], P('fs', 'tp'), may hold values from -6 to 6
- pool_mix: bfloat16 [8, 256, 256], P('tp'), may hold values from -0.375 to 0.375
- pool_scale: float32 [2048], P('tp'), may hold values from 0.1 to 1.9
- chain_exit: bfloat16 [2048, 2048], P('tp', ('sp', 'fs')), may hold values from -0.09375 to 0.09375
- pool_exit: bfloat16 [2048, 2048], P('tp', ('sp', 'fs')), may hold values from -0.09375 to 0.09375
Outputs:
- mixed_rows: bfloat16 [8, 1536, 2048], P('fs', ('sp', 'tp'))
The draws below stay inside these ranges and needn't reach their ends.
All inputs are finite; a program needn't handle non-finite values.
Results may differ from the reference program's by a relative error of at most 0.01.
Values may be sent and summed in bfloat16 or wider, within the bound.
A program may use at most 128 MiB of HBM per device.

```python
import math
import jax
import jax.numpy as jnp
from jax import lax

D = 2048
HEAD = 256
CHAIN_HEADS = 8
POOL_GROUPS = 8
CONV_TAPS = 4
POOL_SPAN = 16
TOK_DEV = 384
CHAIN_WIDTH = 2048
POOL_WIDTH = 2048
LEN = 1536
SEQS = 8


def draw_decay_log(key, part):
    inner = jax.random.fold_in(key, 7)
    return jax.random.uniform(inner, (CHAIN_WIDTH,), jnp.float32, -9.0, 5.0)


def draw_decay_shift(key, part):
    inner = jax.random.fold_in(key, 11)
    first_key, second_key, third_key, fourth_key, fifth_key, sixth_key, seventh_key = jax.random.split(inner, 7)
    block_span = TOK_DEV // 4
    block_total = SEQS * LEN // block_span
    slowness = jnp.exp(jax.random.uniform(first_key, (block_total, 1, CHAIN_WIDTH), jnp.float32, math.log(0.1), math.log(0.8)))
    jitter = jax.random.uniform(second_key, (block_total, block_span, CHAIN_WIDTH), jnp.float32, 0.5, 1.5)
    fast_share = 0.5
    fast_pick = jax.random.uniform(fifth_key, (CHAIN_WIDTH,), jnp.float32) < fast_share
    fast_rate = jnp.exp(jax.random.uniform(sixth_key, (CHAIN_WIDTH,), jnp.float32, math.log(0.012), math.log(0.035)))
    fast_boost = jnp.exp(jax.random.uniform(seventh_key, (block_total, 1, CHAIN_WIDTH), jnp.float32, math.log(0.6), math.log(1.6)))
    rate = slowness / LEN + jnp.where(fast_pick, fast_rate, 0.0)[None, None, :] * fast_boost
    steady = -(rate * jitter).reshape(SEQS, LEN, CHAIN_WIDTH)
    places = jax.random.randint(third_key, (SEQS, 4), 0, LEN)
    struck = jnp.any(jnp.arange(LEN)[None, :, None] == places[:, None, :], axis=2)
    depth = jax.random.uniform(fourth_key, (SEQS, LEN, CHAIN_WIDTH), jnp.float32, -0.7, -0.2)
    return steady + jnp.where(struck[:, :, None], depth, 0.0)


def steps_of(stream_key, extent, pieces, least, high):
    level, own = 1.0, jax.random.fold_in(stream_key, 6)
    for dim, shards_of in pieces:
        heights = jnp.exp(jax.random.uniform(jax.random.fold_in(own, dim), (shards_of,), jnp.float32, least / len(pieces), high / len(pieces)))
        level = level * jnp.repeat(heights, extent[dim] // shards_of).reshape([-1 if axis == dim else 1 for axis in range(len(extent))])
    return level


def scatter_about(stream_key, dims, width, reach, pieces=(), kind=jnp.bfloat16):
    array = width * jax.random.normal(stream_key, dims, jnp.float32)
    if pieces:
        array = array * steps_of(stream_key, dims, pieces, -0.22, 0.18)
    return jnp.clip(array, -reach, reach).astype(kind)


def setup_inputs(seed: int = 0) -> dict:
    seeds = jax.random.split(jax.random.key(seed), 15)
    return {
        "tokens": scatter_about(seeds[0], (SEQS, LEN, D), 1.0, 6.0, ((0, 4), (1, 8))),
        "norm_gain": jnp.clip(1.0 + 0.18 * jax.random.normal(seeds[1], (D,), jnp.float32), 0.1, 1.9),
        "chain_entry": scatter_about(seeds[2], (D, CHAIN_WIDTH), D ** -0.5, 0.125, ((0, 16), (1, 2))),
        "pool_entry": scatter_about(seeds[3], (D, POOL_WIDTH), D ** -0.5, 0.125, ((0, 16), (1, 2))),
        "conv_taps": scatter_about(seeds[4], (CONV_TAPS, CHAIN_WIDTH), CONV_TAPS ** -0.5, 3.0, ((1, 2),)),
        "recur_gate": scatter_about(seeds[5], (CHAIN_HEADS, HEAD, HEAD), HEAD ** -0.5, 0.375, ((0, 2),)),
        "input_gate": scatter_about(seeds[6], (CHAIN_HEADS, HEAD, HEAD), HEAD ** -0.5, 0.375, ((0, 2),)),
        "decay_log": draw_decay_log(jax.random.fold_in(seeds[14], 71), 0),
        "decay_shift": draw_decay_shift(jax.random.fold_in(seeds[14], 71), 0),
        "start_state": scatter_about(seeds[9], (SEQS, CHAIN_WIDTH), 1.0, 6.0, ((0, 4), (1, 2)), jnp.float32),
        "pool_mix": scatter_about(seeds[10], (POOL_GROUPS, HEAD, HEAD), HEAD ** -0.5, 0.375, ((0, 2),)),
        "pool_scale": jnp.clip(1.0 + 0.18 * jax.random.normal(seeds[11], (POOL_WIDTH,), jnp.float32), 0.1, 1.9),
        "chain_exit": scatter_about(seeds[12], (CHAIN_WIDTH, D), (CHAIN_WIDTH + POOL_WIDTH) ** -0.5, 0.09375, ((0, 2), (1, 16))),
        "pool_exit": scatter_about(seeds[13], (POOL_WIDTH, D), (CHAIN_WIDTH + POOL_WIDTH) ** -0.5, 0.09375, ((0, 2), (1, 16))),
    }


NORM_EPSILON = 1e-06
RECUR_SCALE = 8.0

def block_map(values, weight):
    row_total = values.shape[0]
    groups, block_width, _ = weight.shape
    blocks = values.astype(jnp.float32).reshape(row_total, groups, block_width)
    mapped = jnp.einsum('sgi,gij->sgj', blocks, weight.astype(jnp.float32))
    return mapped.reshape(row_total, groups * block_width)

def combine(earlier, latter):
    return (earlier[0] * latter[0], latter[0] * earlier[1] + latter[1])

def trailing(padded, row_total, window_id):
    sum_two = padded[1:] + padded[:-1]
    sum_four = sum_two[2:] + sum_two[:-2]
    sum_eight = sum_four[4:] + sum_four[:-4]
    sixteen = sum_eight[8:] + sum_eight[:-8]
    return jnp.where(window_id == 0, sum_two[-row_total:], jnp.where(window_id == 1, sum_four[-row_total:], jnp.where(window_id == 2, sum_eight[-row_total:], sixteen[-row_total:])))

def reference(tokens, norm_gain, chain_entry, pool_entry, conv_taps, recur_gate, input_gate, decay_log, decay_shift, start_state, pool_mix, pool_scale, chain_exit, pool_exit):
    channel = jnp.arange(POOL_WIDTH, dtype=jnp.int32) // HEAD
    window_id = (channel % 4)[None, :]
    window = jnp.power(2.0, (window_id + 1).astype(jnp.float32))
    position = jnp.arange(LEN, dtype=jnp.float32)[:, None]
    counts = jnp.minimum(position + 1.0, window)
    decay_rate = jnp.exp(decay_log) / LEN

    def one_sequence(inputs):
        values, shift_rows, begin_state = inputs
        widened = values.astype(jnp.float32)
        normed = (widened * lax.rsqrt(lax.optimization_barrier(jnp.mean(widened * widened, axis=-1, keepdims=True)) + NORM_EPSILON) * norm_gain.astype(jnp.float32)).astype(jnp.bfloat16)
        chain_input = jnp.dot(normed, chain_entry, preferred_element_type=jnp.float32).astype(jnp.bfloat16)
        pool_input = jnp.dot(normed, pool_entry, preferred_element_type=jnp.float32).astype(jnp.bfloat16)
        padded = jnp.pad(chain_input.astype(jnp.float32), ((CONV_TAPS - 1, 0), (0, 0)))
        conv_out = jnp.zeros((LEN, CHAIN_WIDTH), jnp.float32)
        for offset in range(CONV_TAPS):
            conv_out = conv_out + padded[offset:offset + LEN] * conv_taps[offset].astype(jnp.float32)
        conv_out = conv_out.astype(jnp.bfloat16)
        gate_recur = jax.nn.sigmoid(block_map(conv_out, recur_gate))
        gate_input = jax.nn.sigmoid(block_map(conv_out, input_gate))
        log_decay = -RECUR_SCALE * gate_recur * decay_rate + shift_rows
        decay_factor = jnp.exp(log_decay)
        drive_term = jnp.sqrt(-jnp.expm1(2.0 * log_decay)) * gate_input * conv_out.astype(jnp.float32)
        drive_term = drive_term.at[0].add(decay_factor[0] * begin_state)
        state = lax.associative_scan(combine, (decay_factor, drive_term), axis=0)[1]
        recurrent = state.astype(jnp.bfloat16)
        pool_pad = jnp.pad(pool_input.astype(jnp.float32), ((POOL_SPAN - 1, 0), (0, 0)))
        trail_sum = trailing(pool_pad, LEN, window_id)
        pool_diff = (trail_sum / counts - pool_input.astype(jnp.float32)).astype(jnp.bfloat16)
        pooled = (block_map(pool_diff, pool_mix) * pool_scale.astype(jnp.float32)).astype(jnp.bfloat16)
        mixed_rows = jnp.dot(recurrent, chain_exit, preferred_element_type=jnp.float32) + jnp.dot(pooled, pool_exit, preferred_element_type=jnp.float32)
        return mixed_rows.astype(jnp.bfloat16)
    return lax.map(one_sequence, (tokens, decay_shift, start_state))
```

```python
import functools

import jax
import jax.numpy as jnp
from jax import lax
from jax.experimental import pallas as pl
from jax.experimental.pallas import tpu as pltpu
from jax.sharding import PartitionSpec as P

MESH = pl.DeviceIdType.MESH
NORM_EPSILON = 1e-06
RECUR_SCALE = 8.0
HALO = 16
COLS = 256
ROWS = 64
ENTRY = (0, 1)
EXIT = (2, 3)
OWN, PEER = 0, 1
F32 = jnp.float32
BF16 = jnp.bfloat16


def neg_expm1(x):
    y = -x
    poly = 1.0 - y * (1.0 / 9.0)
    for k in range(8, 1, -1):
        poly = 1.0 - y * (1.0 / k) * poly
    return jnp.where(y < 0.5, y * poly, 1.0 - jnp.exp(x))


def nearest(n):
    order = [sorted(range(n), key=lambda z, s=s: (abs(z - s), (z - s) * (1 if 2 * s < n else -1)))
             for s in range(n)]
    return [sum(order[s][r] * n**s for s in range(n)) for r in range(n)]


def kernel(
    n, m,
    tokens, gain, chain_entry, pool_entry, taps, rgate, igate, dlog, shift_hbm, start,
    pmix, pscale, chain_exit, pool_exit,
    out,
    w0, w1, w2, w3, raw, normed, cacc, pacc, cbuf, pbuf, shift, wide, narrow, peer_shift,
    my_start, peer_start, rg, ig, pm,
    convb, zr, zi, cum_a, cum_b, rec, pooled, my_ab, all_ab, ent,
    acc, core_send, core_recv, x_send, x_recv,
    xs, xr, zs, zrv, ys, yr, loc, nsem_s, nsem_r, ssem_s, ssem_r, hsem_s, hsem_r, ab_s, ab_r,
    core_s, core_r, out_s, out_r,
):
    sp, fs, tp = lax.axis_index("sp"), lax.axis_index("fs"), lax.axis_index("tp")
    ny = m // 2
    x, y = fs % 2, fs // 2
    shards = (chain_entry, pool_entry, chain_exit, pool_exit)
    bufs = (w0, w1, w2, w3)
    seqs, half_rows, width = raw.shape
    rows = 2 * half_rows
    half = cbuf.shape[2]
    nb = half // COLS
    depth = chain_entry.shape[0]
    out_cols = 2 * chain_exit.shape[1]
    zdepth = m * depth

    codes = nearest(n)

    def digit(code):
        value = sp * 0
        for s in range(n):
            value = value + code // n**s % n * jnp.where(sp == s, 1, 0)
        return value

    ranks = [digit(code) for code in codes]
    x_peer = {"fs": y * 2 + 1 - x}
    core_peer = {"tp": 1 - tp}

    def y_peer(k):
        return {"fs": ((y + k) % ny) * 2 + x}

    barrier = pltpu.get_barrier_semaphore()
    greet = [{"sp": (sp + k) % n} for k in range(1, n)] + [core_peer, x_peer]
    greet += [y_peer(k) for k in range(1, ny)]
    for device in greet:
        pl.semaphore_signal(barrier, inc=1, device_id=device, device_id_type=MESH)

    started = []

    def launch(copy, cond=None):
        if cond is None:
            copy.start()
        else:
            pl.when(cond)(copy.start)
        started.append((copy, cond))

    def remote(src, dst, send, recv, device):
        return pltpu.make_async_remote_copy(
            src_ref=src, dst_ref=dst, send_sem=send, recv_sem=recv, device_id=device,
            device_id_type=MESH)

    def region(w, z, yy, xx):
        b = z * m + yy * 2 + xx
        if w in ENTRY:
            return bufs[w].at[pl.ds(pl.multiple_of(b * depth, depth), depth)]
        return bufs[w].at[b]

    def shard(w, h):
        at = pl.ds(pl.multiple_of(h * half, half), half)
        return shards[w].at[:, at] if w in ENTRY else shards[w].at[at]

    def cross(w):
        return remote(shard(w, 1 - x), region(w, sp, y, x), xs.at[w], xr.at[w], x_peer)

    def cross_wait(w):
        ref = region(w, sp, y, 1 - x)
        remote(ref, ref, xs.at[w], xr.at[w], x_peer).wait_recv()

    def z_copy(w, z, xx, way, src=None):
        ref = region(w, z, y, xx)
        at = (w * n + z) * 2 + xx
        return remote(ref if src is None else src, ref, zs.at[at * 2 + way], zrv.at[at],
                      {"sp": (sp + (1, n - 1)[way]) % n})

    def y_copy(w, z, xx, k, src=None):
        ref = region(w, z, y, xx)
        at = ((w * n + z) * 2 + xx) * ny + k
        return remote(ref if src is None else src, ref, ys.at[at], yr.at[at], y_peer(k))

    def y_wait(w, z, xx, k):
        ref = region(w, z, (y + ny - k) % ny, xx)
        at = ((w * n + z) * 2 + xx) * ny + k
        remote(ref, ref, ys.at[at], yr.at[at], y_peer(k)).wait_recv()

    def pass_on(w, r, xx, src=None):
        z = ranks[r]
        if n > 1:
            launch(z_copy(w, z, xx, 0, src), (z <= sp) & (sp < n - 1))
            launch(z_copy(w, z, xx, 1, src), (z >= sp) & (sp > 0))
        for k in range(1, ny):
            launch(y_copy(w, z, xx, k, src))

    def forward(kinds, r):
        for unit in (0, 1):
            xx = x if unit == 0 else 1 - x
            for w in kinds:
                if r == 0 and unit == 0:
                    pass_on(w, r, xx, shard(w, x))
                    continue
                if r == 0:
                    cross_wait(w)
                else:
                    z_copy(w, ranks[r], xx, 0).wait_recv()
                pass_on(w, r, xx)

    def arrived(kinds, r, k):
        if k:
            for w in kinds:
                for xx in (0, 1):
                    y_wait(w, ranks[r], xx, k)

    def lanes(c, base=0):
        return pl.ds(pl.multiple_of(base + c * COLS, COLS), COLS)

    mine_lanes = pl.ds(pl.multiple_of(x * half, half), half)
    peer_lanes = pl.ds(pl.multiple_of((1 - x) * half, half), half)
    heads = pl.ds(x * nb, nb)

    local = [
        pltpu.make_async_copy(tokens, raw, loc.at[0]),
        pltpu.make_async_copy(shift_hbm.at[:, :, peer_lanes], wide, loc.at[1]),
        pltpu.make_async_copy(shift_hbm.at[:, :, mine_lanes], shift, loc.at[2]),
        pltpu.make_async_copy(rgate.at[heads], rg, loc.at[3]),
        pltpu.make_async_copy(igate.at[heads], ig, loc.at[4]),
        pltpu.make_async_copy(pmix.at[heads], pm, loc.at[5]),
    ] + [pltpu.make_async_copy(shard(w, x), region(w, sp, y, x), loc.at[6 + w]) for w in range(4)]
    for copy in local:
        copy.start()
    my_start[...] = jnp.zeros(my_start.shape, F32)
    my_start[:seqs, :] = start[:, peer_lanes]

    pl.semaphore_wait(barrier, len(greet))
    for w in ENTRY:
        launch(cross(w))
    for w in ENTRY:
        pass_on(w, 0, x, shard(w, x))

    local[0].wait()

    def half_of(s, owner):
        return normed.at[s, pl.ds(pl.multiple_of(owner * half_rows, ROWS), half_rows)]

    def norm_x(s):
        return remote(half_of(s, tp), half_of(seqs + s, tp), nsem_s.at[s], nsem_r.at[s], x_peer)

    def norm_core(s):
        return remote(half_of(s, tp), half_of(s, tp), nsem_s.at[seqs + s], nsem_r.at[seqs + s],
                      core_peer)

    for s in range(seqs):
        def norm_step(i, c, s=s):
            r = pl.multiple_of(i * ROWS, ROWS)
            v = raw[s, pl.ds(r, ROWS), :].astype(F32)
            scale = lax.rsqrt(jnp.mean(v * v, axis=-1, keepdims=True) + NORM_EPSILON)
            normed[s, pl.ds(pl.multiple_of(tp * half_rows + r, ROWS), ROWS), :] = (
                v * scale * gain[...]).astype(BF16)
            return c

        lax.fori_loop(0, half_rows // ROWS, norm_step, 0)
        launch(norm_x(s))
        launch(norm_core(s))
    for w in EXIT:
        launch(cross(w))

    local[1].wait()

    def narrow_step(i, c):
        s, r = i // (rows // ROWS), pl.multiple_of((i % (rows // ROWS)) * ROWS, ROWS)
        narrow[s, pl.ds(r, ROWS), :] = wide[s, pl.ds(r, ROWS), :].astype(BF16)
        return c

    lax.fori_loop(0, seqs * (rows // ROWS), narrow_step, 0)
    shift_copy = remote(narrow, peer_shift, ssem_s.at[0], ssem_r.at[0], x_peer)
    start_copy = remote(my_start, peer_start, ssem_s.at[1], ssem_r.at[1], x_peer)
    launch(start_copy)
    launch(shift_copy)
    for copy in local[2:]:
        copy.wait()

    for w in ENTRY:
        cross_wait(w)
        pass_on(w, 0, 1 - x)

    def entry_part(s, r, last):
        at = pl.ds(pl.multiple_of(ranks[r] * zdepth, zdepth), zdepth)

        def step(j, c):
            b = lanes(j)
            v = normed[s, :, at]
            for w, total, dst in ((w0, cacc, cbuf), (w1, pacc, pbuf)):
                part = jnp.dot(v, w[at, b], preferred_element_type=F32)
                if r:
                    part = total[s, :, b] + part
                if last:
                    dst[s, HALO:, b] = part.astype(BF16)
                else:
                    total[s, :, b] = part
            return c

        lax.fori_loop(0, nb, step, 0)

    def core_wait(s):
        ref = half_of(s, 1 - tp)
        remote(ref, ref, nsem_s.at[seqs + s], nsem_r.at[seqs + s], core_peer).wait_recv()

    def relay(s):
        ref = half_of(seqs + s, tp)
        remote(ref, ref, nsem_s.at[s], nsem_r.at[s], x_peer).wait_recv()
        at = 2 * seqs + s
        launch(remote(ref, ref, nsem_s.at[at], nsem_r.at[at], core_peer))

    def relay_wait(s):
        ref = half_of(seqs + s, 1 - tp)
        at = 2 * seqs + s
        remote(ref, ref, nsem_s.at[at], nsem_r.at[at], core_peer).wait_recv()

    own = range(seqs)
    last = n - 1
    for r in range(1, n):
        forward(ENTRY, r)
        if r == 1:
            for s in own:
                core_wait(s)
        if r == last:
            forward(EXIT, 0)
        for k in range(1, ny):
            arrived(ENTRY, r - 1, k)
        for s in own:
            entry_part(s, r - 1, False)
    for s in own:
        relay(s)
        relay_wait(s)
        for r in range(last):
            entry_part(seqs + s, r, False)
    if n == 1:
        forward(EXIT, 0)
        for s in own:
            core_wait(s)
    for k in range(1, ny):
        arrived(ENTRY, last, k)

    def halo(pair, i):
        ref = (cbuf, pbuf)[i]
        at = pl.ds(pair * seqs, seqs)
        return remote(ref.at[at, pl.ds(rows, HALO)], ref.at[at, pl.ds(0, HALO)],
                      hsem_s.at[pair * 2 + i], hsem_r.at[pair * 2 + i], {"sp": (sp + 1) % n})

    for pair in (PEER, OWN):
        for s in own:
            entry_part(pair * seqs + s, last, True)
        for i in (0, 1):
            launch(halo(pair, i), sp < n - 1)
    if n > 1:
        forward(EXIT, 1)

    def halo_wait(pair):
        @pl.when(sp > 0)
        def _():
            halo(pair, 0).wait_recv()
            halo(pair, 1).wait_recv()

        @pl.when(sp == 0)
        def _():
            zero = jnp.zeros((seqs, HALO, half), BF16)
            cbuf[pair * seqs : (pair + 1) * seqs, :HALO, :] = zero
            pbuf[pair * seqs : (pair + 1) * seqs, :HALO, :] = zero

    tap_count = taps.shape[0]
    inverse_length = 1.0 / (rows * n)

    def chain(pair, s0):
        s = pair * seqs + s0

        def group(g, carry):
            b = lanes(g)
            whole = lanes(g, x * half)
            tap = taps[:, whole].astype(F32)

            def conv(i, c):
                r = pl.multiple_of(i * ROWS, ROWS)
                v = cbuf[s, pl.ds(r, ROWS + HALO), b].astype(F32)
                total = v * tap[tap_count - 1 : tap_count]
                for j in range(tap_count - 1):
                    total = total + pltpu.roll(v, tap_count - 1 - j, 0) * tap[j : j + 1]
                convb[pl.ds(r, ROWS), :] = total[HALO:].astype(BF16)
                return c

            lax.fori_loop(0, rows // ROWS, conv, 0)
            v = convb[...]
            zr[...] = jnp.dot(v, rg[g], preferred_element_type=F32)
            zi[...] = jnp.dot(v, ig[g], preferred_element_type=F32)
            rate = -RECUR_SCALE * (jnp.exp(dlog[:, whole]) * inverse_length)
            row = lax.broadcasted_iota(jnp.int32, (ROWS, COLS), 0)
            source = peer_shift if pair == PEER else shift

            def scan(i, ends):
                r = pl.multiple_of(i * ROWS, ROWS)
                at = pl.ds(r, ROWS)
                log_decay = (jax.nn.sigmoid(zr[at, :]) * rate
                             + source[s0, at, b].astype(F32))
                a = jnp.exp(log_decay)
                d = (jnp.sqrt(neg_expm1(2.0 * log_decay)) * jax.nn.sigmoid(zi[at, :])
                     * convb[at, :].astype(F32))
                k = 1
                while k < ROWS:
                    before = row >= k
                    d = d + a * jnp.where(before, pltpu.roll(d, k, 0), 0.0)
                    a = a * jnp.where(before, pltpu.roll(a, k, 0), 1.0)
                    k *= 2
                d = d + a * ends[1]
                a = a * ends[0]
                cum_a[s, at, b] = a
                cum_b[s, at, b] = d
                return a[ROWS - 1 :], d[ROWS - 1 :]

            end = lax.fori_loop(
                0, rows // ROWS, scan, (jnp.ones((1, COLS), F32), jnp.zeros((1, COLS), F32)))
            my_ab[pair, pl.ds(s0, 1), b] = end[0]
            my_ab[pair, pl.ds(seqs + s0, 1), b] = end[1]
            return carry

        lax.fori_loop(0, nb, group, 0)

    def ab_copy(pair, k):
        at = pair * n + k
        return remote(my_ab.at[pair], all_ab.at[at], ab_s.at[at], ab_r.at[at],
                      {"sp": (sp + k) % n})

    def ab_send(pair):
        for k in range(1, n):
            launch(ab_copy(pair, k), sp + k < n)

    def pool(pair):
        def group(g, window):
            b = lanes(g)

            def diff(i, c):
                s = pair * seqs + i // (rows // ROWS)
                r = pl.multiple_of((i % (rows // ROWS)) * ROWS, ROWS)
                v = pbuf[s, pl.ds(r, ROWS + HALO), b].astype(F32)
                total, k = v, 1
                while k < window:
                    total = total + pltpu.roll(total, k, 0)
                    k *= 2
                t = lax.broadcasted_iota(jnp.int32, (ROWS, COLS), 0) + (sp * rows + r + 1)
                count = jnp.minimum(t, window).astype(F32)
                pooled[s, pl.ds(r, ROWS), b] = (total[HALO:] / count - v[HALO:]).astype(BF16)
                return c

            lax.fori_loop(0, seqs * (rows // ROWS), diff, 0)
            for s0 in own:
                s = pair * seqs + s0
                p = jnp.dot(pooled[s, :, b], pm[g], preferred_element_type=F32)
                pooled[s, :, b] = (p * pscale[:, lanes(g, x * half)]).astype(BF16)

        for xx in (0, 1):
            @pl.when(x == xx)
            def _(xx=xx):
                for g in range(nb):
                    group(g, 2 ** (1 + (xx * nb + g) % 4))

    def fix(pair):
        if pair == OWN:
            entry_state = start[:, mine_lanes]
        else:
            remote(my_start, peer_start, ssem_s.at[1], ssem_r.at[1], x_peer).wait_recv()
            entry_state = peer_start[:seqs, :]
        ent[...] = entry_state
        for k in range(n - 1, 0, -1):
            @pl.when(sp >= k)
            def _(k=k):
                ab_copy(pair, k).wait_recv()
                at = pair * n + k
                ent[...] = all_ab[at, :seqs, :] * ent[...] + all_ab[at, seqs : 2 * seqs, :]

        for s0 in own:
            s = pair * seqs + s0

            def step(i, c, s=s, s0=s0):
                at = pl.ds(pl.multiple_of(i * ROWS, ROWS), ROWS)
                rec[s, at, :] = (
                    cum_a[s, at, :] * ent[s0 : s0 + 1, :] + cum_b[s, at, :]).astype(BF16)
                return c

            lax.fori_loop(0, rows // ROWS, step, 0)

    groups = sorted(((r, k) for r in range(n) for k in range(ny)),
                    key=lambda rk: rk[0] + 1.5 * rk[1])

    def partial(pair, owner, c):
        r, k = groups[c]
        b = ranks[r] * m + ((y + ny - k) % ny) * 2
        at = pl.ds(pl.multiple_of(owner * half_rows, ROWS), half_rows)
        which = slice(pair * seqs, (pair + 1) * seqs)
        u = rec[which, at, :].reshape(seqs * half_rows, half)
        v = pooled[which, at, :].reshape(seqs * half_rows, half)
        return jnp.dot(
            u, jnp.concatenate([w2[b], w2[b + 1]], axis=1), preferred_element_type=F32
        ) + jnp.dot(v, jnp.concatenate([w3[b], w3[b + 1]], axis=1), preferred_element_type=F32)

    count = len(groups)

    def core_copy(pair, c):
        at = pair * count + c
        return remote(core_send.at[at], core_recv.at[at], core_s.at[at], core_r.at[at], core_peer)

    def x_copy(c):
        return remote(x_send.at[c], x_recv.at[c], out_s.at[c], out_r.at[c], x_peer)

    def exit_dots(pair, c):
        at = pair * count + c
        core_send[at] = partial(pair, 1 - tp, c).astype(BF16)
        launch(core_copy(pair, c))
        acc[at] = partial(pair, tp, c)

    def exit_send(c):
        at = PEER * count + c
        core_copy(PEER, c).wait_recv()
        x_send[c] = (acc[at] + core_recv[at].astype(F32)).astype(BF16)
        launch(x_copy(c))

    def exit_out(c):
        r, k = groups[c]
        at = OWN * count + c
        core_copy(OWN, c).wait_recv()
        x_copy(c).wait_recv()
        total = acc[at] + core_recv[at].astype(F32) + x_recv[c].astype(F32)
        col = (ranks[r] * ny + (y + ny - k) % ny) * out_cols
        out[:, :, pl.ds(pl.multiple_of(col, out_cols), out_cols)] = (
            total.astype(BF16).reshape(seqs, half_rows, out_cols))

    halo_wait(PEER)
    remote(narrow, peer_shift, ssem_s.at[0], ssem_r.at[0], x_peer).wait_recv()
    for s0 in own:
        chain(PEER, s0)
    ab_send(PEER)
    if n > 2:
        forward(EXIT, 2)
    pool(PEER)
    for r in range(3, n):
        forward(EXIT, r)
    fix(PEER)

    done = []

    def peer_out(upto):
        for c in range(len(done), min(upto, count)):
            arrived(EXIT, *groups[c])
            exit_dots(PEER, c)
            done.append(c)
        for c in done:
            if c not in sent:
                exit_send(c)
                sent.append(c)

    sent = []
    peer_out(2)
    halo_wait(OWN)
    for s0 in own:
        chain(OWN, s0)
        peer_out(3 + s0)
    ab_send(OWN)
    pool(OWN)
    peer_out(len(done) + 1)
    fix(OWN)
    ready = 0
    while len(done) < count:
        peer_out(len(done) + 1)
        while ready < len(done):
            exit_dots(OWN, ready)
            ready += 1
    while ready < count:
        exit_dots(OWN, ready)
        ready += 1
    for c in range(count):
        exit_out(c)

    for copy, cond in started:
        if cond is None:
            copy.wait_send()
        else:
            pl.when(cond)(copy.wait_send)


def per_device(n, m, *args):
    (tokens, norm_gain, chain_entry, pool_entry, conv_taps, recur_gate, input_gate, decay_log,
     decay_shift, start_state, pool_mix, pool_scale, chain_exit, pool_exit) = args
    seqs, half_rows, width = tokens.shape
    rows, half = 2 * half_rows, chain_entry.shape[1] // 2
    nb = half // COLS
    ny = m // 2
    assert pool_mix.shape[0] % 4 == 0 and pool_mix.shape[1] == COLS and m % 2 == 0
    hbm, vmem = pl.BlockSpec(memory_space=pl.ANY), pl.BlockSpec(memory_space=pltpu.VMEM)
    dma = pltpu.SemaphoreType.DMA
    ab_rows = -(-2 * seqs // 8) * 8
    out_cols = 2 * chain_exit.shape[1]
    count = n * ny
    tile = (seqs * half_rows, out_cols)
    scratch = [pltpu.VMEM((width, half), BF16)] * 2 + [
        pltpu.VMEM((n * m, half, chain_exit.shape[1]), BF16)] * 2 + [
        pltpu.VMEM((seqs, half_rows, width), BF16),
        pltpu.VMEM((2 * seqs, rows, width), BF16),
        pltpu.VMEM((2 * seqs, rows, half), F32),
        pltpu.VMEM((2 * seqs, rows, half), F32),
        pltpu.VMEM((2 * seqs, HALO + rows, half), BF16),
        pltpu.VMEM((2 * seqs, HALO + rows, half), BF16),
        pltpu.VMEM((seqs, rows, half), F32),
        pltpu.VMEM((seqs, rows, half), F32),
        pltpu.VMEM((seqs, rows, half), BF16),
        pltpu.VMEM((seqs, rows, half), BF16),
        pltpu.VMEM((8, half), F32),
        pltpu.VMEM((8, half), F32),
        pltpu.VMEM((nb, COLS, COLS), BF16),
        pltpu.VMEM((nb, COLS, COLS), BF16),
        pltpu.VMEM((nb, COLS, COLS), BF16),
        pltpu.VMEM((rows, COLS), BF16),
        pltpu.VMEM((rows, COLS), F32),
        pltpu.VMEM((rows, COLS), F32),
        pltpu.VMEM((2 * seqs, rows, half), F32),
        pltpu.VMEM((2 * seqs, rows, half), F32),
        pltpu.VMEM((2 * seqs, rows, half), BF16),
        pltpu.VMEM((2 * seqs, rows, half), BF16),
        pltpu.VMEM((2, ab_rows, half), F32),
        pltpu.VMEM((2 * n, ab_rows, half), F32),
        pltpu.VMEM((seqs, half), F32),
        pltpu.VMEM((2 * count, *tile), F32),
        pltpu.VMEM((2 * count, *tile), BF16),
        pltpu.VMEM((2 * count, *tile), BF16),
        pltpu.VMEM((count, *tile), BF16),
        pltpu.VMEM((count, *tile), BF16),
        dma((4,)), dma((4,)), dma((16 * n,)), dma((8 * n,)), dma((8 * n * ny,)),
        dma((8 * n * ny,)), dma((10,)), dma((3 * seqs,)), dma((3 * seqs,)), dma((2,)), dma((2,)),
        dma((4,)), dma((4,)), dma((2 * n,)), dma((2 * n,)), dma((2 * count,)),
        dma((2 * count,)), dma((count,)), dma((count,)),
    ]
    return pl.pallas_call(
        functools.partial(kernel, n, m),
        name="layer",
        out_shape=jax.ShapeDtypeStruct(tokens.shape, BF16),
        in_specs=[hbm, vmem, hbm, hbm, vmem, hbm, hbm, vmem, hbm, vmem, hbm, vmem, hbm, hbm],
        out_specs=vmem,
        scratch_shapes=scratch,
        compiler_params=pltpu.CompilerParams(
            collective_id=0, has_side_effects=True, vmem_limit_bytes=63 * 1024 * 1024),
    )(tokens, norm_gain[None], chain_entry, pool_entry, conv_taps, recur_gate, input_gate,
      decay_log[None], decay_shift, start_state, pool_mix, pool_scale[None],
      chain_exit, pool_exit)


def ring_kernel(
    n, m,
    tokens, gain, chain_entry, pool_entry, taps, rgate, igate, dlog, shift_hbm, start,
    pmix, pscale, chain_exit, pool_exit,
    out,
    w0, w1, w2, w3, raw, normed, cbuf, pbuf, shift, rg, ig, pm,
    convb, zr, zi, cum_a, cum_b, rec, pooled, my_ab, all_ab, ent, acc, sendbuf, recvbuf,
    s1, r1, s2, r2, t1s, t1r, t2s, t2r, loc, nsem, hsem_s, hsem_r, ab_s, ab_r, out_s, out_r,
):
    sp, fs, tp = lax.axis_index("sp"), lax.axis_index("fs"), lax.axis_index("tp")
    shards = (chain_entry, pool_entry, chain_exit, pool_exit)
    bufs = (w0, w1, w2, w3)
    seqs, half_rows, width = raw.shape
    rows = 2 * half_rows
    chans = cbuf.shape[2]
    nb = chans // COLS
    far = m // 2
    full = (m - 1) // 2

    def ring(i):
        return i + (i // 2) * (5 - 2 * i) if m == 4 else i

    pos = ring(fs)
    right, left = ring((pos + 1) % m), ring((pos + m - 1) % m)

    barrier = pltpu.get_barrier_semaphore()
    greet = [{"sp": (sp + k) % n} for k in range(1, n)] + [{"tp": 1 - tp}]
    greet += [{"fs": ring((pos + k) % m)} for k in range(1, m)]
    for device in greet:
        pl.semaphore_signal(barrier, inc=1, device_id=device, device_id_type=MESH)

    def span(w, part):
        block = shards[w].shape[0]
        tail = block // 8 // 16 * 16
        head = block - tail
        cut = -(-head // 32) * 16
        if w % 2:
            cut = head - cut
        return {"all": (0, block), None: (0, head), 0: (0, cut), 1: (cut, head - cut),
                2: (head, tail)}[part]

    def region(w, p, q, part=None):
        lo, size = span(w, part)
        at = (((sp + p) % n) * m + ring((pos + q + m) % m)) * shards[w].shape[0] + lo
        return bufs[w].at[pl.ds(pl.multiple_of(at, 16), size)]

    def own(w, part=None):
        lo, size = span(w, part)
        return shards[w].at[pl.ds(lo, size)]

    has_tail = span(0, 2)[1] > 0 and m > 1

    started = []

    def launch(copy):
        copy.start()
        started.append(copy)

    def first(w, k):
        return pltpu.make_async_remote_copy(
            src_ref=own(w), dst_ref=region(w, 0, 0), send_sem=s1.at[w * n + k],
            recv_sem=r1.at[w * n + n - k], device_id={"sp": (sp + k) % n}, device_id_type=MESH)

    def first_wait(w, p):
        pltpu.make_async_remote_copy(
            src_ref=own(w), dst_ref=region(w, p, 0), send_sem=s1.at[w * n + p],
            recv_sem=r1.at[w * n + p], device_id={"sp": (sp + p) % n},
            device_id_type=MESH).wait_recv()

    def second(w, p, way, d):
        q = -d if way == 0 else d
        part = way if (m % 2 == 0 and d + 1 == far) else None
        if p == 0 and d == 0:
            src = own(w, part)
        else:
            src = region(w, p, q, part)
        at = ((w * n + p) * 2 + way) * max(far, 1) + d
        return pltpu.make_async_remote_copy(
            src_ref=src, dst_ref=region(w, p, q, part), send_sem=s2.at[at], recv_sem=r2.at[at],
            device_id={"fs": right if way == 0 else left}, device_id_type=MESH)

    def second_wait(w, p, way, d):
        q = -d if way == 0 else d
        part = way if (m % 2 == 0 and d == far) else None
        at = ((w * n + p) * 2 + way) * max(far, 1) + d - 1
        ref = region(w, p, q, part)
        pltpu.make_async_remote_copy(
            src_ref=ref, dst_ref=ref, send_sem=s2.at[at], recv_sem=r2.at[at],
            device_id={"fs": right if way == 0 else left}, device_id_type=MESH).wait_recv()

    def second_all(w, p):
        if far >= 1:
            for way in (0, 1):
                launch(second(w, p, way, 0))

    def forward(w, p):
        for d in range(1, far):
            for way in (0, 1):
                second_wait(w, p, way, d)
                launch(second(w, p, way, d))

    def last_wait(w, p):
        tail_wait(w, p)
        if far >= 1:
            for way in (0, 1):
                second_wait(w, p, way, far)

    def tail_one(w, k):
        return pltpu.make_async_remote_copy(
            src_ref=own(w, 2), dst_ref=region(w, 0, 0, 2), send_sem=t1s.at[w * m + k],
            recv_sem=t1r.at[w * m + m - k], device_id={"fs": ring((pos + k) % m)},
            device_id_type=MESH)

    def tail_one_wait(w, q):
        ref = region(w, 0, q, 2)
        pltpu.make_async_remote_copy(
            src_ref=ref, dst_ref=ref, send_sem=t1s.at[w * m + q], recv_sem=t1r.at[w * m + q],
            device_id={"fs": ring((pos + q) % m)}, device_id_type=MESH).wait_recv()

    def tail_two(w, q, k):
        at = (w * m + q) * n
        return pltpu.make_async_remote_copy(
            src_ref=own(w, 2) if q == 0 else region(w, 0, q, 2), dst_ref=region(w, 0, q, 2),
            send_sem=t2s.at[at + k], recv_sem=t2r.at[at + n - k],
            device_id={"sp": (sp + k) % n}, device_id_type=MESH)

    def tail_start(w):
        if has_tail:
            for k in range(1, m):
                launch(tail_one(w, k))

    def tail_forward(w):
        if has_tail:
            for q in range(m):
                if q:
                    tail_one_wait(w, q)
                for k in order:
                    launch(tail_two(w, q, k))

    def tail_wait(w, p):
        if has_tail and p:
            for q in range(m):
                ref = region(w, p, q, 2)
                at = (w * m + q) * n + p
                pltpu.make_async_remote_copy(
                    src_ref=ref, dst_ref=ref, send_sem=t2s.at[at], recv_sem=t2r.at[at],
                    device_id={"sp": (sp + p) % n}, device_id_type=MESH).wait_recv()

    order = sorted(range(1, n), key=lambda p: min(p, n - p))
    local = [
        pltpu.make_async_copy(tokens, raw, loc.at[0]),
        pltpu.make_async_copy(shift_hbm, shift, loc.at[1]),
        pltpu.make_async_copy(rgate, rg, loc.at[2]),
        pltpu.make_async_copy(igate, ig, loc.at[3]),
        pltpu.make_async_copy(pmix, pm, loc.at[4]),
    ] + [pltpu.make_async_copy(shards[w], region(w, 0, 0, "all"), loc.at[5 + w]) for w in range(4)]
    for copy in local:
        copy.start()

    pl.semaphore_wait(barrier, len(greet))
    for w in (0, 1):
        second_all(w, 0)
        for k in order:
            launch(first(w, k))
        tail_start(w)

    local[0].wait()
    mine = tp * half_rows

    def norm_step(i, c):
        s, r = i // (half_rows // ROWS), (i % (half_rows // ROWS)) * ROWS
        x = raw[s, pl.ds(pl.multiple_of(r, ROWS), ROWS), :].astype(F32)
        scale = lax.rsqrt(jnp.mean(x * x, axis=-1, keepdims=True) + NORM_EPSILON)
        normed[s, pl.ds(pl.multiple_of(mine + r, ROWS), ROWS), :] = (
            x * scale * gain[...]).astype(BF16)
        return c

    lax.fori_loop(0, seqs * (half_rows // ROWS), norm_step, 0)

    def normed_copy(owner):
        ref = normed.at[:, pl.ds(pl.multiple_of(owner * half_rows, ROWS), half_rows)]
        return pltpu.make_async_remote_copy(
            src_ref=ref, dst_ref=ref, send_sem=nsem.at[0], recv_sem=nsem.at[1],
            device_id={"tp": 1 - tp}, device_id_type=MESH)

    for p in order:
        for w in (0, 1):
            first_wait(w, p)
            second_all(w, p)
        if p == order[0]:
            launch(normed_copy(tp))
    for w in (0, 1):
        tail_forward(w)
    for w in (2, 3):
        for k in order:
            launch(first(w, k))
        tail_start(w)
    for p in [0] + order:
        for w in (0, 1):
            forward(w, p)
    for w in (2, 3):
        second_all(w, 0)
    for p in [0] + order:
        for w in (0, 1):
            last_wait(w, p)
    for p in order:
        for w in (2, 3):
            first_wait(w, p)
            second_all(w, p)
    for w in (2, 3):
        tail_forward(w)
    for copy in local[1:]:
        copy.wait()
    normed_copy(1 - tp).wait_recv()

    def lanes(c):
        return pl.ds(pl.multiple_of(c * COLS, COLS), COLS)

    def entry_step(i, c):
        s, b = i // nb, lanes(i % nb)
        x = normed[s]
        cbuf[s, HALO:, b] = jnp.dot(x, w0[:, b], preferred_element_type=F32).astype(BF16)
        pbuf[s, HALO:, b] = jnp.dot(x, w1[:, b], preferred_element_type=F32).astype(BF16)
        return c

    lax.fori_loop(0, seqs * nb, entry_step, 0)

    def halo(i, ref):
        return pltpu.make_async_remote_copy(
            src_ref=ref.at[:, rows:], dst_ref=ref.at[:, :HALO], send_sem=hsem_s.at[i],
            recv_sem=hsem_r.at[i], device_id={"sp": (sp + 1) % n}, device_id_type=MESH)

    todo = [(w, p) for p in [0] + order for w in (2, 3)]

    def some_forwards(count):
        for w, p in todo[:count]:
            forward(w, p)
        del todo[:count]

    some_forwards(2)

    @pl.when(sp < n - 1)
    def _():
        halo(0, cbuf).start()
        halo(1, pbuf).start()

    @pl.when(sp > 0)
    def _():
        halo(0, cbuf).wait_recv()
        halo(1, pbuf).wait_recv()

    @pl.when(sp == 0)
    def _():
        cbuf[:, :HALO, :] = jnp.zeros((seqs, HALO, chans), BF16)
        pbuf[:, :HALO, :] = jnp.zeros((seqs, HALO, chans), BF16)

    tap_count = taps.shape[0]
    inverse_length = 1.0 / (rows * n)

    def chain_step(g, s):
        b = lanes(g)
        tap = taps[:, b].astype(F32)

        def conv(i, c):
            r = pl.multiple_of(i * ROWS, ROWS)
            v = cbuf[s, pl.ds(r, ROWS + HALO), b].astype(F32)
            total = v * tap[tap_count - 1 : tap_count]
            for j in range(tap_count - 1):
                total = total + pltpu.roll(v, tap_count - 1 - j, 0) * tap[j : j + 1]
            convb[pl.ds(r, ROWS), :] = total[HALO:].astype(BF16)
            return c

        lax.fori_loop(0, rows // ROWS, conv, 0)
        x = convb[...]
        zr[...] = jnp.dot(x, rg[g], preferred_element_type=F32)
        zi[...] = jnp.dot(x, ig[g], preferred_element_type=F32)
        rate = -RECUR_SCALE * (jnp.exp(dlog[:, b]) * inverse_length)
        row = lax.broadcasted_iota(jnp.int32, (ROWS, COLS), 0)

        def scan(i, carry):
            r = pl.multiple_of(i * ROWS, ROWS)
            at = pl.ds(r, ROWS)
            log_decay = jax.nn.sigmoid(zr[at, :]) * rate + shift[s, at, b]
            a = jnp.exp(log_decay)
            d = (jnp.sqrt(neg_expm1(2.0 * log_decay)) * jax.nn.sigmoid(zi[at, :])
                 * convb[at, :].astype(F32))
            k = 1
            while k < ROWS:
                before = row >= k
                d = d + a * jnp.where(before, pltpu.roll(d, k, 0), 0.0)
                a = a * jnp.where(before, pltpu.roll(a, k, 0), 1.0)
                k *= 2
            d = d + a * carry[1]
            a = a * carry[0]
            cum_a[s, at, b] = a
            cum_b[s, at, b] = d
            return a[ROWS - 1 :], d[ROWS - 1 :]

        end = lax.fori_loop(
            0, rows // ROWS, scan, (jnp.ones((1, COLS), F32), jnp.zeros((1, COLS), F32)))
        my_ab[pl.ds(s, 1), b] = end[0]
        my_ab[pl.ds(seqs + s, 1), b] = end[1]

    for s in range(seqs):
        def chain_group(g, c, s=s):
            chain_step(g, s)
            return c

        for g0 in range(0, nb, 2):
            lax.fori_loop(g0, min(g0 + 2, nb), chain_group, 0)
            some_forwards(max(1, len(todo) // (2 * seqs)))

    def ab_copy(k):
        return pltpu.make_async_remote_copy(
            src_ref=my_ab, dst_ref=all_ab.at[k], send_sem=ab_s.at[k], recv_sem=ab_r.at[k],
            device_id={"sp": (sp + k) % n}, device_id_type=MESH)

    def pool_group(g):
        b = slice(g * COLS, (g + 1) * COLS)
        window = 2 ** (1 + g % 4)

        def diff(i, c):
            s, r = i // (rows // ROWS), pl.multiple_of((i % (rows // ROWS)) * ROWS, ROWS)
            v = pbuf[s, pl.ds(r, ROWS + HALO), b].astype(F32)
            total, k = v, 1
            while k < window:
                total = total + pltpu.roll(total, k, 0)
                k *= 2
            t = lax.broadcasted_iota(jnp.int32, (ROWS, COLS), 0) + (sp * rows + r + 1)
            count = jnp.minimum(t, window).astype(F32)
            convb_pool = total[HALO:] / count - v[HALO:]
            pooled[s, pl.ds(r, ROWS), b] = convb_pool.astype(BF16)
            return c

        lax.fori_loop(0, seqs * (rows // ROWS), diff, 0)
        for s in range(seqs):
            y = jnp.dot(pooled[s, :, b], pm[g], preferred_element_type=F32)
            pooled[s, :, b] = (y * pscale[:, b]).astype(BF16)

    pool_group(0)
    for k in range(1, n):
        @pl.when(sp + k < n)
        def _(k=k):
            ab_copy(k).start()

    for g in range(1, nb):
        pool_group(g)
        some_forwards(1)
    some_forwards(len(todo))

    ent[...] = start[...]
    for k in range(n - 1, 0, -1):
        @pl.when(sp >= k)
        def _(k=k):
            ab_copy(k).wait_recv()
            ent[...] = all_ab[k, :seqs, :] * ent[...] + all_ab[k, seqs : 2 * seqs, :]

    for s in range(seqs):
        def fix(i, c, s=s):
            at = pl.ds(pl.multiple_of(i * ROWS, ROWS), ROWS)
            rec[s, at, :] = (cum_a[s, at, :] * ent[s : s + 1, :] + cum_b[s, at, :]).astype(BF16)
            return c

        lax.fori_loop(0, rows // ROWS, fix, 0)

    dims = (((1,), (1,)), ((), ()))
    out_cols = sendbuf.shape[2]
    out_count = width // out_cols
    per_group = m * chain_exit.shape[0] // out_cols

    def out_lanes(j):
        return pl.ds(pl.multiple_of(j * out_cols, out_cols), out_cols)

    def partial(owner, j):
        at = pl.ds(pl.multiple_of(owner * half_rows, ROWS), half_rows)
        b = out_lanes(j)
        x = rec[:, at, :].reshape(seqs * half_rows, chans)
        y = pooled[:, at, :].reshape(seqs * half_rows, chans)
        return lax.dot_general(x, w2[b, :], dims, preferred_element_type=F32) + lax.dot_general(
            y, w3[b, :], dims, preferred_element_type=F32)

    def out_copy(j):
        return pltpu.make_async_remote_copy(
            src_ref=sendbuf.at[j], dst_ref=recvbuf.at[j], send_sem=out_s.at[j],
            recv_sem=out_r.at[j], device_id={"tp": 1 - tp}, device_id_type=MESH)

    def exit_step(j, c):
        sendbuf[j] = partial(1 - tp, j).astype(BF16)
        acc[j] = partial(tp, j)
        out_copy(j).start()
        return c

    def out_step(j, c):
        out_copy(j).wait_recv()
        total = (acc[j] + recvbuf[j].astype(F32)).astype(BF16)
        out[:, :, out_lanes(j)] = total.reshape(seqs, half_rows, out_cols)
        return c

    def group(p, step):
        j = ((sp + p) % n) * per_group
        lax.fori_loop(j, j + per_group, step, 0)

    before = None
    for p in [0] + order:
        for w in (2, 3):
            last_wait(w, p)
        group(p, exit_step)
        if before is not None:
            group(before, out_step)
        before = p
    group(before, out_step)

    def out_end(j, c):
        out_copy(j).wait_send()
        return c

    lax.fori_loop(0, out_count, out_end, 0)
    for copy in started:
        copy.wait_send()

    @pl.when(sp < n - 1)
    def _():
        halo(0, cbuf).wait_send()
        halo(1, pbuf).wait_send()

    for k in range(1, n):
        @pl.when(sp + k < n)
        def _(k=k):
            ab_copy(k).wait_send()


def ring_device(n, m, *args):
    (tokens, norm_gain, chain_entry, pool_entry, conv_taps, recur_gate, input_gate, decay_log,
     decay_shift, start_state, pool_mix, pool_scale, chain_exit, pool_exit) = args
    seqs, half_rows, width = tokens.shape
    rows, chans = 2 * half_rows, chain_entry.shape[1]
    nb = chans // COLS
    assert pool_mix.shape[0] % 4 == 0 and pool_mix.shape[1] == COLS
    far = max(m // 2, 1)
    hbm, vmem = pl.BlockSpec(memory_space=pl.ANY), pl.BlockSpec(memory_space=pltpu.VMEM)
    dma = pltpu.SemaphoreType.DMA
    ab_rows = -(-2 * seqs // 8) * 8
    out_cols = min(COLS, m * chain_exit.shape[1])
    out_count = width // out_cols
    scratch = [pltpu.VMEM((width, chans), BF16)] * 4 + [
        pltpu.VMEM((seqs, half_rows, width), BF16),
        pltpu.VMEM((seqs, rows, width), BF16),
        pltpu.VMEM((seqs, HALO + rows, chans), BF16),
        pltpu.VMEM((seqs, HALO + rows, chans), BF16),
        pltpu.VMEM((seqs, rows, chans), F32),
        pltpu.VMEM(recur_gate.shape, BF16),
        pltpu.VMEM(input_gate.shape, BF16),
        pltpu.VMEM(pool_mix.shape, BF16),
        pltpu.VMEM((rows, COLS), BF16),
        pltpu.VMEM((rows, COLS), F32),
        pltpu.VMEM((rows, COLS), F32),
        pltpu.VMEM((seqs, rows, chans), F32),
        pltpu.VMEM((seqs, rows, chans), F32),
        pltpu.VMEM((seqs, rows, chans), BF16),
        pltpu.VMEM((seqs, rows, chans), BF16),
        pltpu.VMEM((ab_rows, chans), F32),
        pltpu.VMEM((n, ab_rows, chans), F32),
        pltpu.VMEM((seqs, chans), F32),
        pltpu.VMEM((out_count, seqs * half_rows, out_cols), F32),
        pltpu.VMEM((out_count, seqs * half_rows, out_cols), BF16),
        pltpu.VMEM((out_count, seqs * half_rows, out_cols), BF16),
        dma((4 * n,)), dma((4 * n,)), dma((8 * n * far,)), dma((8 * n * far,)),
        dma((4 * m,)), dma((4 * m,)), dma((4 * m * n,)), dma((4 * m * n,)),
        dma((9,)), dma((2,)), dma((2,)), dma((2,)), dma((n,)), dma((n,)),
        dma((out_count,)), dma((out_count,)),
    ]
    return pl.pallas_call(
        functools.partial(ring_kernel, n, m),
        name="layer",
        out_shape=jax.ShapeDtypeStruct(tokens.shape, BF16),
        in_specs=[hbm, vmem, hbm, hbm, vmem, hbm, hbm, vmem, hbm, vmem, hbm, vmem, hbm, hbm],
        out_specs=vmem,
        scratch_shapes=scratch,
        compiler_params=pltpu.CompilerParams(
            collective_id=0, has_side_effects=True, vmem_limit_bytes=62 * 1024 * 1024),
    )(tokens, norm_gain[None], chain_entry, pool_entry, conv_taps, recur_gate, input_gate,
      decay_log[None], decay_shift, start_state, pool_mix, pool_scale[None],
      chain_exit.T, pool_exit.T)


def solution(mesh):
    in_specs = (
        P("fs", ("sp", "tp"), None),
        P(),
        P(("sp", "fs"), "tp"),
        P(("sp", "fs"), "tp"),
        P(None, "tp"),
        P("tp", None, None),
        P("tp", None, None),
        P("tp"),
        P("fs", "sp", "tp"),
        P("fs", "tp"),
        P("tp", None, None),
        P("tp"),
        P("tp", ("sp", "fs")),
        P("tp", ("sp", "fs")),
    )
    out_specs = P("fs", ("sp", "tp"), None)
    n, m = mesh.shape["sp"], mesh.shape["fs"]

    def layer(*args):
        wide = m % 2 == 0 and args[12].shape[1] % 128 == 0
        return (per_device if wide else ring_device)(n, m, *args)

    return jax.shard_map(
        layer, mesh=mesh, in_specs=in_specs, out_specs=out_specs, check_vma=False)
```

```python
import functools

import jax
import jax.numpy as jnp
from jax import lax
from jax.experimental import pallas as pl
from jax.experimental.pallas import tpu as pltpu
from jax.sharding import PartitionSpec as P

MESH = pl.DeviceIdType.MESH
NORM_EPSILON = 1e-06
RECUR_SCALE = 8.0
HALO = 16
COLS = 256
ROWS = 64
ENTRY = (0, 1)
EXIT = (2, 3)
OWN, PEER = 0, 1
TURN = 1
PEER_SLOTS = 4
F32 = jnp.float32
BF16 = jnp.bfloat16


def neg_expm1(x):
    y = -x
    poly = 1.0 - y * (1.0 / 9.0)
    for k in range(8, 1, -1):
        poly = 1.0 - y * (1.0 / k) * poly
    return jnp.where(y < 0.5, y * poly, 1.0 - jnp.exp(x))


def nearest(n):
    order = [sorted(range(n), key=lambda z, s=s: (abs(z - s), (z - s) * (-1 if 2 * s < n else 1)))
             for s in range(n)]
    return [sum(order[s][r] * n**s for s in range(n)) for r in range(n)]


def kernel(
    n, m,
    tokens, gain, chain_entry, pool_entry, taps, rgate, igate, dlog, shift_hbm, start,
    pmix, pscale, chain_exit, pool_exit,
    out,
    w0, w1, exits, raw, normed, cum_a, cum_b, cbuf, pbuf, shift, wide, narrow, peer_shift,
    my_start, peer_start, rg, ig, pm,
    convb, zr, zi, mix, my_ab, all_ab, ent,
    peer_acc, own_acc, core_send, core_recv, x_send, x_recv,
    xs, xr, zs, zrv, zts, ztr, ys, yr, loc, nsem_s, nsem_r, ssem_s, ssem_r, hsem_s, hsem_r,
    ab_s, ab_r, core_s, core_r, out_s, out_r,
):
    scope = jax.named_scope
    sp, fs, tp = lax.axis_index("sp"), lax.axis_index("fs"), lax.axis_index("tp")
    ny = m // 2
    x, y = fs % 2, fs // 2
    shards = (chain_entry, pool_entry, chain_exit, pool_exit)
    bufs = (w0, w1)
    seqs, half_rows, width = raw.shape
    rows = 2 * half_rows
    half = cbuf.shape[2]
    rec, pooled = mix.at[:, :, pl.ds(0, half)], mix.at[:, :, pl.ds(half, half)]
    nb = half // COLS
    depth = chain_entry.shape[0]
    cols = chain_exit.shape[1]
    zdepth = m * depth
    own = range(seqs)
    last = n - 1

    codes = nearest(n)

    def digit(code):
        value = sp * 0
        for s in range(n):
            value = value + code // n**s % n * jnp.where(sp == s, 1, 0)
        return value

    ranks = [digit(code) for code in codes]
    units = (x, 1 - x)
    x_peer = {"fs": y * 2 + 1 - x}
    core_peer = {"tp": 1 - tp}

    def y_peer(k):
        return {"fs": ((y + k) % ny) * 2 + x}

    def y_from(k):
        return (y + ny - k) % ny

    barrier = pltpu.get_barrier_semaphore()
    greet = [{"sp": (sp + k) % n} for k in range(1, n)] + [core_peer, x_peer]
    greet += [y_peer(k) for k in range(1, ny)]
    for device in greet:
        pl.semaphore_signal(barrier, inc=1, device_id=device, device_id_type=MESH)

    started = []

    def launch(copy, cond=None):
        if cond is None:
            copy.start()
        else:
            pl.when(cond)(copy.start)
        started.append((copy, cond))

    def remote(src, dst, send, recv, device):
        return pltpu.make_async_remote_copy(
            src_ref=src, dst_ref=dst, send_sem=send, recv_sem=recv, device_id=device,
            device_id_type=MESH)

    def region(w, z, yy, xx):
        if w in ENTRY:
            b = z * m + yy * 2 + xx
            return bufs[w].at[pl.ds(pl.multiple_of(b * depth, depth), depth)]
        at = pl.ds((w - EXIT[0]) * half, half)
        return exits.at[z * 2 + xx, at, pl.ds(pl.multiple_of(yy * cols, cols), cols)]

    def shard(w, h):
        at = pl.ds(pl.multiple_of(h * half, half), half)
        return shards[w].at[:, at] if w in ENTRY else shards[w].at[at]

    def cross(w):
        return remote(shard(w, 1 - x), region(w, sp, y, x), xs.at[w], xr.at[w], x_peer)

    def cross_wait(w):
        ref = region(w, sp, y, 1 - x)
        remote(ref, ref, xs.at[w], xr.at[w], x_peer).wait_recv()

    def z_peer(way):
        return {"sp": (sp + (1, n - 1)[way]) % n}

    def z_copy(w, z, xx, way, src=None):
        ref = region(w, z, y, xx)
        at = (w * n + z) * 2 + xx
        return remote(ref if src is None else src, ref, zs.at[at * 2 + way], zrv.at[at],
                      z_peer(way))

    def z_turn(z, k, way):
        ref = region(TURN, z, y_from(k), x)
        at = z * ny + k
        return remote(ref, ref, zts.at[at * 2 + way], ztr.at[at], z_peer(way))

    def y_copy(w, z, xx, k, src=None):
        ref = region(w, z, y, xx)
        at = ((w * n + z) * 2 + xx) * ny + k
        return remote(ref if src is None else src, ref, ys.at[at], yr.at[at], y_peer(k))

    def y_wait(w, z, xx, k):
        ref = region(w, z, y_from(k), xx)
        at = ((w * n + z) * 2 + xx) * ny + k
        remote(ref, ref, ys.at[at], yr.at[at], y_peer(k)).wait_recv()

    def source(w, unit):
        return shard(w, x) if unit == 0 else None

    def z_send(w, unit):
        if n > 1:
            launch(z_copy(w, sp, units[unit], 0, source(w, unit)), sp + 1 < n)
            launch(z_copy(w, sp, units[unit], 1, source(w, unit)), sp > 0)

    def exit_z_send(early):
        toward = [sp + 2 == n, sp == 1]
        for w in EXIT:
            if n > 1:
                for way, inside in ((0, sp + 1 < n), (1, sp > 0)):
                    edge_link = toward[way] if n > 2 else sp < 0
                    cond = inside & ((edge_link == False) if early else edge_link)
                    launch(z_copy(w, sp, x, way, shard(w, x)), cond)

    def turn_send():
        for k in range(1, ny):
            if n > 1:
                launch(z_turn(sp, k, 0), sp + 1 < n)
                launch(z_turn(sp, k, 1), sp > 0)

    def y_send(w, unit):
        for k in range(1, ny):
            launch(y_copy(w, sp, units[unit], k, source(w, unit)))

    def both(cond, other):
        return other if cond is None else cond & other

    def relay_on(z, make, cond):
        if n > 2:
            launch(make(0), both(cond, (z < sp) & (sp + 1 < n)))
            launch(make(1), both(cond, (z > sp) & (sp > 0)))

    def wait_if(make, cond):
        if cond is None:
            make().wait_recv()
        else:
            pl.when(cond)(lambda: make().wait_recv())

    def forward(w, r, unit, cond=None):
        z, xx = ranks[r], units[unit]
        wait_if(lambda: z_copy(w, z, xx, 0), cond)
        relay_on(z, lambda way: z_copy(w, z, xx, way), cond)
        if (w, unit) != (TURN, 0):
            for k in range(1, ny):
                launch(y_copy(w, z, xx, k), cond)

    def turn_forward(r, cond=None):
        z = ranks[r]
        for k in range(1, ny):
            wait_if(lambda k=k: z_turn(z, k, 0), cond)
            relay_on(z, lambda way, k=k: z_turn(z, k, way), cond)

    edge = (sp == 0) | (sp == n - 1)
    inner = (sp > 0) & (sp < n - 1)

    def entry_forward(r, cond=None, part=None):
        todo = [(0, 0), (1, 0), (0, 1), (1, 1)]
        todo = todo if part is None else (todo[:3], todo[3:])[part]
        with scope(f"efwd#r={r}"):
            for w, unit in todo:
                forward(w, r, unit, cond)
            if part != 0:
                turn_forward(r, cond)

    def entry_arrived(r):
        for k in range(1, ny):
            for w in ENTRY:
                for unit in (0, 1):
                    if (w, unit) != (TURN, 0):
                        y_wait(w, ranks[r], units[unit], k)

    def exit_arrived(r, unit):
        for k in range(1, ny):
            for w in EXIT:
                y_wait(w, ranks[r], units[unit], k)

    def exit_forward(r, unit, cond=None):
        with scope(f"xfwd#r={r}#u={unit}"):
            for w in EXIT:
                if r:
                    forward(w, r, unit, cond)
                else:
                    cross_wait(w)
                    z_send(w, unit)
                    y_send(w, unit)

    def lanes(c, base=0):
        return pl.ds(pl.multiple_of(base + c * COLS, COLS), COLS)

    mine_lanes = pl.ds(pl.multiple_of(x * half, half), half)
    peer_lanes = pl.ds(pl.multiple_of((1 - x) * half, half), half)
    heads = pl.ds(x * nb, nb)

    local = [
        pltpu.make_async_copy(tokens, raw, loc.at[0]),
        pltpu.make_async_copy(shift_hbm.at[:, :, peer_lanes], wide, loc.at[1]),
        pltpu.make_async_copy(shift_hbm.at[:, :, mine_lanes], shift, loc.at[2]),
        pltpu.make_async_copy(rgate.at[heads], rg, loc.at[3]),
        pltpu.make_async_copy(igate.at[heads], ig, loc.at[4]),
        pltpu.make_async_copy(pmix.at[heads], pm, loc.at[5]),
    ] + [pltpu.make_async_copy(shard(w, x), region(w, sp, y, x), loc.at[6 + w]) for w in range(4)]
    for copy in local:
        copy.start()
    my_start[...] = jnp.zeros(my_start.shape, F32)
    my_start[:seqs, :] = start[:, peer_lanes]

    with scope("entry_barrier"):
        pl.semaphore_wait(barrier, len(greet))
    for w in ENTRY:
        launch(cross(w))
    for w in ENTRY:
        z_send(w, 0)
        y_send(w, 0)

    local[0].wait()

    def half_of(s, owner):
        return normed.at[s, pl.ds(pl.multiple_of(owner * half_rows, ROWS), half_rows)]

    def norm_x(s):
        return remote(half_of(s, tp), half_of(seqs + s, tp), nsem_s.at[s], nsem_r.at[s], x_peer)

    def norm_core(s):
        return remote(half_of(s, tp), half_of(s, tp), nsem_s.at[seqs + s], nsem_r.at[seqs + s],
                      core_peer)

    for s in own:
        def norm_step(i, c, s=s):
            r = pl.multiple_of(i * ROWS, ROWS)
            v = raw[s, pl.ds(r, ROWS), :].astype(F32)
            scale = lax.rsqrt(jnp.mean(v * v, axis=-1, keepdims=True) + NORM_EPSILON)
            normed[s, pl.ds(pl.multiple_of(tp * half_rows + r, ROWS), ROWS), :] = (
                v * scale * gain[...]).astype(BF16)
            return c

        lax.fori_loop(0, half_rows // ROWS, norm_step, 0)

    local[1].wait()

    def narrow_step(i, c):
        s, r = i // (rows // ROWS), pl.multiple_of((i % (rows // ROWS)) * ROWS, ROWS)
        narrow[s, pl.ds(r, ROWS), :] = wide[s, pl.ds(r, ROWS), :].astype(BF16)
        return c

    lax.fori_loop(0, seqs * (rows // ROWS), narrow_step, 0)
    for copy in local[2:]:
        copy.wait()
    start_copy = remote(my_start, peer_start, ssem_s.at[seqs], ssem_r.at[seqs], x_peer)

    def shift_copy(s):
        return remote(narrow.at[s], peer_shift.at[s], ssem_s.at[s], ssem_r.at[s], x_peer)

    for s in own:
        launch(norm_core(s))
    with scope("cross_fwd"):
        for w in ENTRY:
            cross_wait(w)
            z_send(w, 1)
            y_send(w, 1)
    launch(norm_x(0))
    launch(start_copy)
    for w in EXIT:
        y_send(w, 0)
    with scope("turn_fwd"):
        for k in range(1, ny):
            y_wait(TURN, sp, x, k)
        turn_send()

    def entry_part(s, r):
        at = pl.ds(pl.multiple_of(ranks[r] * zdepth, zdepth), zdepth)

        def step(j, c):
            b = lanes(j)
            v = normed[s, :, at]
            for w, total, dst in ((w0, cum_a, cbuf), (w1, cum_b, pbuf)):
                part = jnp.dot(v, w[at, b], preferred_element_type=F32)
                if r:
                    part = total[s, :, b] + part
                if r == last:
                    dst[s, HALO:, b] = part.astype(BF16)
                else:
                    total[s, :, b] = part
            return c

        lax.fori_loop(0, nb, step, 0)

    def core_wait(s):
        ref = half_of(s, 1 - tp)
        remote(ref, ref, nsem_s.at[seqs + s], nsem_r.at[seqs + s], core_peer).wait_recv()

    def relay(s):
        ref = half_of(seqs + s, tp)
        remote(ref, ref, nsem_s.at[s], nsem_r.at[s], x_peer).wait_recv()
        at = 2 * seqs + s
        launch(remote(ref, ref, nsem_s.at[at], nsem_r.at[at], core_peer))

    def relay_wait(s):
        ref = half_of(seqs + s, 1 - tp)
        at = 2 * seqs + s
        remote(ref, ref, nsem_s.at[at], nsem_r.at[at], core_peer).wait_recv()

    def entry_parts(seqs_of, r):
        with scope(f"edot#r={r}"):
            for s in seqs_of:
                entry_part(s, r)

    def entry_ready(r):
        with scope(f"earr#r={r}"):
            entry_arrived(r)

    peer = range(seqs, 2 * seqs)
    for r in range(1, last):
        entry_forward(r)
        if r == 1:
            for s in own:
                core_wait(s)
        entry_ready(r - 1)
        entry_parts(own, r - 1)
        if r == 1:
            for s in own[1:]:
                launch(norm_x(s))
            exit_z_send(True)
    if n > 1:
        entry_forward(last, inner)
    if n < 3:
        for s in own:
            core_wait(s)
        for s in own[1:]:
            launch(norm_x(s))
        exit_z_send(True)
    with scope("relay#s=0"):
        relay(0)
        relay_wait(0)
    for r in range(last - 1):
        entry_parts([seqs], r)
    if n > 1:
        entry_forward(last, edge, 0)
        entry_ready(last - 1)
        entry_parts(range(seqs + 1), last - 1)
    with scope("relay#s=1"):
        for s in own[1:]:
            relay(s)
    launch(shift_copy(0))
    for w in EXIT:
        launch(cross(w))
    if n > 1:
        entry_forward(last, edge, 1)
    with scope("relay_wait#s=1"):
        for s in own[1:]:
            relay_wait(s)
    for r in range(last):
        entry_parts(range(seqs + 1, 2 * seqs), r)
    exit_z_send(False)
    with scope("earr_last"):
        entry_arrived(last)

    def halo(pair, i):
        ref = (cbuf, pbuf)[i]
        at = pl.ds(pair * seqs, seqs)
        return remote(ref.at[at, pl.ds(rows, HALO)], ref.at[at, pl.ds(0, HALO)],
                      hsem_s.at[pair * 2 + i], hsem_r.at[pair * 2 + i], {"sp": (sp + 1) % n})

    for pair in (PEER, OWN):
        for s in own:
            entry_part(pair * seqs + s, last)
        for i in (0, 1):
            launch(halo(pair, i), sp < n - 1)
    for s in own[1:]:
        launch(shift_copy(s))
    for r in range(1, min(2, n)):
        exit_forward(r, 0)
    if n > 2:
        exit_forward(2, 0, inner)

    def halo_wait(pair):
        @pl.when(sp > 0)
        def _():
            halo(pair, 0).wait_recv()
            halo(pair, 1).wait_recv()

        @pl.when(sp == 0)
        def _():
            zero = jnp.zeros((seqs, HALO, half), BF16)
            cbuf[pair * seqs : (pair + 1) * seqs, :HALO, :] = zero
            pbuf[pair * seqs : (pair + 1) * seqs, :HALO, :] = zero

    tap_count = taps.shape[0]
    inverse_length = 1.0 / (rows * n)

    def chain(pair, s0):
        s = pair * seqs + s0

        def group(g, carry):
            b = lanes(g)
            whole = lanes(g, x * half)
            tap = taps[:, whole].astype(F32)

            def conv(i, c):
                r = pl.multiple_of(i * ROWS, ROWS)
                v = cbuf[s, pl.ds(r, ROWS + HALO), b].astype(F32)
                total = v * tap[tap_count - 1 : tap_count]
                for j in range(tap_count - 1):
                    total = total + pltpu.roll(v, tap_count - 1 - j, 0) * tap[j : j + 1]
                convb[pl.ds(r, ROWS), :] = total[HALO:].astype(BF16)
                return c

            lax.fori_loop(0, rows // ROWS, conv, 0)
            v = convb[...]
            zr[...] = jnp.dot(v, rg[g], preferred_element_type=F32)
            zi[...] = jnp.dot(v, ig[g], preferred_element_type=F32)
            rate = -RECUR_SCALE * (jnp.exp(dlog[:, whole]) * inverse_length)
            row = lax.broadcasted_iota(jnp.int32, (ROWS, COLS), 0)
            source = peer_shift if pair == PEER else shift

            def scan(i, ends):
                r = pl.multiple_of(i * ROWS, ROWS)
                at = pl.ds(r, ROWS)
                log_decay = (jax.nn.sigmoid(zr[at, :]) * rate
                             + source[s0, at, b].astype(F32))
                a = jnp.exp(log_decay)
                d = (jnp.sqrt(neg_expm1(2.0 * log_decay)) * jax.nn.sigmoid(zi[at, :])
                     * convb[at, :].astype(F32))
                k = 1
                while k < ROWS:
                    before = row >= k
                    d = d + a * jnp.where(before, pltpu.roll(d, k, 0), 0.0)
                    a = a * jnp.where(before, pltpu.roll(a, k, 0), 1.0)
                    k *= 2
                d = d + a * ends[1]
                a = a * ends[0]
                cum_a[s, at, b] = a
                cum_b[s, at, b] = d
                return a[ROWS - 1 :], d[ROWS - 1 :]

            end = lax.fori_loop(
                0, rows // ROWS, scan, (jnp.ones((1, COLS), F32), jnp.zeros((1, COLS), F32)))
            my_ab[s, pl.ds(0, 1), b] = end[0]
            my_ab[s, pl.ds(1, 1), b] = end[1]
            return carry

        with scope(f"chain#p={pair}#s={s0}"):
            lax.fori_loop(0, nb, group, 0)
        for k in range(1, n):
            launch(ab_copy(s, k), sp + k < n)

    def ab_copy(s, k):
        at = s * n + k
        return remote(my_ab.at[s], all_ab.at[at], ab_s.at[at], ab_r.at[at], {"sp": (sp + k) % n})

    def pool(pair):
        def group(g, window):
            b = lanes(g)

            def diff(i, c):
                s = pair * seqs + i // (rows // ROWS)
                r = pl.multiple_of((i % (rows // ROWS)) * ROWS, ROWS)
                v = pbuf[s, pl.ds(r, ROWS + HALO), b].astype(F32)
                total, k = v, 1
                while k < window:
                    total = total + pltpu.roll(total, k, 0)
                    k *= 2
                t = lax.broadcasted_iota(jnp.int32, (ROWS, COLS), 0) + (sp * rows + r + 1)
                count = jnp.minimum(t, window).astype(F32)
                pooled[s, pl.ds(r, ROWS), b] = (total[HALO:] / count - v[HALO:]).astype(BF16)
                return c

            lax.fori_loop(0, seqs * (rows // ROWS), diff, 0)
            for s0 in own:
                s = pair * seqs + s0
                p = jnp.dot(pooled[s, :, b], pm[g], preferred_element_type=F32)
                pooled[s, :, b] = (p * pscale[:, lanes(g, x * half)]).astype(BF16)

        with scope(f"pool#p={pair}"):
            for xx in (0, 1):
                @pl.when(x == xx)
                def _(xx=xx):
                    for g in range(nb):
                        group(g, 2 ** (1 + (xx * nb + g) % 4))

    def fix(pair, s0):
        s = pair * seqs + s0
        with scope(f"fix#p={pair}#s={s0}"):
            if pair == OWN:
                ent[s : s + 1, :] = start[s0 : s0 + 1, mine_lanes]
            else:
                ent[s : s + 1, :] = peer_start[s0 : s0 + 1, :]
            for k in range(n - 1, 0, -1):
                @pl.when(sp >= k)
                def _(k=k):
                    ab_copy(s, k).wait_recv()
                    at = s * n + k
                    ent[s : s + 1, :] = all_ab[at, 0:1, :] * ent[s : s + 1, :] + all_ab[at, 1:2, :]

            def step(i, c):
                at = pl.ds(pl.multiple_of(i * ROWS, ROWS), ROWS)
                rec[s, at, :] = (
                    cum_a[s, at, :] * ent[s : s + 1, :] + cum_b[s, at, :]).astype(BF16)
                return c

            lax.fori_loop(0, rows // ROWS, step, 0)

    groups = [(unit, r) for unit in (0, 1) for r in range(n)]
    count = len(groups)

    def core_copy(at):
        return remote(core_send.at[at], core_recv.at[at], core_s.at[at], core_r.at[at], core_peer)

    def x_copy(s0, c):
        at = c * seqs + s0
        return remote(x_send.at[at], x_recv.at[at], out_s.at[at], out_r.at[at], x_peer)

    def owner_rows(owner):
        return pl.ds(pl.multiple_of(owner * half_rows, ROWS), half_rows)

    def dots(pair, s0, c):
        unit, r = groups[c]
        s = pair * seqs + s0
        b = ranks[r] * 2 + units[unit]
        at = (pair * count + c) * seqs + s0
        total = peer_acc.at[(c * seqs + s0) % PEER_SLOTS] if pair else own_acc.at[c * seqs + s0]
        with scope(f"dots#p={pair}#s={s0}#c={c}"):
            total[...] = jnp.dot(mix[s], exits[b], preferred_element_type=F32)
            core_send[at] = total[owner_rows(1 - tp), :].astype(BF16)
        launch(core_copy(at))

    def peer_send(s0, c):
        at = (PEER * count + c) * seqs + s0
        with scope(f"send#s={s0}#c={c}"):
            core_copy(at).wait_recv()
            x_send[c * seqs + s0] = (
                peer_acc[(c * seqs + s0) % PEER_SLOTS, owner_rows(tp), :]
                + core_recv[at].astype(F32)).astype(BF16)
        launch(x_copy(s0, c))

    def own_out(s0, c):
        unit, r = groups[c]
        at = (OWN * count + c) * seqs + s0
        other = groups.index((1 - unit, r))
        with scope(f"out#s={s0}#c={c}"):
            core_copy(at).wait_recv()
            x_copy(s0, other).wait_recv()
            total = (own_acc[c * seqs + s0, owner_rows(tp), :] + core_recv[at].astype(F32)
                     + x_recv[other * seqs + s0].astype(F32)).astype(BF16)
            for yy in range(ny):
                col = (ranks[r] * m + yy * 2 + units[unit]) * cols
                out[s0, :, pl.ds(pl.multiple_of(col, cols), cols)] = (
                    total[:, yy * cols : (yy + 1) * cols])

    waiting = []

    def peer_step(s0, c, arrive=True):
        if arrive:
            with scope(f"xarr#c={c}"):
                exit_arrived(groups[c][1], groups[c][0])
        dots(PEER, s0, c)
        flush()
        waiting.append((s0, c))

    def flush():
        while waiting:
            peer_send(*waiting.pop())

    first = list(range(n))
    second = list(range(n, 2 * n))
    later = own[1:]

    def forwards(r, unit, cond):
        for rr in range(r, n if r == 3 else min(r + 1, n)):
            exit_forward(rr, unit, cond)

    with scope("halo_p"):
        halo_wait(PEER)
    forwards(3, 0, inner)
    pool(PEER)
    with scope("shift_wait#s=0"):
        shift_copy(0).wait_recv()
    chain(PEER, 0)
    forwards(2, 0, edge)
    exit_forward(0, 1)
    with scope("start_wait"):
        start_copy.wait_recv()
    fix(PEER, 0)
    for c in first[:2]:
        peer_step(0, c)
    flush()
    forwards(3, 0, edge)
    with scope("halo_o"):
        halo_wait(OWN)
    chain(OWN, 0)
    for c in first[2:3]:
        peer_step(0, c)
    for s0 in later:
        with scope(f"shift_wait#s={s0}"):
            shift_copy(s0).wait_recv()
        chain(PEER, s0)
    forwards(1, 1, None)
    forwards(2, 1, inner)
    for c in first[3:]:
        peer_step(0, c)
    forwards(3, 1, inner)
    for s0 in later:
        fix(PEER, s0)
        for c in first[:2]:
            peer_step(s0, c, False)
    forwards(2, 1, edge)
    for s0 in later:
        for c in first[2:]:
            peer_step(s0, c, False)
    for s0 in own:
        peer_step(s0, second[0], s0 == 0)
    flush()
    for s0 in later:
        chain(OWN, s0)
    forwards(3, 1, edge)
    for c in second[1:2]:
        for s0 in own:
            peer_step(s0, c, s0 == 0)
    flush()
    pool(OWN)
    for s0 in own:
        fix(OWN, s0)
    for c in first:
        for s0 in own:
            dots(OWN, s0, c)
    for c in second[2:3]:
        for s0 in own:
            peer_step(s0, c, s0 == 0)
    flush()
    for c in second[:2]:
        for s0 in own:
            dots(OWN, s0, c)
    for c in second[3:]:
        for s0 in own:
            peer_step(s0, c, s0 == 0)
    flush()
    for c in second[2:]:
        for s0 in own:
            dots(OWN, s0, c)
    for c in second + first:
        for s0 in own:
            own_out(s0, c)

    with scope("drain"):
        for copy, cond in started:
            if cond is None:
                copy.wait_send()
            else:
                pl.when(cond)(copy.wait_send)


def per_device(n, m, *args):
    (tokens, norm_gain, chain_entry, pool_entry, conv_taps, recur_gate, input_gate, decay_log,
     decay_shift, start_state, pool_mix, pool_scale, chain_exit, pool_exit) = args
    seqs, half_rows, width = tokens.shape
    rows, half = 2 * half_rows, chain_entry.shape[1] // 2
    nb = half // COLS
    ny = m // 2
    assert pool_mix.shape[0] % 4 == 0 and pool_mix.shape[1] == COLS
    hbm, vmem = pl.BlockSpec(memory_space=pl.ANY), pl.BlockSpec(memory_space=pltpu.VMEM)
    dma = pltpu.SemaphoreType.DMA
    cols = ny * chain_exit.shape[1]
    count = 2 * n
    total = (rows, cols)
    tile = (half_rows, cols)
    scratch = [pltpu.VMEM((width, half), BF16)] * 2 + [
        pltpu.VMEM((2 * n, 2 * half, cols), BF16),
        pltpu.VMEM((seqs, half_rows, width), BF16),
        pltpu.VMEM((2 * seqs, rows, width), BF16),
        pltpu.VMEM((2 * seqs, rows, half), F32),
        pltpu.VMEM((2 * seqs, rows, half), F32),
        pltpu.VMEM((2 * seqs, HALO + rows, half), BF16),
        pltpu.VMEM((2 * seqs, HALO + rows, half), BF16),
        pltpu.VMEM((seqs, rows, half), F32),
        pltpu.VMEM((seqs, rows, half), F32),
        pltpu.VMEM((seqs, rows, half), BF16),
        pltpu.VMEM((seqs, rows, half), BF16),
        pltpu.VMEM((8, half), F32),
        pltpu.VMEM((8, half), F32),
        pltpu.VMEM((nb, COLS, COLS), BF16),
        pltpu.VMEM((nb, COLS, COLS), BF16),
        pltpu.VMEM((nb, COLS, COLS), BF16),
        pltpu.VMEM((rows, COLS), BF16),
        pltpu.VMEM((rows, COLS), F32),
        pltpu.VMEM((rows, COLS), F32),
        pltpu.VMEM((2 * seqs, rows, 2 * half), BF16),
        pltpu.VMEM((2 * seqs, 8, half), F32),
        pltpu.VMEM((2 * seqs * n, 8, half), F32),
        pltpu.VMEM((2 * seqs, half), F32),
        pltpu.VMEM((PEER_SLOTS, *total), F32),
        pltpu.VMEM((count * seqs, *total), F32),
        pltpu.VMEM((2 * count * seqs, *tile), BF16),
        pltpu.VMEM((2 * count * seqs, *tile), BF16),
        pltpu.VMEM((count * seqs, *tile), BF16),
        pltpu.VMEM((count * seqs, *tile), BF16),
        dma((4,)), dma((4,)), dma((16 * n,)), dma((8 * n,)), dma((2 * n * ny,)), dma((n * ny,)),
        dma((8 * n * ny,)), dma((8 * n * ny,)), dma((10,)), dma((3 * seqs,)), dma((3 * seqs,)),
        dma((seqs + 1,)), dma((seqs + 1,)), dma((4,)), dma((4,)), dma((2 * seqs * n,)),
        dma((2 * seqs * n,)), dma((2 * count * seqs,)), dma((2 * count * seqs,)),
        dma((count * seqs,)), dma((count * seqs,)),
    ]
    return pl.pallas_call(
        functools.partial(kernel, n, m),
        name="layer",
        out_shape=jax.ShapeDtypeStruct(tokens.shape, BF16),
        in_specs=[hbm, vmem, hbm, hbm, vmem, hbm, hbm, vmem, hbm, vmem, hbm, vmem, hbm, hbm],
        out_specs=vmem,
        scratch_shapes=scratch,
        compiler_params=pltpu.CompilerParams(
            collective_id=0, has_side_effects=True, vmem_limit_bytes=63 * 1024 * 1024),
    )(tokens, norm_gain[None], chain_entry, pool_entry, conv_taps, recur_gate, input_gate,
      decay_log[None], decay_shift, start_state, pool_mix, pool_scale[None],
      chain_exit, pool_exit)


def ring_kernel(
    n, m,
    tokens, gain, chain_entry, pool_entry, taps, rgate, igate, dlog, shift_hbm, start,
    pmix, pscale, chain_exit, pool_exit,
    out,
    w0, w1, w2, w3, raw, normed, cbuf, pbuf, shift, rg, ig, pm,
    convb, zr, zi, cum_a, cum_b, rec, pooled, my_ab, all_ab, ent, acc, sendbuf, recvbuf,
    s1, r1, s2, r2, t1s, t1r, t2s, t2r, loc, nsem, hsem_s, hsem_r, ab_s, ab_r, out_s, out_r,
):
    sp, fs, tp = lax.axis_index("sp"), lax.axis_index("fs"), lax.axis_index("tp")
    shards = (chain_entry, pool_entry, chain_exit, pool_exit)
    bufs = (w0, w1, w2, w3)
    seqs, half_rows, width = raw.shape
    rows = 2 * half_rows
    chans = cbuf.shape[2]
    nb = chans // COLS
    far = m // 2
    full = (m - 1) // 2

    def ring(i):
        return i + (i // 2) * (5 - 2 * i) if m == 4 else i

    pos = ring(fs)
    right, left = ring((pos + 1) % m), ring((pos + m - 1) % m)

    barrier = pltpu.get_barrier_semaphore()
    greet = [{"sp": (sp + k) % n} for k in range(1, n)] + [{"tp": 1 - tp}]
    greet += [{"fs": ring((pos + k) % m)} for k in range(1, m)]
    for device in greet:
        pl.semaphore_signal(barrier, inc=1, device_id=device, device_id_type=MESH)

    def span(w, part):
        block = shards[w].shape[0]
        tail = block // 8 // 16 * 16
        head = block - tail
        cut = -(-head // 32) * 16
        if w % 2:
            cut = head - cut
        return {"all": (0, block), None: (0, head), 0: (0, cut), 1: (cut, head - cut),
                2: (head, tail)}[part]

    def region(w, p, q, part=None):
        lo, size = span(w, part)
        at = (((sp + p) % n) * m + ring((pos + q + m) % m)) * shards[w].shape[0] + lo
        return bufs[w].at[pl.ds(pl.multiple_of(at, 16), size)]

    def own(w, part=None):
        lo, size = span(w, part)
        return shards[w].at[pl.ds(lo, size)]

    has_tail = span(0, 2)[1] > 0 and m > 1

    started = []

    def launch(copy):
        copy.start()
        started.append(copy)

    def first(w, k):
        return pltpu.make_async_remote_copy(
            src_ref=own(w), dst_ref=region(w, 0, 0), send_sem=s1.at[w * n + k],
            recv_sem=r1.at[w * n + n - k], device_id={"sp": (sp + k) % n}, device_id_type=MESH)

    def first_wait(w, p):
        pltpu.make_async_remote_copy(
            src_ref=own(w), dst_ref=region(w, p, 0), send_sem=s1.at[w * n + p],
            recv_sem=r1.at[w * n + p], device_id={"sp": (sp + p) % n},
            device_id_type=MESH).wait_recv()

    def second(w, p, way, d):
        q = -d if way == 0 else d
        part = way if (m % 2 == 0 and d + 1 == far) else None
        if p == 0 and d == 0:
            src = own(w, part)
        else:
            src = region(w, p, q, part)
        at = ((w * n + p) * 2 + way) * max(far, 1) + d
        return pltpu.make_async_remote_copy(
            src_ref=src, dst_ref=region(w, p, q, part), send_sem=s2.at[at], recv_sem=r2.at[at],
            device_id={"fs": right if way == 0 else left}, device_id_type=MESH)

    def second_wait(w, p, way, d):
        q = -d if way == 0 else d
        part = way if (m % 2 == 0 and d == far) else None
        at = ((w * n + p) * 2 + way) * max(far, 1) + d - 1
        ref = region(w, p, q, part)
        pltpu.make_async_remote_copy(
            src_ref=ref, dst_ref=ref, send_sem=s2.at[at], recv_sem=r2.at[at],
            device_id={"fs": right if way == 0 else left}, device_id_type=MESH).wait_recv()

    def second_all(w, p):
        if far >= 1:
            for way in (0, 1):
                launch(second(w, p, way, 0))

    def forward(w, p):
        for d in range(1, far):
            for way in (0, 1):
                second_wait(w, p, way, d)
                launch(second(w, p, way, d))

    def last_wait(w, p):
        tail_wait(w, p)
        if far >= 1:
            for way in (0, 1):
                second_wait(w, p, way, far)

    def tail_one(w, k):
        return pltpu.make_async_remote_copy(
            src_ref=own(w, 2), dst_ref=region(w, 0, 0, 2), send_sem=t1s.at[w * m + k],
            recv_sem=t1r.at[w * m + m - k], device_id={"fs": ring((pos + k) % m)},
            device_id_type=MESH)

    def tail_one_wait(w, q):
        ref = region(w, 0, q, 2)
        pltpu.make_async_remote_copy(
            src_ref=ref, dst_ref=ref, send_sem=t1s.at[w * m + q], recv_sem=t1r.at[w * m + q],
            device_id={"fs": ring((pos + q) % m)}, device_id_type=MESH).wait_recv()

    def tail_two(w, q, k):
        at = (w * m + q) * n
        return pltpu.make_async_remote_copy(
            src_ref=own(w, 2) if q == 0 else region(w, 0, q, 2), dst_ref=region(w, 0, q, 2),
            send_sem=t2s.at[at + k], recv_sem=t2r.at[at + n - k],
            device_id={"sp": (sp + k) % n}, device_id_type=MESH)

    def tail_start(w):
        if has_tail:
            for k in range(1, m):
                launch(tail_one(w, k))

    def tail_forward(w):
        if has_tail:
            for q in range(m):
                if q:
                    tail_one_wait(w, q)
                for k in order:
                    launch(tail_two(w, q, k))

    def tail_wait(w, p):
        if has_tail and p:
            for q in range(m):
                ref = region(w, p, q, 2)
                at = (w * m + q) * n + p
                pltpu.make_async_remote_copy(
                    src_ref=ref, dst_ref=ref, send_sem=t2s.at[at], recv_sem=t2r.at[at],
                    device_id={"sp": (sp + p) % n}, device_id_type=MESH).wait_recv()

    order = sorted(range(1, n), key=lambda p: min(p, n - p))
    local = [
        pltpu.make_async_copy(tokens, raw, loc.at[0]),
        pltpu.make_async_copy(shift_hbm, shift, loc.at[1]),
        pltpu.make_async_copy(rgate, rg, loc.at[2]),
        pltpu.make_async_copy(igate, ig, loc.at[3]),
        pltpu.make_async_copy(pmix, pm, loc.at[4]),
    ] + [pltpu.make_async_copy(shards[w], region(w, 0, 0, "all"), loc.at[5 + w]) for w in range(4)]
    for copy in local:
        copy.start()

    pl.semaphore_wait(barrier, len(greet))
    for w in (0, 1):
        second_all(w, 0)
        for k in order:
            launch(first(w, k))
        tail_start(w)

    local[0].wait()
    mine = tp * half_rows

    def norm_step(i, c):
        s, r = i // (half_rows // ROWS), (i % (half_rows // ROWS)) * ROWS
        x = raw[s, pl.ds(pl.multiple_of(r, ROWS), ROWS), :].astype(F32)
        scale = lax.rsqrt(jnp.mean(x * x, axis=-1, keepdims=True) + NORM_EPSILON)
        normed[s, pl.ds(pl.multiple_of(mine + r, ROWS), ROWS), :] = (
            x * scale * gain[...]).astype(BF16)
        return c

    lax.fori_loop(0, seqs * (half_rows // ROWS), norm_step, 0)

    def normed_copy(owner):
        ref = normed.at[:, pl.ds(pl.multiple_of(owner * half_rows, ROWS), half_rows)]
        return pltpu.make_async_remote_copy(
            src_ref=ref, dst_ref=ref, send_sem=nsem.at[0], recv_sem=nsem.at[1],
            device_id={"tp": 1 - tp}, device_id_type=MESH)

    for p in order:
        for w in (0, 1):
            first_wait(w, p)
            second_all(w, p)
        if p == order[0]:
            launch(normed_copy(tp))
    for w in (0, 1):
        tail_forward(w)
    for w in (2, 3):
        for k in order:
            launch(first(w, k))
        tail_start(w)
    for p in [0] + order:
        for w in (0, 1):
            forward(w, p)
    for w in (2, 3):
        second_all(w, 0)
    for p in [0] + order:
        for w in (0, 1):
            last_wait(w, p)
    for p in order:
        for w in (2, 3):
            first_wait(w, p)
            second_all(w, p)
    for w in (2, 3):
        tail_forward(w)
    for copy in local[1:]:
        copy.wait()
    normed_copy(1 - tp).wait_recv()

    def lanes(c):
        return pl.ds(pl.multiple_of(c * COLS, COLS), COLS)

    def entry_step(i, c):
        s, b = i // nb, lanes(i % nb)
        x = normed[s]
        cbuf[s, HALO:, b] = jnp.dot(x, w0[:, b], preferred_element_type=F32).astype(BF16)
        pbuf[s, HALO:, b] = jnp.dot(x, w1[:, b], preferred_element_type=F32).astype(BF16)
        return c

    lax.fori_loop(0, seqs * nb, entry_step, 0)

    def halo(i, ref):
        return pltpu.make_async_remote_copy(
            src_ref=ref.at[:, rows:], dst_ref=ref.at[:, :HALO], send_sem=hsem_s.at[i],
            recv_sem=hsem_r.at[i], device_id={"sp": (sp + 1) % n}, device_id_type=MESH)

    todo = [(w, p) for p in [0] + order for w in (2, 3)]

    def some_forwards(count):
        for w, p in todo[:count]:
            forward(w, p)
        del todo[:count]

    some_forwards(2)

    @pl.when(sp < n - 1)
    def _():
        halo(0, cbuf).start()
        halo(1, pbuf).start()

    @pl.when(sp > 0)
    def _():
        halo(0, cbuf).wait_recv()
        halo(1, pbuf).wait_recv()

    @pl.when(sp == 0)
    def _():
        cbuf[:, :HALO, :] = jnp.zeros((seqs, HALO, chans), BF16)
        pbuf[:, :HALO, :] = jnp.zeros((seqs, HALO, chans), BF16)

    tap_count = taps.shape[0]
    inverse_length = 1.0 / (rows * n)

    def chain_step(g, s):
        b = lanes(g)
        tap = taps[:, b].astype(F32)

        def conv(i, c):
            r = pl.multiple_of(i * ROWS, ROWS)
            v = cbuf[s, pl.ds(r, ROWS + HALO), b].astype(F32)
            total = v * tap[tap_count - 1 : tap_count]
            for j in range(tap_count - 1):
                total = total + pltpu.roll(v, tap_count - 1 - j, 0) * tap[j : j + 1]
            convb[pl.ds(r, ROWS), :] = total[HALO:].astype(BF16)
            return c

        lax.fori_loop(0, rows // ROWS, conv, 0)
        x = convb[...]
        zr[...] = jnp.dot(x, rg[g], preferred_element_type=F32)
        zi[...] = jnp.dot(x, ig[g], preferred_element_type=F32)
        rate = -RECUR_SCALE * (jnp.exp(dlog[:, b]) * inverse_length)
        row = lax.broadcasted_iota(jnp.int32, (ROWS, COLS), 0)

        def scan(i, carry):
            r = pl.multiple_of(i * ROWS, ROWS)
            at = pl.ds(r, ROWS)
            log_decay = jax.nn.sigmoid(zr[at, :]) * rate + shift[s, at, b]
            a = jnp.exp(log_decay)
            d = (jnp.sqrt(neg_expm1(2.0 * log_decay)) * jax.nn.sigmoid(zi[at, :])
                 * convb[at, :].astype(F32))
            k = 1
            while k < ROWS:
                before = row >= k
                d = d + a * jnp.where(before, pltpu.roll(d, k, 0), 0.0)
                a = a * jnp.where(before, pltpu.roll(a, k, 0), 1.0)
                k *= 2
            d = d + a * carry[1]
            a = a * carry[0]
            cum_a[s, at, b] = a
            cum_b[s, at, b] = d
            return a[ROWS - 1 :], d[ROWS - 1 :]

        end = lax.fori_loop(
            0, rows // ROWS, scan, (jnp.ones((1, COLS), F32), jnp.zeros((1, COLS), F32)))
        my_ab[pl.ds(s, 1), b] = end[0]
        my_ab[pl.ds(seqs + s, 1), b] = end[1]

    for s in range(seqs):
        def chain_group(g, c, s=s):
            chain_step(g, s)
            return c

        for g0 in range(0, nb, 2):
            lax.fori_loop(g0, min(g0 + 2, nb), chain_group, 0)
            some_forwards(max(1, len(todo) // (2 * seqs)))

    def ab_copy(k):
        return pltpu.make_async_remote_copy(
            src_ref=my_ab, dst_ref=all_ab.at[k], send_sem=ab_s.at[k], recv_sem=ab_r.at[k],
            device_id={"sp": (sp + k) % n}, device_id_type=MESH)

    def pool_group(g):
        b = slice(g * COLS, (g + 1) * COLS)
        window = 2 ** (1 + g % 4)

        def diff(i, c):
            s, r = i // (rows // ROWS), pl.multiple_of((i % (rows // ROWS)) * ROWS, ROWS)
            v = pbuf[s, pl.ds(r, ROWS + HALO), b].astype(F32)
            total, k = v, 1
            while k < window:
                total = total + pltpu.roll(total, k, 0)
                k *= 2
            t = lax.broadcasted_iota(jnp.int32, (ROWS, COLS), 0) + (sp * rows + r + 1)
            count = jnp.minimum(t, window).astype(F32)
            convb_pool = total[HALO:] / count - v[HALO:]
            pooled[s, pl.ds(r, ROWS), b] = convb_pool.astype(BF16)
            return c

        lax.fori_loop(0, seqs * (rows // ROWS), diff, 0)
        for s in range(seqs):
            y = jnp.dot(pooled[s, :, b], pm[g], preferred_element_type=F32)
            pooled[s, :, b] = (y * pscale[:, b]).astype(BF16)

    pool_group(0)
    for k in range(1, n):
        @pl.when(sp + k < n)
        def _(k=k):
            ab_copy(k).start()

    for g in range(1, nb):
        pool_group(g)
        some_forwards(1)
    some_forwards(len(todo))

    ent[...] = start[...]
    for k in range(n - 1, 0, -1):
        @pl.when(sp >= k)
        def _(k=k):
            ab_copy(k).wait_recv()
            ent[...] = all_ab[k, :seqs, :] * ent[...] + all_ab[k, seqs : 2 * seqs, :]

    for s in range(seqs):
        def fix(i, c, s=s):
            at = pl.ds(pl.multiple_of(i * ROWS, ROWS), ROWS)
            rec[s, at, :] = (cum_a[s, at, :] * ent[s : s + 1, :] + cum_b[s, at, :]).astype(BF16)
            return c

        lax.fori_loop(0, rows // ROWS, fix, 0)

    dims = (((1,), (1,)), ((), ()))
    out_cols = sendbuf.shape[2]
    out_count = width // out_cols
    per_group = m * chain_exit.shape[0] // out_cols

    def out_lanes(j):
        return pl.ds(pl.multiple_of(j * out_cols, out_cols), out_cols)

    def partial(owner, j):
        at = pl.ds(pl.multiple_of(owner * half_rows, ROWS), half_rows)
        b = out_lanes(j)
        x = rec[:, at, :].reshape(seqs * half_rows, chans)
        y = pooled[:, at, :].reshape(seqs * half_rows, chans)
        return lax.dot_general(x, w2[b, :], dims, preferred_element_type=F32) + lax.dot_general(
            y, w3[b, :], dims, preferred_element_type=F32)

    def out_copy(j):
        return pltpu.make_async_remote_copy(
            src_ref=sendbuf.at[j], dst_ref=recvbuf.at[j], send_sem=out_s.at[j],
            recv_sem=out_r.at[j], device_id={"tp": 1 - tp}, device_id_type=MESH)

    def exit_step(j, c):
        sendbuf[j] = partial(1 - tp, j).astype(BF16)
        acc[j] = partial(tp, j)
        out_copy(j).start()
        return c

    def out_step(j, c):
        out_copy(j).wait_recv()
        total = (acc[j] + recvbuf[j].astype(F32)).astype(BF16)
        out[:, :, out_lanes(j)] = total.reshape(seqs, half_rows, out_cols)
        return c

    def group(p, step):
        j = ((sp + p) % n) * per_group
        lax.fori_loop(j, j + per_group, step, 0)

    before = None
    for p in [0] + order:
        for w in (2, 3):
            last_wait(w, p)
        group(p, exit_step)
        if before is not None:
            group(before, out_step)
        before = p
    group(before, out_step)

    def out_end(j, c):
        out_copy(j).wait_send()
        return c

    lax.fori_loop(0, out_count, out_end, 0)
    for copy in started:
        copy.wait_send()

    @pl.when(sp < n - 1)
    def _():
        halo(0, cbuf).wait_send()
        halo(1, pbuf).wait_send()

    for k in range(1, n):
        @pl.when(sp + k < n)
        def _(k=k):
            ab_copy(k).wait_send()


def ring_device(n, m, *args):
    (tokens, norm_gain, chain_entry, pool_entry, conv_taps, recur_gate, input_gate, decay_log,
     decay_shift, start_state, pool_mix, pool_scale, chain_exit, pool_exit) = args
    seqs, half_rows, width = tokens.shape
    rows, chans = 2 * half_rows, chain_entry.shape[1]
    nb = chans // COLS
    assert pool_mix.shape[0] % 4 == 0 and pool_mix.shape[1] == COLS
    far = max(m // 2, 1)
    hbm, vmem = pl.BlockSpec(memory_space=pl.ANY), pl.BlockSpec(memory_space=pltpu.VMEM)
    dma = pltpu.SemaphoreType.DMA
    ab_rows = -(-2 * seqs // 8) * 8
    out_cols = min(COLS, m * chain_exit.shape[1])
    out_count = width // out_cols
    scratch = [pltpu.VMEM((width, chans), BF16)] * 4 + [
        pltpu.VMEM((seqs, half_rows, width), BF16),
        pltpu.VMEM((seqs, rows, width), BF16),
        pltpu.VMEM((seqs, HALO + rows, chans), BF16),
        pltpu.VMEM((seqs, HALO + rows, chans), BF16),
        pltpu.VMEM((seqs, rows, chans), F32),
        pltpu.VMEM(recur_gate.shape, BF16),
        pltpu.VMEM(input_gate.shape, BF16),
        pltpu.VMEM(pool_mix.shape, BF16),
        pltpu.VMEM((rows, COLS), BF16),
        pltpu.VMEM((rows, COLS), F32),
        pltpu.VMEM((rows, COLS), F32),
        pltpu.VMEM((seqs, rows, chans), F32),
        pltpu.VMEM((seqs, rows, chans), F32),
        pltpu.VMEM((seqs, rows, chans), BF16),
        pltpu.VMEM((seqs, rows, chans), BF16),
        pltpu.VMEM((ab_rows, chans), F32),
        pltpu.VMEM((n, ab_rows, chans), F32),
        pltpu.VMEM((seqs, chans), F32),
        pltpu.VMEM((out_count, seqs * half_rows, out_cols), F32),
        pltpu.VMEM((out_count, seqs * half_rows, out_cols), BF16),
        pltpu.VMEM((out_count, seqs * half_rows, out_cols), BF16),
        dma((4 * n,)), dma((4 * n,)), dma((8 * n * far,)), dma((8 * n * far,)),
        dma((4 * m,)), dma((4 * m,)), dma((4 * m * n,)), dma((4 * m * n,)),
        dma((9,)), dma((2,)), dma((2,)), dma((2,)), dma((n,)), dma((n,)),
        dma((out_count,)), dma((out_count,)),
    ]
    return pl.pallas_call(
        functools.partial(ring_kernel, n, m),
        name="layer",
        out_shape=jax.ShapeDtypeStruct(tokens.shape, BF16),
        in_specs=[hbm, vmem, hbm, hbm, vmem, hbm, hbm, vmem, hbm, vmem, hbm, vmem, hbm, hbm],
        out_specs=vmem,
        scratch_shapes=scratch,
        compiler_params=pltpu.CompilerParams(
            collective_id=0, has_side_effects=True, vmem_limit_bytes=62 * 1024 * 1024),
    )(tokens, norm_gain[None], chain_entry, pool_entry, conv_taps, recur_gate, input_gate,
      decay_log[None], decay_shift, start_state, pool_mix, pool_scale[None],
      chain_exit.T, pool_exit.T)


def solution(mesh):
    in_specs = (
        P("fs", ("sp", "tp"), None),
        P(),
        P(("sp", "fs"), "tp"),
        P(("sp", "fs"), "tp"),
        P(None, "tp"),
        P("tp", None, None),
        P("tp", None, None),
        P("tp"),
        P("fs", "sp", "tp"),
        P("fs", "tp"),
        P("tp", None, None),
        P("tp"),
        P("tp", ("sp", "fs")),
        P("tp", ("sp", "fs")),
    )
    out_specs = P("fs", ("sp", "tp"), None)
    n, m = mesh.shape["sp"], mesh.shape["fs"]

    def layer(*args):
        wide = m % 2 == 0 and args[12].shape[1] % 128 == 0
        return (per_device if wide else ring_device)(n, m, *args)

    return jax.shard_map(
        layer, mesh=mesh, in_specs=in_specs, out_specs=out_specs, check_vma=False)
```

```python
import functools

import jax
import jax.numpy as jnp
from jax import lax
from jax.experimental import pallas as pl
from jax.experimental.pallas import tpu as pltpu
from jax.sharding import PartitionSpec as P

MESH = pl.DeviceIdType.MESH
NORM_EPSILON = 1e-06
RECUR_SCALE = 8.0
HALO = 16
COLS = 256
ROWS = 64
ENTRY = (0, 1)
EXIT = (2, 3)
OWN, PEER = 0, 1
TURN = 1
PEER_SLOTS = 2
F32 = jnp.float32
BF16 = jnp.bfloat16


def neg_expm1(x):
    y = -x
    poly = 1.0 - y * (1.0 / 9.0)
    for k in range(8, 1, -1):
        poly = 1.0 - y * (1.0 / k) * poly
    return jnp.where(y < 0.5, y * poly, 1.0 - jnp.exp(x))


def nearest(n):
    order = [sorted(range(n), key=lambda z, s=s: (abs(z - s), (z - s) * (-1 if 2 * s < n else 1)))
             for s in range(n)]
    return [sum(order[s][r] * n**s for s in range(n)) for r in range(n)]


def kernel(
    n, m,
    tokens, gain, chain_entry, pool_entry, taps, rgate, igate, dlog, shift_hbm, start,
    pmix, pscale, chain_exit, pool_exit,
    out,
    w0, w1, exits, raw, normed, cum_a, cum_b, cbuf, pbuf, shift, wide, narrow, peer_shift,
    my_start, peer_start, rg, ig, pm,
    convb, zr, zi, mix, my_ab, all_ab, ent,
    peer_acc, own_acc, core_send, core_recv, x_send, x_recv,
    xs, xr, zs, zrv, zts, ztr, ys, yr, loc, nsem_s, nsem_r, ssem_s, ssem_r, hsem_s, hsem_r,
    ab_s, ab_r, core_s, core_r, out_s, out_r,
):
    scope = jax.named_scope
    sp, fs, tp = lax.axis_index("sp"), lax.axis_index("fs"), lax.axis_index("tp")
    ny = m // 2
    x, y = fs % 2, fs // 2
    shards = (chain_entry, pool_entry, chain_exit, pool_exit)
    bufs = (w0, w1)
    seqs, half_rows, width = raw.shape
    rows = 2 * half_rows
    half = cbuf.shape[2]
    rec, pooled = mix.at[:, :, pl.ds(0, half)], mix.at[:, :, pl.ds(half, half)]
    nb = half // COLS
    depth = chain_entry.shape[0]
    cols = chain_exit.shape[1]
    zdepth = m * depth
    own = range(seqs)
    last = n - 1

    codes = nearest(n)

    def digit(code):
        value = sp * 0
        for s in range(n):
            value = value + code // n**s % n * jnp.where(sp == s, 1, 0)
        return value

    ranks = [digit(code) for code in codes]
    units = (x, 1 - x)
    x_peer = {"fs": y * 2 + 1 - x}
    core_peer = {"tp": 1 - tp}

    def y_peer(k):
        return {"fs": ((y + k) % ny) * 2 + x}

    def y_from(k):
        return (y + ny - k) % ny

    barrier = pltpu.get_barrier_semaphore()
    greet = [{"sp": (sp + k) % n} for k in range(1, n)] + [core_peer, x_peer]
    greet += [y_peer(k) for k in range(1, ny)]
    for device in greet:
        pl.semaphore_signal(barrier, inc=1, device_id=device, device_id_type=MESH)

    started = []

    def launch(copy, cond=None):
        if cond is None:
            copy.start()
        else:
            pl.when(cond)(copy.start)
        started.append((copy, cond))

    def remote(src, dst, send, recv, device):
        return pltpu.make_async_remote_copy(
            src_ref=src, dst_ref=dst, send_sem=send, recv_sem=recv, device_id=device,
            device_id_type=MESH)

    def region(w, z, yy, xx):
        if w in ENTRY:
            b = z * m + yy * 2 + xx
            return bufs[w].at[pl.ds(pl.multiple_of(b * depth, depth), depth)]
        at = pl.ds((w - EXIT[0]) * half, half)
        return exits.at[z * 2 + xx, at, pl.ds(pl.multiple_of(yy * cols, cols), cols)]

    def shard(w, h):
        at = pl.ds(pl.multiple_of(h * half, half), half)
        return shards[w].at[:, at] if w in ENTRY else shards[w].at[at]

    def cross(w):
        return remote(shard(w, 1 - x), region(w, sp, y, x), xs.at[w], xr.at[w], x_peer)

    def cross_wait(w):
        ref = region(w, sp, y, 1 - x)
        remote(ref, ref, xs.at[w], xr.at[w], x_peer).wait_recv()

    def z_peer(way):
        return {"sp": (sp + (1, n - 1)[way]) % n}

    def z_copy(w, z, xx, way, src=None, home=False):
        ref = region(w, z, y, xx)
        at = (w * 2 + xx) * (n + 1)
        return remote(ref if src is None else src, ref, zs.at[at + (n if home and way else z)],
                      zrv.at[(w * 2 + xx) * n + z], z_peer(way))

    def z_turn(z, k, way, home=False):
        ref = region(TURN, z, y_from(k), x)
        at = (n if home and way else z) * (ny - 1) + k - 1
        return remote(ref, ref, zts.at[at], ztr.at[z * (ny - 1) + k - 1], z_peer(way))

    def y_copy(w, z, xx, k, src=None):
        ref = region(w, z, y, xx)
        at = ((w * n + z) * 2 + xx) * (ny - 1) + k - 1
        return remote(ref if src is None else src, ref, ys.at[at], yr.at[at], y_peer(k))

    def y_wait(w, z, xx, k):
        ref = region(w, z, y_from(k), xx)
        at = ((w * n + z) * 2 + xx) * (ny - 1) + k - 1
        remote(ref, ref, ys.at[at], yr.at[at], y_peer(k)).wait_recv()

    def source(w, unit):
        return shard(w, x) if unit == 0 else None

    def z_send(w, unit):
        if n > 1:
            launch(z_copy(w, sp, units[unit], 0, source(w, unit), True), sp + 1 < n)
            launch(z_copy(w, sp, units[unit], 1, source(w, unit), True), sp > 0)

    def exit_z_send(unit, to_end):
        ends = (sp + 2 == n, sp == 1) if n > 2 else (sp < 0, sp < 0)
        for w in EXIT:
            if n > 1:
                for way, inside in ((0, sp + 1 < n), (1, sp > 0)):
                    end = ends[way] if to_end else jnp.logical_not(ends[way])
                    launch(z_copy(w, sp, units[unit], way, source(w, unit), True), inside & end)

    def turn_send():
        for k in range(1, ny):
            if n > 1:
                launch(z_turn(sp, k, 0, True), sp + 1 < n)
                launch(z_turn(sp, k, 1, True), sp > 0)

    def y_send(w, unit):
        for k in range(1, ny):
            launch(y_copy(w, sp, units[unit], k, source(w, unit)))

    def both(cond, other):
        return other if cond is None else cond & other

    def relay_on(z, make, cond):
        if n > 2:
            launch(make(0), both(cond, (z < sp) & (sp + 1 < n)))
            launch(make(1), both(cond, (z > sp) & (sp > 0)))

    def wait_if(make, cond):
        if cond is None:
            make().wait_recv()
        else:
            pl.when(cond)(lambda: make().wait_recv())

    def forward(w, r, unit, cond=None):
        z, xx = ranks[r], units[unit]
        wait_if(lambda: z_copy(w, z, xx, 0), cond)
        relay_on(z, lambda way: z_copy(w, z, xx, way), cond)
        if (w, unit) != (TURN, 0):
            for k in range(1, ny):
                launch(y_copy(w, z, xx, k), cond)

    def turn_forward(r, cond=None):
        z = ranks[r]
        for k in range(1, ny):
            wait_if(lambda k=k: z_turn(z, k, 0), cond)
            relay_on(z, lambda way, k=k: z_turn(z, k, way), cond)

    edge = (sp == 0) | (sp == n - 1)
    inner = (sp > 0) & (sp < n - 1)

    def entry_forward(r, cond=None, part=None):
        todo = [(0, 0), (1, 0), (0, 1), (1, 1)]
        todo = todo if part is None else (todo[:3], todo[3:])[part]
        with scope(f"efwd#r={r}"):
            for w, unit in todo:
                forward(w, r, unit, cond)
            if part != 0:
                turn_forward(r, cond)

    def entry_arrived(r):
        for k in range(1, ny):
            for w in ENTRY:
                for unit in (0, 1):
                    if (w, unit) != (TURN, 0):
                        y_wait(w, ranks[r], units[unit], k)

    def exit_arrived(r, unit):
        for k in range(1, ny):
            for w in EXIT:
                y_wait(w, ranks[r], units[unit], k)

    def exit_forward(r, unit, cond=None):
        with scope(f"xfwd#r={r}#u={unit}"):
            for w in EXIT:
                if r:
                    forward(w, r, unit, cond)
                else:
                    cross_wait(w)
                    y_send(w, unit)
            if r == 0:
                exit_z_send(unit, False)

    def forwards(r, unit, cond):
        for rr in range(r, n if r == 3 else min(r + 1, n)):
            exit_forward(rr, unit, cond)

    def lanes(c, base=0):
        return pl.ds(pl.multiple_of(base + c * COLS, COLS), COLS)

    mine_lanes = pl.ds(pl.multiple_of(x * half, half), half)
    peer_lanes = pl.ds(pl.multiple_of((1 - x) * half, half), half)
    heads = pl.ds(x * nb, nb)

    local = [
        pltpu.make_async_copy(tokens, raw, loc.at[0]),
        pltpu.make_async_copy(shift_hbm.at[:, :, peer_lanes], wide, loc.at[1]),
        pltpu.make_async_copy(shift_hbm.at[:, :, mine_lanes], shift, loc.at[2]),
        pltpu.make_async_copy(rgate.at[heads], rg, loc.at[3]),
        pltpu.make_async_copy(igate.at[heads], ig, loc.at[4]),
        pltpu.make_async_copy(pmix.at[heads], pm, loc.at[5]),
    ] + [pltpu.make_async_copy(shard(w, x), region(w, sp, y, x), loc.at[6 + w]) for w in range(4)]
    for copy in local:
        copy.start()
    my_start[...] = jnp.zeros(my_start.shape, F32)
    my_start[:seqs, :] = start[:, peer_lanes]

    with scope("entry_barrier"):
        pl.semaphore_wait(barrier, len(greet))
    for w in ENTRY:
        launch(cross(w))
    for w in ENTRY:
        z_send(w, 0)
        y_send(w, 0)

    local[0].wait()

    def half_of(s, owner):
        return normed.at[s, pl.ds(pl.multiple_of(owner * half_rows, ROWS), half_rows)]

    def norm_x(s):
        return remote(half_of(s, tp), half_of(seqs + s, tp), nsem_s.at[s], nsem_r.at[s], x_peer)

    def norm_core(s):
        return remote(half_of(s, tp), half_of(s, tp), nsem_s.at[seqs + s], nsem_r.at[seqs + s],
                      core_peer)

    for s in own:
        def norm_step(i, c, s=s):
            r = pl.multiple_of(i * ROWS, ROWS)
            v = raw[s, pl.ds(r, ROWS), :].astype(F32)
            scale = lax.rsqrt(jnp.mean(v * v, axis=-1, keepdims=True) + NORM_EPSILON)
            normed[s, pl.ds(pl.multiple_of(tp * half_rows + r, ROWS), ROWS), :] = (
                v * scale * gain[...]).astype(BF16)
            return c

        lax.fori_loop(0, half_rows // ROWS, norm_step, 0)

    local[1].wait()

    def narrow_step(i, c):
        s, r = i // (rows // ROWS), pl.multiple_of((i % (rows // ROWS)) * ROWS, ROWS)
        narrow[s, pl.ds(r, ROWS), :] = wide[s, pl.ds(r, ROWS), :].astype(BF16)
        return c

    lax.fori_loop(0, seqs * (rows // ROWS), narrow_step, 0)
    for copy in local[2:]:
        copy.wait()
    start_copy = remote(my_start, peer_start, ssem_s.at[seqs], ssem_r.at[seqs], x_peer)

    def shift_copy(s):
        return remote(narrow.at[s], peer_shift.at[s], ssem_s.at[s], ssem_r.at[s], x_peer)

    for s in own:
        launch(norm_core(s))
    with scope("cross_fwd"):
        for w in ENTRY:
            cross_wait(w)
            z_send(w, 1)
            y_send(w, 1)
            if w == ENTRY[0]:
                launch(norm_x(0))
    launch(start_copy)
    for w in EXIT:
        y_send(w, 0)
    with scope("turn_fwd"):
        for k in range(1, ny):
            y_wait(TURN, sp, x, k)
        turn_send()

    def entry_part(s, r):
        at = pl.ds(pl.multiple_of(ranks[r] * zdepth, zdepth), zdepth)

        def step(j, c):
            b = lanes(j)
            v = normed[s, :, at]
            for w, total, dst in ((w0, cum_a, cbuf), (w1, cum_b, pbuf)):
                part = jnp.dot(v, w[at, b], preferred_element_type=F32)
                if r:
                    part = total[s, :, b] + part
                if r == last:
                    dst[s, HALO:, b] = part.astype(BF16)
                else:
                    total[s, :, b] = part
            return c

        lax.fori_loop(0, nb, step, 0)

    def core_wait(s):
        ref = half_of(s, 1 - tp)
        remote(ref, ref, nsem_s.at[seqs + s], nsem_r.at[seqs + s], core_peer).wait_recv()

    def relay(s):
        ref = half_of(seqs + s, tp)
        remote(ref, ref, nsem_s.at[s], nsem_r.at[s], x_peer).wait_recv()
        at = 2 * seqs + s
        launch(remote(ref, ref, nsem_s.at[at], nsem_r.at[at], core_peer))

    def relay_wait(s):
        ref = half_of(seqs + s, 1 - tp)
        at = 2 * seqs + s
        remote(ref, ref, nsem_s.at[at], nsem_r.at[at], core_peer).wait_recv()

    def entry_parts(seqs_of, r):
        with scope(f"edot#r={r}"):
            for s in seqs_of:
                entry_part(s, r)

    def entry_ready(r):
        with scope(f"earr#r={r}"):
            entry_arrived(r)

    peer = range(seqs, 2 * seqs)
    for r in range(1, last):
        entry_forward(r)
        if r == 1:
            for s in own:
                core_wait(s)
        entry_ready(r - 1)
        entry_parts(own, r - 1)
        if r == 1:
            for w in EXIT:
                launch(cross(w))
            for s in own[1:]:
                launch(norm_x(s))
            exit_z_send(0, False)
    if n > 1:
        entry_forward(last, inner)
    if n < 3:
        for s in own:
            core_wait(s)
        for w in EXIT:
            launch(cross(w))
        for s in own[1:]:
            launch(norm_x(s))
        exit_z_send(0, False)
    with scope("relay#s=0"):
        relay(0)
        relay_wait(0)
    for r in range(last - 1):
        entry_parts([seqs], r)
    if n > 1:
        entry_forward(last, edge, 0)
        entry_ready(last - 1)
        entry_parts(range(seqs + 1), last - 1)
    exit_z_send(0, True)
    forwards(1, 0, inner)
    forwards(2, 0, inner)
    if n > 1:
        entry_forward(last, edge, 1)
    exit_forward(0, 1)
    with scope("relay#s=1"):
        for s in own[1:]:
            relay(s)
    launch(shift_copy(0))
    with scope("relay_wait#s=1"):
        for s in own[1:]:
            relay_wait(s)
    for r in range(last):
        entry_parts(range(seqs + 1, 2 * seqs), r)
    with scope("earr_last"):
        entry_arrived(last)

    def halo(pair, i):
        ref = (cbuf, pbuf)[i]
        at = pl.ds(pair * seqs, seqs)
        return remote(ref.at[at, pl.ds(rows, HALO)], ref.at[at, pl.ds(0, HALO)],
                      hsem_s.at[pair * 2 + i], hsem_r.at[pair * 2 + i], {"sp": (sp + 1) % n})

    for pair in (PEER, OWN):
        for s in own:
            entry_part(pair * seqs + s, last)
        for i in (0, 1):
            launch(halo(pair, i), sp < n - 1)
    for s in own[1:]:
        launch(shift_copy(s))
    forwards(1, 0, edge)
    forwards(3, 0, inner)

    def halo_wait(pair):
        @pl.when(sp > 0)
        def _():
            halo(pair, 0).wait_recv()
            halo(pair, 1).wait_recv()

        @pl.when(sp == 0)
        def _():
            zero = jnp.zeros((seqs, HALO, half), BF16)
            cbuf[pair * seqs : (pair + 1) * seqs, :HALO, :] = zero
            pbuf[pair * seqs : (pair + 1) * seqs, :HALO, :] = zero

    tap_count = taps.shape[0]
    inverse_length = 1.0 / (rows * n)

    def chain(pair, s0):
        s = pair * seqs + s0

        def group(g, carry):
            b = lanes(g)
            whole = lanes(g, x * half)
            tap = taps[:, whole].astype(F32)

            def conv(i, c):
                r = pl.multiple_of(i * ROWS, ROWS)
                v = cbuf[s, pl.ds(r, ROWS + HALO), b].astype(F32)
                total = v * tap[tap_count - 1 : tap_count]
                for j in range(tap_count - 1):
                    total = total + pltpu.roll(v, tap_count - 1 - j, 0) * tap[j : j + 1]
                convb[pl.ds(r, ROWS), :] = total[HALO:].astype(BF16)
                return c

            lax.fori_loop(0, rows // ROWS, conv, 0)
            v = convb[...]
            zr[...] = jnp.dot(v, rg[g], preferred_element_type=F32)
            zi[...] = jnp.dot(v, ig[g], preferred_element_type=F32)
            rate = -RECUR_SCALE * (jnp.exp(dlog[:, whole]) * inverse_length)
            row = lax.broadcasted_iota(jnp.int32, (ROWS, COLS), 0)
            source = peer_shift if pair == PEER else shift

            def scan(i, ends):
                r = pl.multiple_of(i * ROWS, ROWS)
                at = pl.ds(r, ROWS)
                log_decay = (jax.nn.sigmoid(zr[at, :]) * rate
                             + source[s0, at, b].astype(F32))
                a = jnp.exp(log_decay)
                d = (jnp.sqrt(neg_expm1(2.0 * log_decay)) * jax.nn.sigmoid(zi[at, :])
                     * convb[at, :].astype(F32))
                k = 1
                while k < ROWS:
                    before = row >= k
                    d = d + a * jnp.where(before, pltpu.roll(d, k, 0), 0.0)
                    a = a * jnp.where(before, pltpu.roll(a, k, 0), 1.0)
                    k *= 2
                d = d + a * ends[1]
                a = a * ends[0]
                cum_a[s, at, b] = a
                cum_b[s, at, b] = d
                return a[ROWS - 1 :], d[ROWS - 1 :]

            end = lax.fori_loop(
                0, rows // ROWS, scan, (jnp.ones((1, COLS), F32), jnp.zeros((1, COLS), F32)))
            my_ab[s, pl.ds(0, 1), b] = end[0]
            my_ab[s, pl.ds(1, 1), b] = end[1]
            return carry

        with scope(f"chain#p={pair}#s={s0}"):
            lax.fori_loop(0, nb, group, 0)
        for k in range(1, n):
            launch(ab_copy(s, k), sp + k < n)

    def ab_copy(s, k):
        at = s * (n - 1) + k - 1
        return remote(my_ab.at[s], all_ab.at[at], ab_s.at[at], ab_r.at[at], {"sp": (sp + k) % n})

    def pool(pair):
        def group(g, window):
            b = lanes(g)

            def diff(i, c):
                s = pair * seqs + i // (rows // ROWS)
                r = pl.multiple_of((i % (rows // ROWS)) * ROWS, ROWS)
                v = pbuf[s, pl.ds(r, ROWS + HALO), b].astype(F32)
                total, k = v, 1
                while k < window:
                    total = total + pltpu.roll(total, k, 0)
                    k *= 2
                t = lax.broadcasted_iota(jnp.int32, (ROWS, COLS), 0) + (sp * rows + r + 1)
                count = jnp.minimum(t, window).astype(F32)
                pooled[s, pl.ds(r, ROWS), b] = (total[HALO:] / count - v[HALO:]).astype(BF16)
                return c

            lax.fori_loop(0, seqs * (rows // ROWS), diff, 0)
            for s0 in own:
                s = pair * seqs + s0
                p = jnp.dot(pooled[s, :, b], pm[g], preferred_element_type=F32)
                pooled[s, :, b] = (p * pscale[:, lanes(g, x * half)]).astype(BF16)

        with scope(f"pool#p={pair}"):
            for xx in (0, 1):
                @pl.when(x == xx)
                def _(xx=xx):
                    for g in range(nb):
                        group(g, 2 ** (1 + (xx * nb + g) % 4))

    def fix(pair, s0):
        s = pair * seqs + s0
        with scope(f"fix#p={pair}#s={s0}"):
            if pair == OWN:
                ent[s : s + 1, :] = start[s0 : s0 + 1, mine_lanes]
            else:
                ent[s : s + 1, :] = peer_start[s0 : s0 + 1, :]
            for k in range(n - 1, 0, -1):
                @pl.when(sp >= k)
                def _(k=k):
                    ab_copy(s, k).wait_recv()
                    at = s * (n - 1) + k - 1
                    ent[s : s + 1, :] = all_ab[at, 0:1, :] * ent[s : s + 1, :] + all_ab[at, 1:2, :]

            def step(i, c):
                at = pl.ds(pl.multiple_of(i * ROWS, ROWS), ROWS)
                rec[s, at, :] = (
                    cum_a[s, at, :] * ent[s : s + 1, :] + cum_b[s, at, :]).astype(BF16)
                return c

            lax.fori_loop(0, rows // ROWS, step, 0)

    groups = [(unit, r) for unit in (0, 1) for r in range(n)]
    count = len(groups)

    def core_copy(pair, c, which):
        at = pair * count + c
        sem = c * seqs + which.start if pair else count * seqs + c
        return remote(core_send.at[at, which], core_recv.at[at, which], core_s.at[sem],
                      core_r.at[sem], core_peer)

    def x_copy(c, which):
        sem = c * seqs + which.start
        return remote(x_send.at[c, which], x_recv.at[c, which], out_s.at[sem], out_r.at[sem],
                      x_peer)

    def owner_rows(owner):
        return pl.ds(pl.multiple_of(owner * half_rows, ROWS), half_rows)

    def slot(which, c):
        return slots.setdefault((c, which.start), len(slots) % PEER_SLOTS)

    slots = {}

    def dots(pair, which, c):
        unit, r = groups[c]
        size = which.size
        b = ranks[r] * 2 + units[unit]
        total = peer_acc.at[slot(which, c), which] if pair else own_acc.at[c, which]
        with scope(f"dots#p={pair}#s={which.start}#c={c}"):
            def part(owner):
                v = mix[pl.ds(pair * seqs + which.start, size), owner_rows(owner), :]
                v = v.reshape(size * half_rows, 2 * half)
                return jnp.dot(v, exits[b], preferred_element_type=F32).reshape(total.shape)

            core_send[pair * count + c, which] = part(1 - tp).astype(BF16)
            total[...] = part(tp)
        launch(core_copy(pair, c, which))

    def peer_send(which, c):
        with scope(f"send#s={which.start}#c={c}"):
            core_copy(PEER, c, which).wait_recv()
            x_send[c, which] = (
                peer_acc[slot(which, c), which]
                + core_recv[PEER * count + c, which].astype(F32)).astype(BF16)
        launch(x_copy(c, which))
        sent[c].append(which)

    sent = [[] for _ in groups]

    def own_out(c):
        unit, r = groups[c]
        other = groups.index((1 - unit, r))
        with scope(f"out#c={c}"):
            core_copy(OWN, c, every).wait_recv()
            for which in sent[other]:
                x_copy(other, which).wait_recv()
            total = (own_acc[c] + core_recv[OWN * count + c].astype(F32)
                     + x_recv[other].astype(F32)).astype(BF16)
            for yy in range(ny):
                col = (ranks[r] * m + yy * 2 + units[unit]) * cols
                out[:, :, pl.ds(pl.multiple_of(col, cols), cols)] = (
                    total[:, :, yy * cols : (yy + 1) * cols])

    every = pl.ds(0, seqs)
    waiting = []
    seen = set()

    def peer_step(which, c):
        if c not in seen:
            seen.add(c)
            with scope(f"xarr#c={c}"):
                exit_arrived(groups[c][1], groups[c][0])
        dots(PEER, which, c)
        flush()
        waiting.append((which, c))

    def flush():
        while waiting:
            peer_send(*waiting.pop())

    own_units = list(range(n))
    peer_units = list(range(n, 2 * n))
    later = own[1:]

    with scope("halo_p"):
        halo_wait(PEER)
    pool(PEER)
    forwards(2, 0, edge)
    with scope("shift_wait#s=0"):
        shift_copy(0).wait_recv()
    chain(PEER, 0)
    exit_z_send(1, True)
    forwards(1, 1, inner)
    forwards(2, 1, inner)
    with scope("start_wait"):
        start_copy.wait_recv()
    fix(PEER, 0)
    lead = own_units[:2] + peer_units[:1] + own_units[2:3]
    for c in lead:
        peer_step(pl.ds(0, 1), c)
    flush()
    forwards(3, 0, edge)
    for s0 in later:
        with scope(f"shift_wait#s={s0}"):
            shift_copy(s0).wait_recv()
        chain(PEER, s0)
    forwards(3, 1, inner)
    forwards(1, 1, edge)
    with scope("halo_o"):
        halo_wait(OWN)
    pool(OWN)
    tail = own_units[3:]
    for c in tail:
        peer_step(pl.ds(0, 1), c)
    for s0 in later:
        fix(PEER, s0)
        for c in lead + tail:
            peer_step(pl.ds(s0, 1), c)
    forwards(2, 1, edge)
    flush()
    chain(OWN, 0)
    for c in peer_units[1:2]:
        peer_step(every, c)
    forwards(3, 1, edge)
    fix(OWN, 0)
    flush()
    for s0 in later:
        chain(OWN, s0)
    for c in peer_units[2:3]:
        peer_step(every, c)
    for s0 in later:
        fix(OWN, s0)
    for c in lead[:2]:
        dots(OWN, every, c)
    flush()
    for c in peer_units[3:]:
        peer_step(every, c)
    for c in lead[2:4]:
        dots(OWN, every, c)
    flush()
    for c in lead[4:] + tail:
        dots(OWN, every, c)
    for c in peer_units[1:]:
        dots(OWN, every, c)
    for c in peer_units + own_units:
        own_out(c)

    with scope("drain"):
        for copy, cond in started:
            if cond is None:
                copy.wait_send()
            else:
                pl.when(cond)(copy.wait_send)


def per_device(n, m, *args):
    (tokens, norm_gain, chain_entry, pool_entry, conv_taps, recur_gate, input_gate, decay_log,
     decay_shift, start_state, pool_mix, pool_scale, chain_exit, pool_exit) = args
    seqs, half_rows, width = tokens.shape
    rows, half = 2 * half_rows, chain_entry.shape[1] // 2
    nb = half // COLS
    ny = m // 2
    assert pool_mix.shape[0] % 4 == 0 and pool_mix.shape[1] == COLS
    hbm, vmem = pl.BlockSpec(memory_space=pl.ANY), pl.BlockSpec(memory_space=pltpu.VMEM)
    dma = pltpu.SemaphoreType.DMA
    cols = ny * chain_exit.shape[1]
    count = 2 * n
    hops = ny - 1
    tile = (seqs, half_rows, cols)
    scratch = [pltpu.VMEM((width, half), BF16)] * 2 + [
        pltpu.VMEM((2 * n, 2 * half, cols), BF16),
        pltpu.VMEM((seqs, half_rows, width), BF16),
        pltpu.VMEM((2 * seqs, rows, width), BF16),
        pltpu.VMEM((2 * seqs, rows, half), F32),
        pltpu.VMEM((2 * seqs, rows, half), F32),
        pltpu.VMEM((2 * seqs, HALO + rows, half), BF16),
        pltpu.VMEM((2 * seqs, HALO + rows, half), BF16),
        pltpu.VMEM((seqs, rows, half), F32),
        pltpu.VMEM((seqs, rows, half), F32),
        pltpu.VMEM((seqs, rows, half), BF16),
        pltpu.VMEM((seqs, rows, half), BF16),
        pltpu.VMEM((8, half), F32),
        pltpu.VMEM((8, half), F32),
        pltpu.VMEM((nb, COLS, COLS), BF16),
        pltpu.VMEM((nb, COLS, COLS), BF16),
        pltpu.VMEM((nb, COLS, COLS), BF16),
        pltpu.VMEM((rows, COLS), BF16),
        pltpu.VMEM((rows, COLS), F32),
        pltpu.VMEM((rows, COLS), F32),
        pltpu.VMEM((2 * seqs, rows, 2 * half), BF16),
        pltpu.VMEM((2 * seqs, 8, half), F32),
        pltpu.VMEM((2 * seqs * (n - 1), 8, half), F32),
        pltpu.VMEM((2 * seqs, half), F32),
        pltpu.VMEM((PEER_SLOTS, *tile), F32),
        pltpu.VMEM((count, *tile), F32),
        pltpu.VMEM((2 * count, *tile), BF16),
        pltpu.VMEM((2 * count, *tile), BF16),
        pltpu.VMEM((count, *tile), BF16),
        pltpu.VMEM((count, *tile), BF16),
        dma((4,)), dma((4,)), dma((8 * (n + 1),)), dma((8 * n,)), dma(((n + 1) * hops,)),
        dma((n * hops,)), dma((8 * n * hops,)), dma((8 * n * hops,)), dma((10,)),
        dma((3 * seqs,)), dma((3 * seqs,)), dma((seqs + 1,)), dma((seqs + 1,)), dma((4,)),
        dma((4,)), dma((2 * seqs * (n - 1),)), dma((2 * seqs * (n - 1),)),
        dma((count * (seqs + 1),)), dma((count * (seqs + 1),)), dma((count * seqs,)),
        dma((count * seqs,)),
    ]
    return pl.pallas_call(
        functools.partial(kernel, n, m),
        name="layer",
        out_shape=pltpu.VMEM(tokens.shape, BF16),
        in_specs=[hbm, vmem, hbm, hbm, vmem, hbm, hbm, vmem, hbm, vmem, hbm, vmem, hbm, hbm],
        out_specs=vmem,
        scratch_shapes=scratch,
        compiler_params=pltpu.CompilerParams(
            collective_id=0, has_side_effects=True, vmem_limit_bytes=60 * 1024 * 1024),
    )(tokens, norm_gain[None], chain_entry, pool_entry, conv_taps, recur_gate, input_gate,
      decay_log[None], decay_shift, start_state, pool_mix, pool_scale[None],
      chain_exit, pool_exit)


def ring_kernel(
    n, m,
    tokens, gain, chain_entry, pool_entry, taps, rgate, igate, dlog, shift_hbm, start,
    pmix, pscale, chain_exit, pool_exit,
    out,
    w0, w1, w2, w3, raw, normed, cbuf, pbuf, shift, rg, ig, pm,
    convb, zr, zi, cum_a, cum_b, rec, pooled, my_ab, all_ab, ent, acc, sendbuf, recvbuf,
    s1, r1, s2, r2, t1s, t1r, t2s, t2r, loc, nsem, hsem_s, hsem_r, ab_s, ab_r, out_s, out_r,
):
    sp, fs, tp = lax.axis_index("sp"), lax.axis_index("fs"), lax.axis_index("tp")
    shards = (chain_entry, pool_entry, chain_exit, pool_exit)
    bufs = (w0, w1, w2, w3)
    seqs, half_rows, width = raw.shape
    rows = 2 * half_rows
    chans = cbuf.shape[2]
    nb = chans // COLS
    far = m // 2
    full = (m - 1) // 2

    def ring(i):
        return i + (i // 2) * (5 - 2 * i) if m == 4 else i

    pos = ring(fs)
    right, left = ring((pos + 1) % m), ring((pos + m - 1) % m)

    barrier = pltpu.get_barrier_semaphore()
    greet = [{"sp": (sp + k) % n} for k in range(1, n)] + [{"tp": 1 - tp}]
    greet += [{"fs": ring((pos + k) % m)} for k in range(1, m)]
    for device in greet:
        pl.semaphore_signal(barrier, inc=1, device_id=device, device_id_type=MESH)

    def span(w, part):
        block = shards[w].shape[0]
        tail = block // 8 // 16 * 16
        head = block - tail
        cut = -(-head // 32) * 16
        if w % 2:
            cut = head - cut
        return {"all": (0, block), None: (0, head), 0: (0, cut), 1: (cut, head - cut),
                2: (head, tail)}[part]

    def region(w, p, q, part=None):
        lo, size = span(w, part)
        at = (((sp + p) % n) * m + ring((pos + q + m) % m)) * shards[w].shape[0] + lo
        return bufs[w].at[pl.ds(pl.multiple_of(at, 16), size)]

    def own(w, part=None):
        lo, size = span(w, part)
        return shards[w].at[pl.ds(lo, size)]

    has_tail = span(0, 2)[1] > 0 and m > 1

    started = []

    def launch(copy):
        copy.start()
        started.append(copy)

    def first(w, k):
        return pltpu.make_async_remote_copy(
            src_ref=own(w), dst_ref=region(w, 0, 0), send_sem=s1.at[w * n + k],
            recv_sem=r1.at[w * n + n - k], device_id={"sp": (sp + k) % n}, device_id_type=MESH)

    def first_wait(w, p):
        pltpu.make_async_remote_copy(
            src_ref=own(w), dst_ref=region(w, p, 0), send_sem=s1.at[w * n + p],
            recv_sem=r1.at[w * n + p], device_id={"sp": (sp + p) % n},
            device_id_type=MESH).wait_recv()

    def second(w, p, way, d):
        q = -d if way == 0 else d
        part = way if (m % 2 == 0 and d + 1 == far) else None
        if p == 0 and d == 0:
            src = own(w, part)
        else:
            src = region(w, p, q, part)
        at = ((w * n + p) * 2 + way) * max(far, 1) + d
        return pltpu.make_async_remote_copy(
            src_ref=src, dst_ref=region(w, p, q, part), send_sem=s2.at[at], recv_sem=r2.at[at],
            device_id={"fs": right if way == 0 else left}, device_id_type=MESH)

    def second_wait(w, p, way, d):
        q = -d if way == 0 else d
        part = way if (m % 2 == 0 and d == far) else None
        at = ((w * n + p) * 2 + way) * max(far, 1) + d - 1
        ref = region(w, p, q, part)
        pltpu.make_async_remote_copy(
            src_ref=ref, dst_ref=ref, send_sem=s2.at[at], recv_sem=r2.at[at],
            device_id={"fs": right if way == 0 else left}, device_id_type=MESH).wait_recv()

    def second_all(w, p):
        if far >= 1:
            for way in (0, 1):
                launch(second(w, p, way, 0))

    def forward(w, p):
        for d in range(1, far):
            for way in (0, 1):
                second_wait(w, p, way, d)
                launch(second(w, p, way, d))

    def last_wait(w, p):
        tail_wait(w, p)
        if far >= 1:
            for way in (0, 1):
                second_wait(w, p, way, far)

    def tail_one(w, k):
        return pltpu.make_async_remote_copy(
            src_ref=own(w, 2), dst_ref=region(w, 0, 0, 2), send_sem=t1s.at[w * m + k],
            recv_sem=t1r.at[w * m + m - k], device_id={"fs": ring((pos + k) % m)},
            device_id_type=MESH)

    def tail_one_wait(w, q):
        ref = region(w, 0, q, 2)
        pltpu.make_async_remote_copy(
            src_ref=ref, dst_ref=ref, send_sem=t1s.at[w * m + q], recv_sem=t1r.at[w * m + q],
            device_id={"fs": ring((pos + q) % m)}, device_id_type=MESH).wait_recv()

    def tail_two(w, q, k):
        at = (w * m + q) * n
        return pltpu.make_async_remote_copy(
            src_ref=own(w, 2) if q == 0 else region(w, 0, q, 2), dst_ref=region(w, 0, q, 2),
            send_sem=t2s.at[at + k], recv_sem=t2r.at[at + n - k],
            device_id={"sp": (sp + k) % n}, device_id_type=MESH)

    def tail_start(w):
        if has_tail:
            for k in range(1, m):
                launch(tail_one(w, k))

    def tail_forward(w):
        if has_tail:
            for q in range(m):
                if q:
                    tail_one_wait(w, q)
                for k in order:
                    launch(tail_two(w, q, k))

    def tail_wait(w, p):
        if has_tail and p:
            for q in range(m):
                ref = region(w, p, q, 2)
                at = (w * m + q) * n + p
                pltpu.make_async_remote_copy(
                    src_ref=ref, dst_ref=ref, send_sem=t2s.at[at], recv_sem=t2r.at[at],
                    device_id={"sp": (sp + p) % n}, device_id_type=MESH).wait_recv()

    order = sorted(range(1, n), key=lambda p: min(p, n - p))
    local = [
        pltpu.make_async_copy(tokens, raw, loc.at[0]),
        pltpu.make_async_copy(shift_hbm, shift, loc.at[1]),
        pltpu.make_async_copy(rgate, rg, loc.at[2]),
        pltpu.make_async_copy(igate, ig, loc.at[3]),
        pltpu.make_async_copy(pmix, pm, loc.at[4]),
    ] + [pltpu.make_async_copy(shards[w], region(w, 0, 0, "all"), loc.at[5 + w]) for w in range(4)]
    for copy in local:
        copy.start()

    pl.semaphore_wait(barrier, len(greet))
    for w in (0, 1):
        second_all(w, 0)
        for k in order:
            launch(first(w, k))
        tail_start(w)

    local[0].wait()
    mine = tp * half_rows

    def norm_step(i, c):
        s, r = i // (half_rows // ROWS), (i % (half_rows // ROWS)) * ROWS
        x = raw[s, pl.ds(pl.multiple_of(r, ROWS), ROWS), :].astype(F32)
        scale = lax.rsqrt(jnp.mean(x * x, axis=-1, keepdims=True) + NORM_EPSILON)
        normed[s, pl.ds(pl.multiple_of(mine + r, ROWS), ROWS), :] = (
            x * scale * gain[...]).astype(BF16)
        return c

    lax.fori_loop(0, seqs * (half_rows // ROWS), norm_step, 0)

    def normed_copy(owner):
        ref = normed.at[:, pl.ds(pl.multiple_of(owner * half_rows, ROWS), half_rows)]
        return pltpu.make_async_remote_copy(
            src_ref=ref, dst_ref=ref, send_sem=nsem.at[0], recv_sem=nsem.at[1],
            device_id={"tp": 1 - tp}, device_id_type=MESH)

    for p in order:
        for w in (0, 1):
            first_wait(w, p)
            second_all(w, p)
        if p == order[0]:
            launch(normed_copy(tp))
    for w in (0, 1):
        tail_forward(w)
    for w in (2, 3):
        for k in order:
            launch(first(w, k))
        tail_start(w)
    for p in [0] + order:
        for w in (0, 1):
            forward(w, p)
    for w in (2, 3):
        second_all(w, 0)
    for p in [0] + order:
        for w in (0, 1):
            last_wait(w, p)
    for p in order:
        for w in (2, 3):
            first_wait(w, p)
            second_all(w, p)
    for w in (2, 3):
        tail_forward(w)
    for copy in local[1:]:
        copy.wait()
    normed_copy(1 - tp).wait_recv()

    def lanes(c):
        return pl.ds(pl.multiple_of(c * COLS, COLS), COLS)

    def entry_step(i, c):
        s, b = i // nb, lanes(i % nb)
        x = normed[s]
        cbuf[s, HALO:, b] = jnp.dot(x, w0[:, b], preferred_element_type=F32).astype(BF16)
        pbuf[s, HALO:, b] = jnp.dot(x, w1[:, b], preferred_element_type=F32).astype(BF16)
        return c

    lax.fori_loop(0, seqs * nb, entry_step, 0)

    def halo(i, ref):
        return pltpu.make_async_remote_copy(
            src_ref=ref.at[:, rows:], dst_ref=ref.at[:, :HALO], send_sem=hsem_s.at[i],
            recv_sem=hsem_r.at[i], device_id={"sp": (sp + 1) % n}, device_id_type=MESH)

    todo = [(w, p) for p in [0] + order for w in (2, 3)]

    def some_forwards(count):
        for w, p in todo[:count]:
            forward(w, p)
        del todo[:count]

    some_forwards(2)

    @pl.when(sp < n - 1)
    def _():
        halo(0, cbuf).start()
        halo(1, pbuf).start()

    @pl.when(sp > 0)
    def _():
        halo(0, cbuf).wait_recv()
        halo(1, pbuf).wait_recv()

    @pl.when(sp == 0)
    def _():
        cbuf[:, :HALO, :] = jnp.zeros((seqs, HALO, chans), BF16)
        pbuf[:, :HALO, :] = jnp.zeros((seqs, HALO, chans), BF16)

    tap_count = taps.shape[0]
    inverse_length = 1.0 / (rows * n)

    def chain_step(g, s):
        b = lanes(g)
        tap = taps[:, b].astype(F32)

        def conv(i, c):
            r = pl.multiple_of(i * ROWS, ROWS)
            v = cbuf[s, pl.ds(r, ROWS + HALO), b].astype(F32)
            total = v * tap[tap_count - 1 : tap_count]
            for j in range(tap_count - 1):
                total = total + pltpu.roll(v, tap_count - 1 - j, 0) * tap[j : j + 1]
            convb[pl.ds(r, ROWS), :] = total[HALO:].astype(BF16)
            return c

        lax.fori_loop(0, rows // ROWS, conv, 0)
        x = convb[...]
        zr[...] = jnp.dot(x, rg[g], preferred_element_type=F32)
        zi[...] = jnp.dot(x, ig[g], preferred_element_type=F32)
        rate = -RECUR_SCALE * (jnp.exp(dlog[:, b]) * inverse_length)
        row = lax.broadcasted_iota(jnp.int32, (ROWS, COLS), 0)

        def scan(i, carry):
            r = pl.multiple_of(i * ROWS, ROWS)
            at = pl.ds(r, ROWS)
            log_decay = jax.nn.sigmoid(zr[at, :]) * rate + shift[s, at, b]
            a = jnp.exp(log_decay)
            d = (jnp.sqrt(neg_expm1(2.0 * log_decay)) * jax.nn.sigmoid(zi[at, :])
                 * convb[at, :].astype(F32))
            k = 1
            while k < ROWS:
                before = row >= k
                d = d + a * jnp.where(before, pltpu.roll(d, k, 0), 0.0)
                a = a * jnp.where(before, pltpu.roll(a, k, 0), 1.0)
                k *= 2
            d = d + a * carry[1]
            a = a * carry[0]
            cum_a[s, at, b] = a
            cum_b[s, at, b] = d
            return a[ROWS - 1 :], d[ROWS - 1 :]

        end = lax.fori_loop(
            0, rows // ROWS, scan, (jnp.ones((1, COLS), F32), jnp.zeros((1, COLS), F32)))
        my_ab[pl.ds(s, 1), b] = end[0]
        my_ab[pl.ds(seqs + s, 1), b] = end[1]

    for s in range(seqs):
        def chain_group(g, c, s=s):
            chain_step(g, s)
            return c

        for g0 in range(0, nb, 2):
            lax.fori_loop(g0, min(g0 + 2, nb), chain_group, 0)
            some_forwards(max(1, len(todo) // (2 * seqs)))

    def ab_copy(k):
        return pltpu.make_async_remote_copy(
            src_ref=my_ab, dst_ref=all_ab.at[k], send_sem=ab_s.at[k], recv_sem=ab_r.at[k],
            device_id={"sp": (sp + k) % n}, device_id_type=MESH)

    def pool_group(g):
        b = slice(g * COLS, (g + 1) * COLS)
        window = 2 ** (1 + g % 4)

        def diff(i, c):
            s, r = i // (rows // ROWS), pl.multiple_of((i % (rows // ROWS)) * ROWS, ROWS)
            v = pbuf[s, pl.ds(r, ROWS + HALO), b].astype(F32)
            total, k = v, 1
            while k < window:
                total = total + pltpu.roll(total, k, 0)
                k *= 2
            t = lax.broadcasted_iota(jnp.int32, (ROWS, COLS), 0) + (sp * rows + r + 1)
            count = jnp.minimum(t, window).astype(F32)
            convb_pool = total[HALO:] / count - v[HALO:]
            pooled[s, pl.ds(r, ROWS), b] = convb_pool.astype(BF16)
            return c

        lax.fori_loop(0, seqs * (rows // ROWS), diff, 0)
        for s in range(seqs):
            y = jnp.dot(pooled[s, :, b], pm[g], preferred_element_type=F32)
            pooled[s, :, b] = (y * pscale[:, b]).astype(BF16)

    pool_group(0)
    for k in range(1, n):
        @pl.when(sp + k < n)
        def _(k=k):
            ab_copy(k).start()

    for g in range(1, nb):
        pool_group(g)
        some_forwards(1)
    some_forwards(len(todo))

    ent[...] = start[...]
    for k in range(n - 1, 0, -1):
        @pl.when(sp >= k)
        def _(k=k):
            ab_copy(k).wait_recv()
            ent[...] = all_ab[k, :seqs, :] * ent[...] + all_ab[k, seqs : 2 * seqs, :]

    for s in range(seqs):
        def fix(i, c, s=s):
            at = pl.ds(pl.multiple_of(i * ROWS, ROWS), ROWS)
            rec[s, at, :] = (cum_a[s, at, :] * ent[s : s + 1, :] + cum_b[s, at, :]).astype(BF16)
            return c

        lax.fori_loop(0, rows // ROWS, fix, 0)

    dims = (((1,), (1,)), ((), ()))
    out_cols = sendbuf.shape[2]
    out_count = width // out_cols
    per_group = m * chain_exit.shape[0] // out_cols

    def out_lanes(j):
        return pl.ds(pl.multiple_of(j * out_cols, out_cols), out_cols)

    def partial(owner, j):
        at = pl.ds(pl.multiple_of(owner * half_rows, ROWS), half_rows)
        b = out_lanes(j)
        x = rec[:, at, :].reshape(seqs * half_rows, chans)
        y = pooled[:, at, :].reshape(seqs * half_rows, chans)
        return lax.dot_general(x, w2[b, :], dims, preferred_element_type=F32) + lax.dot_general(
            y, w3[b, :], dims, preferred_element_type=F32)

    def out_copy(j):
        return pltpu.make_async_remote_copy(
            src_ref=sendbuf.at[j], dst_ref=recvbuf.at[j], send_sem=out_s.at[j],
            recv_sem=out_r.at[j], device_id={"tp": 1 - tp}, device_id_type=MESH)

    def exit_step(j, c):
        sendbuf[j] = partial(1 - tp, j).astype(BF16)
        acc[j] = partial(tp, j)
        out_copy(j).start()
        return c

    def out_step(j, c):
        out_copy(j).wait_recv()
        total = (acc[j] + recvbuf[j].astype(F32)).astype(BF16)
        out[:, :, out_lanes(j)] = total.reshape(seqs, half_rows, out_cols)
        return c

    def group(p, step):
        j = ((sp + p) % n) * per_group
        lax.fori_loop(j, j + per_group, step, 0)

    before = None
    for p in [0] + order:
        for w in (2, 3):
            last_wait(w, p)
        group(p, exit_step)
        if before is not None:
            group(before, out_step)
        before = p
    group(before, out_step)

    def out_end(j, c):
        out_copy(j).wait_send()
        return c

    lax.fori_loop(0, out_count, out_end, 0)
    for copy in started:
        copy.wait_send()

    @pl.when(sp < n - 1)
    def _():
        halo(0, cbuf).wait_send()
        halo(1, pbuf).wait_send()

    for k in range(1, n):
        @pl.when(sp + k < n)
        def _(k=k):
            ab_copy(k).wait_send()


def ring_device(n, m, *args):
    (tokens, norm_gain, chain_entry, pool_entry, conv_taps, recur_gate, input_gate, decay_log,
     decay_shift, start_state, pool_mix, pool_scale, chain_exit, pool_exit) = args
    seqs, half_rows, width = tokens.shape
    rows, chans = 2 * half_rows, chain_entry.shape[1]
    nb = chans // COLS
    assert pool_mix.shape[0] % 4 == 0 and pool_mix.shape[1] == COLS
    far = max(m // 2, 1)
    hbm, vmem = pl.BlockSpec(memory_space=pl.ANY), pl.BlockSpec(memory_space=pltpu.VMEM)
    dma = pltpu.SemaphoreType.DMA
    ab_rows = -(-2 * seqs // 8) * 8
    out_cols = min(COLS, m * chain_exit.shape[1])
    out_count = width // out_cols
    scratch = [pltpu.VMEM((width, chans), BF16)] * 4 + [
        pltpu.VMEM((seqs, half_rows, width), BF16),
        pltpu.VMEM((seqs, rows, width), BF16),
        pltpu.VMEM((seqs, HALO + rows, chans), BF16),
        pltpu.VMEM((seqs, HALO + rows, chans), BF16),
        pltpu.VMEM((seqs, rows, chans), F32),
        pltpu.VMEM(recur_gate.shape, BF16),
        pltpu.VMEM(input_gate.shape, BF16),
        pltpu.VMEM(pool_mix.shape, BF16),
        pltpu.VMEM((rows, COLS), BF16),
        pltpu.VMEM((rows, COLS), F32),
        pltpu.VMEM((rows, COLS), F32),
        pltpu.VMEM((seqs, rows, chans), F32),
        pltpu.VMEM((seqs, rows, chans), F32),
        pltpu.VMEM((seqs, rows, chans), BF16),
        pltpu.VMEM((seqs, rows, chans), BF16),
        pltpu.VMEM((ab_rows, chans), F32),
        pltpu.VMEM((n, ab_rows, chans), F32),
        pltpu.VMEM((seqs, chans), F32),
        pltpu.VMEM((out_count, seqs * half_rows, out_cols), F32),
        pltpu.VMEM((out_count, seqs * half_rows, out_cols), BF16),
        pltpu.VMEM((out_count, seqs * half_rows, out_cols), BF16),
        dma((4 * n,)), dma((4 * n,)), dma((8 * n * far,)), dma((8 * n * far,)),
        dma((4 * m,)), dma((4 * m,)), dma((4 * m * n,)), dma((4 * m * n,)),
        dma((9,)), dma((2,)), dma((2,)), dma((2,)), dma((n,)), dma((n,)),
        dma((out_count,)), dma((out_count,)),
    ]
    return pl.pallas_call(
        functools.partial(ring_kernel, n, m),
        name="layer",
        out_shape=jax.ShapeDtypeStruct(tokens.shape, BF16),
        in_specs=[hbm, vmem, hbm, hbm, vmem, hbm, hbm, vmem, hbm, vmem, hbm, vmem, hbm, hbm],
        out_specs=vmem,
        scratch_shapes=scratch,
        compiler_params=pltpu.CompilerParams(
            collective_id=0, has_side_effects=True, vmem_limit_bytes=62 * 1024 * 1024),
    )(tokens, norm_gain[None], chain_entry, pool_entry, conv_taps, recur_gate, input_gate,
      decay_log[None], decay_shift, start_state, pool_mix, pool_scale[None],
      chain_exit.T, pool_exit.T)


def solution(mesh):
    in_specs = (
        P("fs", ("sp", "tp"), None),
        P(),
        P(("sp", "fs"), "tp"),
        P(("sp", "fs"), "tp"),
        P(None, "tp"),
        P("tp", None, None),
        P("tp", None, None),
        P("tp"),
        P("fs", "sp", "tp"),
        P("fs", "tp"),
        P("tp", None, None),
        P("tp"),
        P("tp", ("sp", "fs")),
        P("tp", ("sp", "fs")),
    )
    out_specs = P("fs", ("sp", "tp"), None)
    n, m = mesh.shape["sp"], mesh.shape["fs"]

    def layer(*args):
        wide = n > 1 and m > 2 and m % 2 == 0 and args[12].shape[1] % 128 == 0
        return (per_device if wide else ring_device)(n, m, *args)

    return jax.shard_map(
        layer, mesh=mesh, in_specs=in_specs, out_specs=out_specs, check_vma=False)
```

```python
import functools

import jax
import jax.numpy as jnp
from jax import lax
from jax.experimental import pallas as pl
from jax.experimental.pallas import tpu as pltpu
from jax.sharding import PartitionSpec as P

MESH = pl.DeviceIdType.MESH
NORM_EPSILON = 1e-06
RECUR_SCALE = 8.0
HALO = 16
COLS = 256
ROWS = 64
ENTRY = (0, 1)
EXIT = (2, 3)
OWN, PEER = 0, 1
TURN = 1
PEER_SLOTS = 2
F32 = jnp.float32
BF16 = jnp.bfloat16


def neg_expm1(x):
    y = -x
    poly = 1.0 - y * (1.0 / 9.0)
    for k in range(8, 1, -1):
        poly = 1.0 - y * (1.0 / k) * poly
    return jnp.where(y < 0.5, y * poly, 1.0 - jnp.exp(x))


def nearest(n):
    order = [sorted(range(n), key=lambda z, s=s: (abs(z - s), (z - s) * (-1 if 2 * s < n else 1)))
             for s in range(n)]
    return [sum(order[s][r] * n**s for s in range(n)) for r in range(n)]


def kernel(
    n, m,
    tokens, gain, chain_entry, pool_entry, taps, rgate, igate, dlog, shift_hbm, start,
    pmix, pscale, chain_exit, pool_exit,
    out,
    w0, w1, exits, raw, normed, cum_a, cum_b, cbuf, pbuf, shift, wide, narrow, peer_shift,
    my_start, peer_start, rg, ig, pm,
    convb, zr, zi, mix, my_ab, all_ab, ent,
    peer_acc, own_acc, core_send, core_recv, x_send, x_recv,
    xs, xr, zs, zrv, zts, ztr, ys, yr, loc, nsem_s, nsem_r, ssem_s, ssem_r, hsem_s, hsem_r,
    ab_s, ab_r, core_s, core_r, out_s, out_r,
):
    scope = jax.named_scope
    sp, fs, tp = lax.axis_index("sp"), lax.axis_index("fs"), lax.axis_index("tp")
    ny = m // 2
    x, y = fs % 2, fs // 2
    shards = (chain_entry, pool_entry, chain_exit, pool_exit)
    bufs = (w0, w1)
    seqs, half_rows, width = raw.shape
    rows = 2 * half_rows
    half = cbuf.shape[2]
    rec, pooled = mix.at[:, :, pl.ds(0, half)], mix.at[:, :, pl.ds(half, half)]
    nb = half // COLS
    depth = chain_entry.shape[0]
    cols = chain_exit.shape[1]
    zdepth = m * depth
    own = range(seqs)
    last = n - 1

    codes = nearest(n)

    def digit(code):
        value = sp * 0
        for s in range(n):
            value = value + code // n**s % n * jnp.where(sp == s, 1, 0)
        return value

    ranks = [digit(code) for code in codes]
    units = (x, 1 - x)
    x_peer = {"fs": y * 2 + 1 - x}
    core_peer = {"tp": 1 - tp}

    def y_peer(k):
        return {"fs": ((y + k) % ny) * 2 + x}

    def y_from(k):
        return (y + ny - k) % ny

    barrier = pltpu.get_barrier_semaphore()
    greet = [{"sp": (sp + k) % n} for k in range(1, n)] + [core_peer, x_peer]
    greet += [y_peer(k) for k in range(1, ny)]
    for device in greet:
        pl.semaphore_signal(barrier, inc=1, device_id=device, device_id_type=MESH)

    started = []

    def launch(copy, cond=None):
        if cond is None:
            copy.start()
        else:
            pl.when(cond)(copy.start)
        started.append((copy, cond))

    def remote(src, dst, send, recv, device):
        return pltpu.make_async_remote_copy(
            src_ref=src, dst_ref=dst, send_sem=send, recv_sem=recv, device_id=device,
            device_id_type=MESH)

    def region(w, z, yy, xx):
        if w in ENTRY:
            b = z * m + yy * 2 + xx
            return bufs[w].at[pl.ds(pl.multiple_of(b * depth, depth), depth)]
        at = pl.ds((w - EXIT[0]) * half, half)
        return exits.at[z * 2 + xx, at, pl.ds(pl.multiple_of(yy * cols, cols), cols)]

    def shard(w, h):
        at = pl.ds(pl.multiple_of(h * half, half), half)
        return shards[w].at[:, at] if w in ENTRY else shards[w].at[at]

    def cross(w):
        return remote(shard(w, 1 - x), region(w, sp, y, x), xs.at[w], xr.at[w], x_peer)

    def cross_wait(w):
        ref = region(w, sp, y, 1 - x)
        remote(ref, ref, xs.at[w], xr.at[w], x_peer).wait_recv()

    def z_peer(way):
        return {"sp": (sp + (1, n - 1)[way]) % n}

    def z_copy(w, z, xx, way, src=None, home=False):
        ref = region(w, z, y, xx)
        at = (w * 2 + xx) * (n + 1)
        return remote(ref if src is None else src, ref, zs.at[at + (n if home and way else z)],
                      zrv.at[(w * 2 + xx) * n + z], z_peer(way))

    def z_turn(z, k, way, home=False):
        ref = region(TURN, z, y_from(k), x)
        at = (n if home and way else z) * (ny - 1) + k - 1
        return remote(ref, ref, zts.at[at], ztr.at[z * (ny - 1) + k - 1], z_peer(way))

    def y_copy(w, z, xx, k, src=None):
        ref = region(w, z, y, xx)
        at = ((w * n + z) * 2 + xx) * (ny - 1) + k - 1
        return remote(ref if src is None else src, ref, ys.at[at], yr.at[at], y_peer(k))

    def y_wait(w, z, xx, k):
        ref = region(w, z, y_from(k), xx)
        at = ((w * n + z) * 2 + xx) * (ny - 1) + k - 1
        remote(ref, ref, ys.at[at], yr.at[at], y_peer(k)).wait_recv()

    def source(w, unit):
        return shard(w, x) if unit == 0 else None

    def z_send(w, unit):
        if n > 1:
            launch(z_copy(w, sp, units[unit], 0, source(w, unit), True), sp + 1 < n)
            launch(z_copy(w, sp, units[unit], 1, source(w, unit), True), sp > 0)

    def exit_z_send(unit, to_end):
        ends = (sp + 2 == n, sp == 1) if n > 2 else (sp < 0, sp < 0)
        for w in EXIT:
            if n > 1:
                for way, inside in ((0, sp + 1 < n), (1, sp > 0)):
                    end = ends[way] if to_end else jnp.logical_not(ends[way])
                    launch(z_copy(w, sp, units[unit], way, source(w, unit), True), inside & end)

    def turn_send():
        for k in range(1, ny):
            if n > 1:
                launch(z_turn(sp, k, 0, True), sp + 1 < n)
                launch(z_turn(sp, k, 1, True), sp > 0)

    def y_send(w, unit):
        for k in range(1, ny):
            launch(y_copy(w, sp, units[unit], k, source(w, unit)))

    def both(cond, other):
        return other if cond is None else cond & other

    def relay_on(z, make, cond):
        if n > 2:
            launch(make(0), both(cond, (z < sp) & (sp + 1 < n)))
            launch(make(1), both(cond, (z > sp) & (sp > 0)))

    def wait_if(make, cond):
        if cond is None:
            make().wait_recv()
        else:
            pl.when(cond)(lambda: make().wait_recv())

    def forward(w, r, unit, cond=None):
        z, xx = ranks[r], units[unit]
        wait_if(lambda: z_copy(w, z, xx, 0), cond)
        relay_on(z, lambda way: z_copy(w, z, xx, way), cond)
        if (w, unit) != (TURN, 0):
            for k in range(1, ny):
                launch(y_copy(w, z, xx, k), cond)

    def turn_forward(r, cond=None):
        z = ranks[r]
        for k in range(1, ny):
            wait_if(lambda k=k: z_turn(z, k, 0), cond)
            relay_on(z, lambda way, k=k: z_turn(z, k, way), cond)

    edge = (sp == 0) | (sp == n - 1)
    inner = (sp > 0) & (sp < n - 1)

    def entry_forward(r, cond=None, part=None):
        todo = [(0, 0), (1, 0), (0, 1), (1, 1)]
        todo = todo if part is None else (todo[:3], todo[3:])[part]
        with scope(f"efwd#r={r}"):
            for w, unit in todo:
                forward(w, r, unit, cond)
            if part != 0:
                turn_forward(r, cond)

    def entry_arrived(r):
        for k in range(1, ny):
            for w in ENTRY:
                for unit in (0, 1):
                    if (w, unit) != (TURN, 0):
                        y_wait(w, ranks[r], units[unit], k)

    def exit_arrived(r, unit):
        for k in range(1, ny):
            for w in EXIT:
                y_wait(w, ranks[r], units[unit], k)

    def exit_forward(r, unit, cond=None):
        with scope(f"xfwd#r={r}#u={unit}"):
            for w in EXIT:
                if r:
                    forward(w, r, unit, cond)
                else:
                    cross_wait(w)
                    y_send(w, unit)
            if r == 0:
                exit_z_send(unit, False)

    def forwards(r, unit, cond):
        for rr in range(r, n if r == 3 else min(r + 1, n)):
            exit_forward(rr, unit, cond)

    def lanes(c, base=0):
        return pl.ds(pl.multiple_of(base + c * COLS, COLS), COLS)

    mine_lanes = pl.ds(pl.multiple_of(x * half, half), half)
    peer_lanes = pl.ds(pl.multiple_of((1 - x) * half, half), half)
    heads = pl.ds(x * nb, nb)

    local = [
        pltpu.make_async_copy(tokens, raw, loc.at[0]),
        pltpu.make_async_copy(shift_hbm.at[:, :, peer_lanes], wide, loc.at[1]),
        pltpu.make_async_copy(shift_hbm.at[:, :, mine_lanes], shift, loc.at[2]),
        pltpu.make_async_copy(rgate.at[heads], rg, loc.at[3]),
        pltpu.make_async_copy(igate.at[heads], ig, loc.at[4]),
        pltpu.make_async_copy(pmix.at[heads], pm, loc.at[5]),
    ] + [pltpu.make_async_copy(shard(w, x), region(w, sp, y, x), loc.at[6 + w]) for w in range(4)]
    for copy in local:
        copy.start()
    my_start[...] = jnp.zeros(my_start.shape, F32)
    my_start[:seqs, :] = start[:, peer_lanes]

    with scope("entry_barrier"):
        pl.semaphore_wait(barrier, len(greet))
    for w in ENTRY:
        launch(cross(w))
    for w in ENTRY:
        z_send(w, 0)
        y_send(w, 0)

    local[0].wait()

    def half_of(s, owner):
        return normed.at[s, pl.ds(pl.multiple_of(owner * half_rows, ROWS), half_rows)]

    def norm_x(s):
        return remote(half_of(s, tp), half_of(seqs + s, tp), nsem_s.at[s], nsem_r.at[s], x_peer)

    def norm_core(s):
        return remote(half_of(s, tp), half_of(s, tp), nsem_s.at[seqs + s], nsem_r.at[seqs + s],
                      core_peer)

    for s in own:
        def norm_step(i, c, s=s):
            r = pl.multiple_of(i * ROWS, ROWS)
            v = raw[s, pl.ds(r, ROWS), :].astype(F32)
            scale = lax.rsqrt(jnp.mean(v * v, axis=-1, keepdims=True) + NORM_EPSILON)
            normed[s, pl.ds(pl.multiple_of(tp * half_rows + r, ROWS), ROWS), :] = (
                v * scale * gain[...]).astype(BF16)
            return c

        lax.fori_loop(0, half_rows // ROWS, norm_step, 0)

    local[1].wait()

    def narrow_step(i, c):
        s, r = i // (rows // ROWS), pl.multiple_of((i % (rows // ROWS)) * ROWS, ROWS)
        narrow[s, pl.ds(r, ROWS), :] = wide[s, pl.ds(r, ROWS), :].astype(BF16)
        return c

    lax.fori_loop(0, seqs * (rows // ROWS), narrow_step, 0)
    for copy in local[2:]:
        copy.wait()
    start_copy = remote(my_start, peer_start, ssem_s.at[seqs], ssem_r.at[seqs], x_peer)

    def shift_copy(s):
        return remote(narrow.at[s], peer_shift.at[s], ssem_s.at[s], ssem_r.at[s], x_peer)

    for s in own:
        launch(norm_core(s))
    with scope("cross_fwd"):
        for w in ENTRY:
            cross_wait(w)
            z_send(w, 1)
            y_send(w, 1)
            if w == ENTRY[0]:
                launch(norm_x(0))
    launch(start_copy)
    for w in EXIT:
        y_send(w, 0)
    with scope("turn_fwd"):
        for k in range(1, ny):
            y_wait(TURN, sp, x, k)
        turn_send()

    def entry_part(s, r):
        at = pl.ds(pl.multiple_of(ranks[r] * zdepth, zdepth), zdepth)

        def step(j, c):
            b = lanes(j)
            v = normed[s, :, at]
            for w, total, dst in ((w0, cum_a, cbuf), (w1, cum_b, pbuf)):
                part = jnp.dot(v, w[at, b], preferred_element_type=F32)
                if r:
                    part = total[s, :, b] + part
                if r == last:
                    dst[s, HALO:, b] = part.astype(BF16)
                else:
                    total[s, :, b] = part
            return c

        lax.fori_loop(0, nb, step, 0)

    def core_wait(s):
        ref = half_of(s, 1 - tp)
        remote(ref, ref, nsem_s.at[seqs + s], nsem_r.at[seqs + s], core_peer).wait_recv()

    def relay(s):
        ref = half_of(seqs + s, tp)
        remote(ref, ref, nsem_s.at[s], nsem_r.at[s], x_peer).wait_recv()
        at = 2 * seqs + s
        launch(remote(ref, ref, nsem_s.at[at], nsem_r.at[at], core_peer))

    def relay_wait(s):
        ref = half_of(seqs + s, 1 - tp)
        at = 2 * seqs + s
        remote(ref, ref, nsem_s.at[at], nsem_r.at[at], core_peer).wait_recv()

    def entry_parts(seqs_of, r):
        with scope(f"edot#r={r}"):
            for s in seqs_of:
                entry_part(s, r)

    def entry_ready(r):
        with scope(f"earr#r={r}"):
            entry_arrived(r)

    peer = range(seqs, 2 * seqs)
    for r in range(1, last):
        entry_forward(r)
        if r == 1:
            for s in own:
                core_wait(s)
        entry_ready(r - 1)
        entry_parts(own, r - 1)
        if r == 1:
            for w in EXIT:
                launch(cross(w))
            for s in own[1:]:
                launch(norm_x(s))
            exit_z_send(0, False)
    if n > 1:
        entry_forward(last, inner)
    if n < 3:
        for s in own:
            core_wait(s)
        for w in EXIT:
            launch(cross(w))
        for s in own[1:]:
            launch(norm_x(s))
        exit_z_send(0, False)
    with scope("relay#s=0"):
        relay(0)
        relay_wait(0)
    for r in range(last - 1):
        entry_parts([seqs], r)
    if n > 1:
        entry_forward(last, edge, 0)
        entry_ready(last - 1)
        entry_parts(range(seqs + 1), last - 1)
    exit_z_send(0, True)
    forwards(1, 0, inner)
    forwards(2, 0, inner)
    if n > 1:
        entry_forward(last, edge, 1)
    exit_forward(0, 1)
    with scope("relay#s=1"):
        for s in own[1:]:
            relay(s)
    launch(shift_copy(0))
    with scope("relay_wait#s=1"):
        for s in own[1:]:
            relay_wait(s)
    for r in range(last):
        entry_parts(range(seqs + 1, 2 * seqs), r)
    with scope("earr_last"):
        entry_arrived(last)
    forwards(1, 0, edge)

    def halo(pair, i):
        ref = (cbuf, pbuf)[i]
        at = pl.ds(pair * seqs, seqs)
        return remote(ref.at[at, pl.ds(rows, HALO)], ref.at[at, pl.ds(0, HALO)],
                      hsem_s.at[pair * 2 + i], hsem_r.at[pair * 2 + i], {"sp": (sp + 1) % n})

    for pair in (PEER, OWN):
        for s in own:
            entry_part(pair * seqs + s, last)
        for i in (0, 1):
            launch(halo(pair, i), sp < n - 1)
    for s in own[1:]:
        launch(shift_copy(s))
    forwards(3, 0, inner)

    def halo_wait(pair):
        @pl.when(sp > 0)
        def _():
            halo(pair, 0).wait_recv()
            halo(pair, 1).wait_recv()

        @pl.when(sp == 0)
        def _():
            zero = jnp.zeros((seqs, HALO, half), BF16)
            cbuf[pair * seqs : (pair + 1) * seqs, :HALO, :] = zero
            pbuf[pair * seqs : (pair + 1) * seqs, :HALO, :] = zero

    tap_count = taps.shape[0]
    inverse_length = 1.0 / (rows * n)

    def chain(pair, s0):
        s = pair * seqs + s0

        def group(g, carry):
            b = lanes(g)
            whole = lanes(g, x * half)
            tap = taps[:, whole].astype(F32)

            def conv(i, c):
                r = pl.multiple_of(i * ROWS, ROWS)
                v = cbuf[s, pl.ds(r, ROWS + HALO), b].astype(F32)
                total = v * tap[tap_count - 1 : tap_count]
                for j in range(tap_count - 1):
                    total = total + pltpu.roll(v, tap_count - 1 - j, 0) * tap[j : j + 1]
                convb[pl.ds(r, ROWS), :] = total[HALO:].astype(BF16)
                return c

            lax.fori_loop(0, rows // ROWS, conv, 0)
            v = convb[...]
            zr[...] = jnp.dot(v, rg[g], preferred_element_type=F32)
            zi[...] = jnp.dot(v, ig[g], preferred_element_type=F32)
            rate = -RECUR_SCALE * (jnp.exp(dlog[:, whole]) * inverse_length)
            row = lax.broadcasted_iota(jnp.int32, (ROWS, COLS), 0)
            source = peer_shift if pair == PEER else shift

            def scan(i, ends):
                r = pl.multiple_of(i * ROWS, ROWS)
                at = pl.ds(r, ROWS)
                log_decay = (jax.nn.sigmoid(zr[at, :]) * rate
                             + source[s0, at, b].astype(F32))
                a = jnp.exp(log_decay)
                d = (jnp.sqrt(neg_expm1(2.0 * log_decay)) * jax.nn.sigmoid(zi[at, :])
                     * convb[at, :].astype(F32))
                k = 1
                while k < ROWS:
                    before = row >= k
                    d = d + a * jnp.where(before, pltpu.roll(d, k, 0), 0.0)
                    a = a * jnp.where(before, pltpu.roll(a, k, 0), 1.0)
                    k *= 2
                d = d + a * ends[1]
                a = a * ends[0]
                cum_a[s, at, b] = a
                cum_b[s, at, b] = d
                return a[ROWS - 1 :], d[ROWS - 1 :]

            end = lax.fori_loop(
                0, rows // ROWS, scan, (jnp.ones((1, COLS), F32), jnp.zeros((1, COLS), F32)))
            my_ab[s, pl.ds(0, 1), b] = end[0]
            my_ab[s, pl.ds(1, 1), b] = end[1]
            return carry

        with scope(f"chain#p={pair}#s={s0}"):
            lax.fori_loop(0, nb, group, 0)
        for k in range(1, n):
            launch(ab_copy(s, k), sp + k < n)

    def ab_copy(s, k):
        at = s * (n - 1) + k - 1
        return remote(my_ab.at[s], all_ab.at[at], ab_s.at[at], ab_r.at[at], {"sp": (sp + k) % n})

    def pool(pair):
        def group(g, window):
            b = lanes(g)

            def diff(i, c):
                s = pair * seqs + i // (rows // ROWS)
                r = pl.multiple_of((i % (rows // ROWS)) * ROWS, ROWS)
                v = pbuf[s, pl.ds(r, ROWS + HALO), b].astype(F32)
                total, k = v, 1
                while k < window:
                    total = total + pltpu.roll(total, k, 0)
                    k *= 2
                t = lax.broadcasted_iota(jnp.int32, (ROWS, COLS), 0) + (sp * rows + r + 1)
                count = jnp.minimum(t, window).astype(F32)
                pooled[s, pl.ds(r, ROWS), b] = (total[HALO:] / count - v[HALO:]).astype(BF16)
                return c

            lax.fori_loop(0, seqs * (rows // ROWS), diff, 0)
            for s0 in own:
                s = pair * seqs + s0
                p = jnp.dot(pooled[s, :, b], pm[g], preferred_element_type=F32)
                pooled[s, :, b] = (p * pscale[:, lanes(g, x * half)]).astype(BF16)

        with scope(f"pool#p={pair}"):
            for xx in (0, 1):
                @pl.when(x == xx)
                def _(xx=xx):
                    for g in range(nb):
                        group(g, 2 ** (1 + (xx * nb + g) % 4))

    def fix(pair, s0):
        s = pair * seqs + s0
        with scope(f"fix#p={pair}#s={s0}"):
            if pair == OWN:
                ent[s : s + 1, :] = start[s0 : s0 + 1, mine_lanes]
            else:
                ent[s : s + 1, :] = peer_start[s0 : s0 + 1, :]
            for k in range(n - 1, 0, -1):
                @pl.when(sp >= k)
                def _(k=k):
                    ab_copy(s, k).wait_recv()
                    at = s * (n - 1) + k - 1
                    ent[s : s + 1, :] = all_ab[at, 0:1, :] * ent[s : s + 1, :] + all_ab[at, 1:2, :]

            def step(i, c):
                at = pl.ds(pl.multiple_of(i * ROWS, ROWS), ROWS)
                rec[s, at, :] = (
                    cum_a[s, at, :] * ent[s : s + 1, :] + cum_b[s, at, :]).astype(BF16)
                return c

            lax.fori_loop(0, rows // ROWS, step, 0)

    groups = [(unit, r) for unit in (0, 1) for r in range(n)]
    count = len(groups)

    def core_copy(pair, c, which):
        at = pair * count + c
        sem = c * seqs + which.start if pair else count * seqs + c
        return remote(core_send.at[at, which], core_recv.at[at, which], core_s.at[sem],
                      core_r.at[sem], core_peer)

    def x_copy(c, which):
        sem = c * seqs + which.start
        return remote(x_send.at[c, which], x_recv.at[c, which], out_s.at[sem], out_r.at[sem],
                      x_peer)

    def owner_rows(owner):
        return pl.ds(pl.multiple_of(owner * half_rows, ROWS), half_rows)

    def slot(which, c):
        return slots.setdefault((c, which.start), len(slots) % PEER_SLOTS)

    slots = {}

    def dots(pair, which, c):
        unit, r = groups[c]
        size = which.size
        b = ranks[r] * 2 + units[unit]
        total = peer_acc.at[slot(which, c), which] if pair else own_acc.at[c, which]
        with scope(f"dots#p={pair}#s={which.start}#c={c}"):
            def part(owner):
                v = mix[pl.ds(pair * seqs + which.start, size), owner_rows(owner), :]
                v = v.reshape(size * half_rows, 2 * half)
                return jnp.dot(v, exits[b], preferred_element_type=F32).reshape(total.shape)

            core_send[pair * count + c, which] = part(1 - tp).astype(BF16)
            total[...] = part(tp)
        launch(core_copy(pair, c, which))

    def peer_send(which, c):
        with scope(f"send#s={which.start}#c={c}"):
            core_copy(PEER, c, which).wait_recv()
            x_send[c, which] = (
                peer_acc[slot(which, c), which]
                + core_recv[PEER * count + c, which].astype(F32)).astype(BF16)
        launch(x_copy(c, which))
        sent[c].append(which)

    sent = [[] for _ in groups]

    def own_out(c):
        unit, r = groups[c]
        other = groups.index((1 - unit, r))
        with scope(f"out#c={c}"):
            core_copy(OWN, c, every).wait_recv()
            for which in sent[other]:
                x_copy(other, which).wait_recv()
            total = (own_acc[c] + core_recv[OWN * count + c].astype(F32)
                     + x_recv[other].astype(F32)).astype(BF16)
            for yy in range(ny):
                col = (ranks[r] * m + yy * 2 + units[unit]) * cols
                out[:, :, pl.ds(pl.multiple_of(col, cols), cols)] = (
                    total[:, :, yy * cols : (yy + 1) * cols])

    every = pl.ds(0, seqs)
    waiting = []
    seen = set()

    def peer_step(which, c):
        if c not in seen:
            seen.add(c)
            with scope(f"xarr#c={c}"):
                exit_arrived(groups[c][1], groups[c][0])
        dots(PEER, which, c)
        flush()
        waiting.append((which, c))

    def flush():
        while waiting:
            peer_send(*waiting.pop())

    own_units = list(range(n))
    peer_units = list(range(n, 2 * n))
    later = own[1:]

    with scope("halo_p"):
        halo_wait(PEER)
    pool(PEER)
    forwards(2, 0, edge)
    with scope("shift_wait#s=0"):
        shift_copy(0).wait_recv()
    chain(PEER, 0)
    exit_z_send(1, True)
    forwards(1, 1, inner)
    forwards(2, 1, inner)
    with scope("start_wait"):
        start_copy.wait_recv()
    fix(PEER, 0)
    lead = own_units[:2] + peer_units[:1] + own_units[2:3]
    for c in lead[:2]:
        peer_step(pl.ds(0, 1), c)
    forwards(3, 0, edge)
    for c in lead[2:]:
        peer_step(pl.ds(0, 1), c)
    flush()
    for s0 in later:
        with scope(f"shift_wait#s={s0}"):
            shift_copy(s0).wait_recv()
        chain(PEER, s0)
    forwards(3, 1, inner)
    forwards(1, 1, edge)
    with scope("halo_o"):
        halo_wait(OWN)
    pool(OWN)
    tail = own_units[3:]
    for c in tail:
        peer_step(pl.ds(0, 1), c)
    for s0 in later:
        fix(PEER, s0)
        for c in lead + tail:
            peer_step(pl.ds(s0, 1), c)
    forwards(2, 1, edge)
    flush()
    chain(OWN, 0)
    for c in peer_units[1:2]:
        peer_step(every, c)
    forwards(3, 1, edge)
    flush()
    for s0 in later:
        chain(OWN, s0)
    for c in peer_units[2:3]:
        peer_step(every, c)
    for s0 in own:
        fix(OWN, s0)
    for c in lead[:2]:
        dots(OWN, every, c)
    flush()
    for c in peer_units[3:]:
        peer_step(every, c)
    for c in lead[2:4]:
        dots(OWN, every, c)
    flush()
    for c in lead[4:] + tail:
        dots(OWN, every, c)
    for c in peer_units[1:]:
        dots(OWN, every, c)
    for c in peer_units + own_units:
        own_out(c)

    with scope("drain"):
        for copy, cond in started:
            if cond is None:
                copy.wait_send()
            else:
                pl.when(cond)(copy.wait_send)


def per_device(n, m, *args):
    (tokens, norm_gain, chain_entry, pool_entry, conv_taps, recur_gate, input_gate, decay_log,
     decay_shift, start_state, pool_mix, pool_scale, chain_exit, pool_exit) = args
    seqs, half_rows, width = tokens.shape
    rows, half = 2 * half_rows, chain_entry.shape[1] // 2
    nb = half // COLS
    ny = m // 2
    assert pool_mix.shape[0] % 4 == 0 and pool_mix.shape[1] == COLS
    hbm, vmem = pl.BlockSpec(memory_space=pl.ANY), pl.BlockSpec(memory_space=pltpu.VMEM)
    dma = pltpu.SemaphoreType.DMA
    cols = ny * chain_exit.shape[1]
    count = 2 * n
    hops = ny - 1
    tile = (seqs, half_rows, cols)
    scratch = [pltpu.VMEM((width, half), BF16)] * 2 + [
        pltpu.VMEM((2 * n, 2 * half, cols), BF16),
        pltpu.VMEM((seqs, half_rows, width), BF16),
        pltpu.VMEM((2 * seqs, rows, width), BF16),
        pltpu.VMEM((2 * seqs, rows, half), F32),
        pltpu.VMEM((2 * seqs, rows, half), F32),
        pltpu.VMEM((2 * seqs, HALO + rows, half), BF16),
        pltpu.VMEM((2 * seqs, HALO + rows, half), BF16),
        pltpu.VMEM((seqs, rows, half), F32),
        pltpu.VMEM((seqs, rows, half), F32),
        pltpu.VMEM((seqs, rows, half), BF16),
        pltpu.VMEM((seqs, rows, half), BF16),
        pltpu.VMEM((8, half), F32),
        pltpu.VMEM((8, half), F32),
        pltpu.VMEM((nb, COLS, COLS), BF16),
        pltpu.VMEM((nb, COLS, COLS), BF16),
        pltpu.VMEM((nb, COLS, COLS), BF16),
        pltpu.VMEM((rows, COLS), BF16),
        pltpu.VMEM((rows, COLS), F32),
        pltpu.VMEM((rows, COLS), F32),
        pltpu.VMEM((2 * seqs, rows, 2 * half), BF16),
        pltpu.VMEM((2 * seqs, 8, half), F32),
        pltpu.VMEM((2 * seqs * (n - 1), 8, half), F32),
        pltpu.VMEM((2 * seqs, half), F32),
        pltpu.VMEM((PEER_SLOTS, *tile), F32),
        pltpu.VMEM((count, *tile), F32),
        pltpu.VMEM((2 * count, *tile), BF16),
        pltpu.VMEM((2 * count, *tile), BF16),
        pltpu.VMEM((count, *tile), BF16),
        pltpu.VMEM((count, *tile), BF16),
        dma((4,)), dma((4,)), dma((8 * (n + 1),)), dma((8 * n,)), dma(((n + 1) * hops,)),
        dma((n * hops,)), dma((8 * n * hops,)), dma((8 * n * hops,)), dma((10,)),
        dma((3 * seqs,)), dma((3 * seqs,)), dma((seqs + 1,)), dma((seqs + 1,)), dma((4,)),
        dma((4,)), dma((2 * seqs * (n - 1),)), dma((2 * seqs * (n - 1),)),
        dma((count * (seqs + 1),)), dma((count * (seqs + 1),)), dma((count * seqs,)),
        dma((count * seqs,)),
    ]
    return pl.pallas_call(
        functools.partial(kernel, n, m),
        name="layer",
        out_shape=pltpu.VMEM(tokens.shape, BF16),
        in_specs=[hbm, vmem, hbm, hbm, vmem, hbm, hbm, vmem, hbm, vmem, hbm, vmem, hbm, hbm],
        out_specs=vmem,
        scratch_shapes=scratch,
        compiler_params=pltpu.CompilerParams(
            collective_id=0, has_side_effects=True, vmem_limit_bytes=60 * 1024 * 1024),
    )(tokens, norm_gain[None], chain_entry, pool_entry, conv_taps, recur_gate, input_gate,
      decay_log[None], decay_shift, start_state, pool_mix, pool_scale[None],
      chain_exit, pool_exit)


def ring_kernel(
    n, m,
    tokens, gain, chain_entry, pool_entry, taps, rgate, igate, dlog, shift_hbm, start,
    pmix, pscale, chain_exit, pool_exit,
    out,
    w0, w1, w2, w3, raw, normed, cbuf, pbuf, shift, rg, ig, pm,
    convb, zr, zi, cum_a, cum_b, rec, pooled, my_ab, all_ab, ent, acc, sendbuf, recvbuf,
    s1, r1, s2, r2, t1s, t1r, t2s, t2r, loc, nsem, hsem_s, hsem_r, ab_s, ab_r, out_s, out_r,
):
    sp, fs, tp = lax.axis_index("sp"), lax.axis_index("fs"), lax.axis_index("tp")
    shards = (chain_entry, pool_entry, chain_exit, pool_exit)
    bufs = (w0, w1, w2, w3)
    seqs, half_rows, width = raw.shape
    rows = 2 * half_rows
    chans = cbuf.shape[2]
    nb = chans // COLS
    far = m // 2
    full = (m - 1) // 2

    def ring(i):
        return i + (i // 2) * (5 - 2 * i) if m == 4 else i

    pos = ring(fs)
    right, left = ring((pos + 1) % m), ring((pos + m - 1) % m)

    barrier = pltpu.get_barrier_semaphore()
    greet = [{"sp": (sp + k) % n} for k in range(1, n)] + [{"tp": 1 - tp}]
    greet += [{"fs": ring((pos + k) % m)} for k in range(1, m)]
    for device in greet:
        pl.semaphore_signal(barrier, inc=1, device_id=device, device_id_type=MESH)

    def span(w, part):
        block = shards[w].shape[0]
        tail = block // 8 // 16 * 16
        head = block - tail
        cut = -(-head // 32) * 16
        if w % 2:
            cut = head - cut
        return {"all": (0, block), None: (0, head), 0: (0, cut), 1: (cut, head - cut),
                2: (head, tail)}[part]

    def region(w, p, q, part=None):
        lo, size = span(w, part)
        at = (((sp + p) % n) * m + ring((pos + q + m) % m)) * shards[w].shape[0] + lo
        return bufs[w].at[pl.ds(pl.multiple_of(at, 16), size)]

    def own(w, part=None):
        lo, size = span(w, part)
        return shards[w].at[pl.ds(lo, size)]

    has_tail = span(0, 2)[1] > 0 and m > 1

    started = []

    def launch(copy):
        copy.start()
        started.append(copy)

    def first(w, k):
        return pltpu.make_async_remote_copy(
            src_ref=own(w), dst_ref=region(w, 0, 0), send_sem=s1.at[w * n + k],
            recv_sem=r1.at[w * n + n - k], device_id={"sp": (sp + k) % n}, device_id_type=MESH)

    def first_wait(w, p):
        pltpu.make_async_remote_copy(
            src_ref=own(w), dst_ref=region(w, p, 0), send_sem=s1.at[w * n + p],
            recv_sem=r1.at[w * n + p], device_id={"sp": (sp + p) % n},
            device_id_type=MESH).wait_recv()

    def second(w, p, way, d):
        q = -d if way == 0 else d
        part = way if (m % 2 == 0 and d + 1 == far) else None
        if p == 0 and d == 0:
            src = own(w, part)
        else:
            src = region(w, p, q, part)
        at = ((w * n + p) * 2 + way) * max(far, 1) + d
        return pltpu.make_async_remote_copy(
            src_ref=src, dst_ref=region(w, p, q, part), send_sem=s2.at[at], recv_sem=r2.at[at],
            device_id={"fs": right if way == 0 else left}, device_id_type=MESH)

    def second_wait(w, p, way, d):
        q = -d if way == 0 else d
        part = way if (m % 2 == 0 and d == far) else None
        at = ((w * n + p) * 2 + way) * max(far, 1) + d - 1
        ref = region(w, p, q, part)
        pltpu.make_async_remote_copy(
            src_ref=ref, dst_ref=ref, send_sem=s2.at[at], recv_sem=r2.at[at],
            device_id={"fs": right if way == 0 else left}, device_id_type=MESH).wait_recv()

    def second_all(w, p):
        if far >= 1:
            for way in (0, 1):
                launch(second(w, p, way, 0))

    def forward(w, p):
        for d in range(1, far):
            for way in (0, 1):
                second_wait(w, p, way, d)
                launch(second(w, p, way, d))

    def last_wait(w, p):
        tail_wait(w, p)
        if far >= 1:
            for way in (0, 1):
                second_wait(w, p, way, far)

    def tail_one(w, k):
        return pltpu.make_async_remote_copy(
            src_ref=own(w, 2), dst_ref=region(w, 0, 0, 2), send_sem=t1s.at[w * m + k],
            recv_sem=t1r.at[w * m + m - k], device_id={"fs": ring((pos + k) % m)},
            device_id_type=MESH)

    def tail_one_wait(w, q):
        ref = region(w, 0, q, 2)
        pltpu.make_async_remote_copy(
            src_ref=ref, dst_ref=ref, send_sem=t1s.at[w * m + q], recv_sem=t1r.at[w * m + q],
            device_id={"fs": ring((pos + q) % m)}, device_id_type=MESH).wait_recv()

    def tail_two(w, q, k):
        at = (w * m + q) * n
        return pltpu.make_async_remote_copy(
            src_ref=own(w, 2) if q == 0 else region(w, 0, q, 2), dst_ref=region(w, 0, q, 2),
            send_sem=t2s.at[at + k], recv_sem=t2r.at[at + n - k],
            device_id={"sp": (sp + k) % n}, device_id_type=MESH)

    def tail_start(w):
        if has_tail:
            for k in range(1, m):
                launch(tail_one(w, k))

    def tail_forward(w):
        if has_tail:
            for q in range(m):
                if q:
                    tail_one_wait(w, q)
                for k in order:
                    launch(tail_two(w, q, k))

    def tail_wait(w, p):
        if has_tail and p:
            for q in range(m):
                ref = region(w, p, q, 2)
                at = (w * m + q) * n + p
                pltpu.make_async_remote_copy(
                    src_ref=ref, dst_ref=ref, send_sem=t2s.at[at], recv_sem=t2r.at[at],
                    device_id={"sp": (sp + p) % n}, device_id_type=MESH).wait_recv()

    order = sorted(range(1, n), key=lambda p: min(p, n - p))
    local = [
        pltpu.make_async_copy(tokens, raw, loc.at[0]),
        pltpu.make_async_copy(shift_hbm, shift, loc.at[1]),
        pltpu.make_async_copy(rgate, rg, loc.at[2]),
        pltpu.make_async_copy(igate, ig, loc.at[3]),
        pltpu.make_async_copy(pmix, pm, loc.at[4]),
    ] + [pltpu.make_async_copy(shards[w], region(w, 0, 0, "all"), loc.at[5 + w]) for w in range(4)]
    for copy in local:
        copy.start()

    pl.semaphore_wait(barrier, len(greet))
    for w in (0, 1):
        second_all(w, 0)
        for k in order:
            launch(first(w, k))
        tail_start(w)

    local[0].wait()
    mine = tp * half_rows

    def norm_step(i, c):
        s, r = i // (half_rows // ROWS), (i % (half_rows // ROWS)) * ROWS
        x = raw[s, pl.ds(pl.multiple_of(r, ROWS), ROWS), :].astype(F32)
        scale = lax.rsqrt(jnp.mean(x * x, axis=-1, keepdims=True) + NORM_EPSILON)
        normed[s, pl.ds(pl.multiple_of(mine + r, ROWS), ROWS), :] = (
            x * scale * gain[...]).astype(BF16)
        return c

    lax.fori_loop(0, seqs * (half_rows // ROWS), norm_step, 0)

    def normed_copy(owner):
        ref = normed.at[:, pl.ds(pl.multiple_of(owner * half_rows, ROWS), half_rows)]
        return pltpu.make_async_remote_copy(
            src_ref=ref, dst_ref=ref, send_sem=nsem.at[0], recv_sem=nsem.at[1],
            device_id={"tp": 1 - tp}, device_id_type=MESH)

    for p in order:
        for w in (0, 1):
            first_wait(w, p)
            second_all(w, p)
        if p == order[0]:
            launch(normed_copy(tp))
    for w in (0, 1):
        tail_forward(w)
    for w in (2, 3):
        for k in order:
            launch(first(w, k))
        tail_start(w)
    for p in [0] + order:
        for w in (0, 1):
            forward(w, p)
    for w in (2, 3):
        second_all(w, 0)
    for p in [0] + order:
        for w in (0, 1):
            last_wait(w, p)
    for p in order:
        for w in (2, 3):
            first_wait(w, p)
            second_all(w, p)
    for w in (2, 3):
        tail_forward(w)
    for copy in local[1:]:
        copy.wait()
    normed_copy(1 - tp).wait_recv()

    def lanes(c):
        return pl.ds(pl.multiple_of(c * COLS, COLS), COLS)

    def entry_step(i, c):
        s, b = i // nb, lanes(i % nb)
        x = normed[s]
        cbuf[s, HALO:, b] = jnp.dot(x, w0[:, b], preferred_element_type=F32).astype(BF16)
        pbuf[s, HALO:, b] = jnp.dot(x, w1[:, b], preferred_element_type=F32).astype(BF16)
        return c

    lax.fori_loop(0, seqs * nb, entry_step, 0)

    def halo(i, ref):
        return pltpu.make_async_remote_copy(
            src_ref=ref.at[:, rows:], dst_ref=ref.at[:, :HALO], send_sem=hsem_s.at[i],
            recv_sem=hsem_r.at[i], device_id={"sp": (sp + 1) % n}, device_id_type=MESH)

    todo = [(w, p) for p in [0] + order for w in (2, 3)]

    def some_forwards(count):
        for w, p in todo[:count]:
            forward(w, p)
        del todo[:count]

    some_forwards(2)

    @pl.when(sp < n - 1)
    def _():
        halo(0, cbuf).start()
        halo(1, pbuf).start()

    @pl.when(sp > 0)
    def _():
        halo(0, cbuf).wait_recv()
        halo(1, pbuf).wait_recv()

    @pl.when(sp == 0)
    def _():
        cbuf[:, :HALO, :] = jnp.zeros((seqs, HALO, chans), BF16)
        pbuf[:, :HALO, :] = jnp.zeros((seqs, HALO, chans), BF16)

    tap_count = taps.shape[0]
    inverse_length = 1.0 / (rows * n)

    def chain_step(g, s):
        b = lanes(g)
        tap = taps[:, b].astype(F32)

        def conv(i, c):
            r = pl.multiple_of(i * ROWS, ROWS)
            v = cbuf[s, pl.ds(r, ROWS + HALO), b].astype(F32)
            total = v * tap[tap_count - 1 : tap_count]
            for j in range(tap_count - 1):
                total = total + pltpu.roll(v, tap_count - 1 - j, 0) * tap[j : j + 1]
            convb[pl.ds(r, ROWS), :] = total[HALO:].astype(BF16)
            return c

        lax.fori_loop(0, rows // ROWS, conv, 0)
        x = convb[...]
        zr[...] = jnp.dot(x, rg[g], preferred_element_type=F32)
        zi[...] = jnp.dot(x, ig[g], preferred_element_type=F32)
        rate = -RECUR_SCALE * (jnp.exp(dlog[:, b]) * inverse_length)
        row = lax.broadcasted_iota(jnp.int32, (ROWS, COLS), 0)

        def scan(i, carry):
            r = pl.multiple_of(i * ROWS, ROWS)
            at = pl.ds(r, ROWS)
            log_decay = jax.nn.sigmoid(zr[at, :]) * rate + shift[s, at, b]
            a = jnp.exp(log_decay)
            d = (jnp.sqrt(neg_expm1(2.0 * log_decay)) * jax.nn.sigmoid(zi[at, :])
                 * convb[at, :].astype(F32))
            k = 1
            while k < ROWS:
                before = row >= k
                d = d + a * jnp.where(before, pltpu.roll(d, k, 0), 0.0)
                a = a * jnp.where(before, pltpu.roll(a, k, 0), 1.0)
                k *= 2
            d = d + a * carry[1]
            a = a * carry[0]
            cum_a[s, at, b] = a
            cum_b[s, at, b] = d
            return a[ROWS - 1 :], d[ROWS - 1 :]

        end = lax.fori_loop(
            0, rows // ROWS, scan, (jnp.ones((1, COLS), F32), jnp.zeros((1, COLS), F32)))
        my_ab[pl.ds(s, 1), b] = end[0]
        my_ab[pl.ds(seqs + s, 1), b] = end[1]

    for s in range(seqs):
        def chain_group(g, c, s=s):
            chain_step(g, s)
            return c

        for g0 in range(0, nb, 2):
            lax.fori_loop(g0, min(g0 + 2, nb), chain_group, 0)
            some_forwards(max(1, len(todo) // (2 * seqs)))

    def ab_copy(k):
        return pltpu.make_async_remote_copy(
            src_ref=my_ab, dst_ref=all_ab.at[k], send_sem=ab_s.at[k], recv_sem=ab_r.at[k],
            device_id={"sp": (sp + k) % n}, device_id_type=MESH)

    def pool_group(g):
        b = slice(g * COLS, (g + 1) * COLS)
        window = 2 ** (1 + g % 4)

        def diff(i, c):
            s, r = i // (rows // ROWS), pl.multiple_of((i % (rows // ROWS)) * ROWS, ROWS)
            v = pbuf[s, pl.ds(r, ROWS + HALO), b].astype(F32)
            total, k = v, 1
            while k < window:
                total = total + pltpu.roll(total, k, 0)
                k *= 2
            t = lax.broadcasted_iota(jnp.int32, (ROWS, COLS), 0) + (sp * rows + r + 1)
            count = jnp.minimum(t, window).astype(F32)
            convb_pool = total[HALO:] / count - v[HALO:]
            pooled[s, pl.ds(r, ROWS), b] = convb_pool.astype(BF16)
            return c

        lax.fori_loop(0, seqs * (rows // ROWS), diff, 0)
        for s in range(seqs):
            y = jnp.dot(pooled[s, :, b], pm[g], preferred_element_type=F32)
            pooled[s, :, b] = (y * pscale[:, b]).astype(BF16)

    pool_group(0)
    for k in range(1, n):
        @pl.when(sp + k < n)
        def _(k=k):
            ab_copy(k).start()

    for g in range(1, nb):
        pool_group(g)
        some_forwards(1)
    some_forwards(len(todo))

    ent[...] = start[...]
    for k in range(n - 1, 0, -1):
        @pl.when(sp >= k)
        def _(k=k):
            ab_copy(k).wait_recv()
            ent[...] = all_ab[k, :seqs, :] * ent[...] + all_ab[k, seqs : 2 * seqs, :]

    for s in range(seqs):
        def fix(i, c, s=s):
            at = pl.ds(pl.multiple_of(i * ROWS, ROWS), ROWS)
            rec[s, at, :] = (cum_a[s, at, :] * ent[s : s + 1, :] + cum_b[s, at, :]).astype(BF16)
            return c

        lax.fori_loop(0, rows // ROWS, fix, 0)

    dims = (((1,), (1,)), ((), ()))
    out_cols = sendbuf.shape[2]
    out_count = width // out_cols
    per_group = m * chain_exit.shape[0] // out_cols

    def out_lanes(j):
        return pl.ds(pl.multiple_of(j * out_cols, out_cols), out_cols)

    def partial(owner, j):
        at = pl.ds(pl.multiple_of(owner * half_rows, ROWS), half_rows)
        b = out_lanes(j)
        x = rec[:, at, :].reshape(seqs * half_rows, chans)
        y = pooled[:, at, :].reshape(seqs * half_rows, chans)
        return lax.dot_general(x, w2[b, :], dims, preferred_element_type=F32) + lax.dot_general(
            y, w3[b, :], dims, preferred_element_type=F32)

    def out_copy(j):
        return pltpu.make_async_remote_copy(
            src_ref=sendbuf.at[j], dst_ref=recvbuf.at[j], send_sem=out_s.at[j],
            recv_sem=out_r.at[j], device_id={"tp": 1 - tp}, device_id_type=MESH)

    def exit_step(j, c):
        sendbuf[j] = partial(1 - tp, j).astype(BF16)
        acc[j] = partial(tp, j)
        out_copy(j).start()
        return c

    def out_step(j, c):
        out_copy(j).wait_recv()
        total = (acc[j] + recvbuf[j].astype(F32)).astype(BF16)
        out[:, :, out_lanes(j)] = total.reshape(seqs, half_rows, out_cols)
        return c

    def group(p, step):
        j = ((sp + p) % n) * per_group
        lax.fori_loop(j, j + per_group, step, 0)

    before = None
    for p in [0] + order:
        for w in (2, 3):
            last_wait(w, p)
        group(p, exit_step)
        if before is not None:
            group(before, out_step)
        before = p
    group(before, out_step)

    def out_end(j, c):
        out_copy(j).wait_send()
        return c

    lax.fori_loop(0, out_count, out_end, 0)
    for copy in started:
        copy.wait_send()

    @pl.when(sp < n - 1)
    def _():
        halo(0, cbuf).wait_send()
        halo(1, pbuf).wait_send()

    for k in range(1, n):
        @pl.when(sp + k < n)
        def _(k=k):
            ab_copy(k).wait_send()


def ring_device(n, m, *args):
    (tokens, norm_gain, chain_entry, pool_entry, conv_taps, recur_gate, input_gate, decay_log,
     decay_shift, start_state, pool_mix, pool_scale, chain_exit, pool_exit) = args
    seqs, half_rows, width = tokens.shape
    rows, chans = 2 * half_rows, chain_entry.shape[1]
    nb = chans // COLS
    assert pool_mix.shape[0] % 4 == 0 and pool_mix.shape[1] == COLS
    far = max(m // 2, 1)
    hbm, vmem = pl.BlockSpec(memory_space=pl.ANY), pl.BlockSpec(memory_space=pltpu.VMEM)
    dma = pltpu.SemaphoreType.DMA
    ab_rows = -(-2 * seqs // 8) * 8
    out_cols = min(COLS, m * chain_exit.shape[1])
    out_count = width // out_cols
    scratch = [pltpu.VMEM((width, chans), BF16)] * 4 + [
        pltpu.VMEM((seqs, half_rows, width), BF16),
        pltpu.VMEM((seqs, rows, width), BF16),
        pltpu.VMEM((seqs, HALO + rows, chans), BF16),
        pltpu.VMEM((seqs, HALO + rows, chans), BF16),
        pltpu.VMEM((seqs, rows, chans), F32),
        pltpu.VMEM(recur_gate.shape, BF16),
        pltpu.VMEM(input_gate.shape, BF16),
        pltpu.VMEM(pool_mix.shape, BF16),
        pltpu.VMEM((rows, COLS), BF16),
        pltpu.VMEM((rows, COLS), F32),
        pltpu.VMEM((rows, COLS), F32),
        pltpu.VMEM((seqs, rows, chans), F32),
        pltpu.VMEM((seqs, rows, chans), F32),
        pltpu.VMEM((seqs, rows, chans), BF16),
        pltpu.VMEM((seqs, rows, chans), BF16),
        pltpu.VMEM((ab_rows, chans), F32),
        pltpu.VMEM((n, ab_rows, chans), F32),
        pltpu.VMEM((seqs, chans), F32),
        pltpu.VMEM((out_count, seqs * half_rows, out_cols), F32),
        pltpu.VMEM((out_count, seqs * half_rows, out_cols), BF16),
        pltpu.VMEM((out_count, seqs * half_rows, out_cols), BF16),
        dma((4 * n,)), dma((4 * n,)), dma((8 * n * far,)), dma((8 * n * far,)),
        dma((4 * m,)), dma((4 * m,)), dma((4 * m * n,)), dma((4 * m * n,)),
        dma((9,)), dma((2,)), dma((2,)), dma((2,)), dma((n,)), dma((n,)),
        dma((out_count,)), dma((out_count,)),
    ]
    return pl.pallas_call(
        functools.partial(ring_kernel, n, m),
        name="layer",
        out_shape=jax.ShapeDtypeStruct(tokens.shape, BF16),
        in_specs=[hbm, vmem, hbm, hbm, vmem, hbm, hbm, vmem, hbm, vmem, hbm, vmem, hbm, hbm],
        out_specs=vmem,
        scratch_shapes=scratch,
        compiler_params=pltpu.CompilerParams(
            collective_id=0, has_side_effects=True, vmem_limit_bytes=62 * 1024 * 1024),
    )(tokens, norm_gain[None], chain_entry, pool_entry, conv_taps, recur_gate, input_gate,
      decay_log[None], decay_shift, start_state, pool_mix, pool_scale[None],
      chain_exit.T, pool_exit.T)


def solution(mesh):
    in_specs = (
        P("fs", ("sp", "tp"), None),
        P(),
        P(("sp", "fs"), "tp"),
        P(("sp", "fs"), "tp"),
        P(None, "tp"),
        P("tp", None, None),
        P("tp", None, None),
        P("tp"),
        P("fs", "sp", "tp"),
        P("fs", "tp"),
        P("tp", None, None),
        P("tp"),
        P("tp", ("sp", "fs")),
        P("tp", ("sp", "fs")),
    )
    out_specs = P("fs", ("sp", "tp"), None)
    n, m = mesh.shape["sp"], mesh.shape["fs"]

    def layer(*args):
        wide = n > 1 and m > 2 and m % 2 == 0 and args[12].shape[1] % 128 == 0
        return (per_device if wide else ring_device)(n, m, *args)

    return jax.shard_map(
        layer, mesh=mesh, in_specs=in_specs, out_specs=out_specs, check_vma=False)
```
